32 devices in a mesh: sp: 4 (over z), tp: 8 (over y, x, core).
Axes of the slice: x: 2, y: 2, z: 4, core: 2. Of those that a mesh axis runs over, the one named last changes fastest.
Arguments:
- latent: bfloat16 [2048, 4096], P(('sp', 'tp')), may hold values from -6 to 6
- context: bfloat16 [512, 4096], P('sp'), may hold values from -6 to 6
- condition: float32 [4096], P('sp'), may hold values from -6 to 6
- context_cond: float32 [4096], P('sp'), may hold values from -6 to 6
- mod_weight: bfloat16 [4096, 12288], P('sp', 'tp'), may hold values from -0.09375 to 0.09375
- norm_gain: float32 [4096], replicated, may hold values from 0.1 to 1.9
- query_weight: bfloat16 [4096, 4096], P(None, 'tp'), may hold values from -0.09375 to 0.09375
- key_weight: bfloat16 [4096, 2048], P(None, 'tp'), may hold values from -0.09375 to 0.09375
- value_weight: bfloat16 [4096, 2048], P(None, 'tp'), may hold values from -0.09375 to 0.09375
- out_weight: bfloat16 [4096, 4096], P(None, 'tp'), may hold values from -0.375 to 0.375
- query_gain: float32 [64], replicated, may hold values from 1.2 to 6
- key_gain: float32 [64], replicated, may hold values from 1.2 to 6
- context_lift: float32 [64], P('tp'), may hold values from 0.5 to 2
Outputs:
- updated: bfloat16 [2048, 4096], P(('sp', 'tp'))
The draws below stay inside these ranges and needn't reach their ends.
All inputs are finite; a program needn't handle non-finite values.
Results may differ from the reference program's by a relative error of at most 0.0085.
The reference program's roundings to bfloat16 on the way count: a program that leaves them out, or rounds other values in their place, can miss the bound.
Values may be sent and summed in bfloat16 or wider, within the bound.
A program may use at most 64 MiB of HBM per device.

```python
import math
import jax
import jax.numpy as jnp
from jax import lax

D = 4096
HD = 64
Q_HEADS = 64
KV_HEADS = 32
GRID_W = 64
CTX = 512
SEQ = 2048


def draw_query_gain(key, part):
    subkey = jax.random.fold_in(key, 101)
    return jax.random.uniform(subkey, (HD,), jnp.float32, 1.2, 2.0)


def draw_key_gain(key, part):
    subkey = jax.random.fold_in(key, 202)
    return jax.random.uniform(subkey, (HD,), jnp.float32, 1.2, 2.0)


def block_scale(rng, dims, split, low, largest):
    level, own = 1.0, jax.random.fold_in(rng, 6)
    for position, shards_of in split:
        draws = jnp.exp(jax.random.uniform(jax.random.fold_in(own, position), (shards_of,), jnp.float32, low / len(split), largest / len(split)))
        level = level * jnp.repeat(draws, dims[position] // shards_of).reshape([-1 if axis == position else 1 for axis in range(len(dims))])
    return level


def normal_values(rng, dims, spread, reach, pieces=(), kind=jnp.bfloat16):
    result = spread * jax.random.normal(rng, dims, jnp.float32)
    if pieces:
        result = result * block_scale(rng, dims, pieces, -0.22, 0.18)
    return jnp.clip(result, -reach, reach).astype(kind)


def setup_inputs(seed: int = 0) -> dict:
    seeds = jax.random.split(jax.random.key(seed), 14)
    latent = normal_values(seeds[0], (SEQ, D), 1.0, 6.0, ((0, 32),))
    context = normal_values(seeds[1], (CTX, D), 1.0, 6.0, ((0, 4),))
    condition = normal_values(seeds[2], (D,), 1.0, 6.0, ((0, 4),), jnp.float32)
    context_cond = normal_values(seeds[3], (D,), 1.0, 6.0, ((0, 4),), jnp.float32)
    mod_weight = normal_values(seeds[4], (D, 3 * D), D ** -0.5, 0.09375, ((0, 4), (1, 8)))
    norm_gain = jnp.clip(1.0 + 0.18 * jax.random.normal(seeds[5], (D,), jnp.float32), 0.1, 1.9)
    query_weight = normal_values(seeds[6], (D, Q_HEADS * HD), D ** -0.5, 0.09375, ((1, 8),))
    key_weight = normal_values(seeds[7], (D, KV_HEADS * HD), D ** -0.5, 0.09375, ((1, 8),))
    value_weight = normal_values(seeds[8], (D, KV_HEADS * HD), D ** -0.5, 0.09375, ((1, 8),))
    out_weight = normal_values(seeds[9], (Q_HEADS * HD, D), (Q_HEADS * HD // 16) ** -0.5, 0.375, ((1, 8),))
    query_gain = draw_query_gain(jax.random.fold_in(seeds[13], 71), 0)
    key_gain = draw_key_gain(jax.random.fold_in(seeds[13], 71), 0)
    context_lift = jnp.clip(0.5 + 1.5 * jax.random.uniform(seeds[12], (Q_HEADS,), jnp.float32) ** block_scale(seeds[12], (Q_HEADS,), ((0, 8),), -0.2, 0.2), 0.5, 2.0)
    return {"latent": latent, "context": context, "condition": condition, "context_cond": context_cond, "mod_weight": mod_weight, "norm_gain": norm_gain, "query_weight": query_weight, "key_weight": key_weight, "value_weight": value_weight, "out_weight": out_weight, "query_gain": query_gain, "key_gain": key_gain, "context_lift": context_lift}


EPS = 1e-06

def modulate(row_block, gain_vec, mod_row, model_width):
    row_values = row_block.astype(jnp.float32)
    normal = row_values * lax.rsqrt(lax.optimization_barrier(jnp.mean(row_values * row_values, axis=-1, keepdims=True)) + EPS)
    shift_part = mod_row[:model_width]
    scale_part = mod_row[model_width:2 * model_width]
    return (normal * gain_vec * (1.0 + scale_part) + shift_part).astype(jnp.bfloat16)

def head_norm(values, gain_vec):
    return values * lax.rsqrt(lax.optimization_barrier(jnp.mean(values * values, axis=-1, keepdims=True)) + EPS) * gain_vec

def rope_tables(positions, head_size):
    freq_count = head_size // 4
    inverse = 10000.0 ** (-jnp.arange(freq_count, dtype=jnp.float32) / freq_count)
    grid_row = (positions // GRID_W).astype(jnp.float32)
    grid_col = (positions % GRID_W).astype(jnp.float32)
    angles = jnp.concatenate([grid_row[:, None] * inverse, grid_col[:, None] * inverse], axis=-1)
    return (jnp.cos(angles), jnp.sin(angles))

def rotate(values, cos_table, sin_table):
    paired = values.reshape(values.shape[:-1] + (values.shape[-1] // 2, 2))
    even_part = paired[..., 0]
    odd_part = paired[..., 1]
    cos_wide = cos_table[:, None, :]
    sin_wide = sin_table[:, None, :]
    turned = jnp.stack([even_part * cos_wide - odd_part * sin_wide, even_part * sin_wide + odd_part * cos_wide], axis=-1)
    return turned.reshape(values.shape)

def reference(latent, context, condition, context_cond, mod_weight, norm_gain, query_weight, key_weight, value_weight, out_weight, query_gain, key_gain, context_lift):
    model_width = latent.shape[1]
    cond_pair = jax.nn.silu(jnp.stack([condition, context_cond]).astype(jnp.float32)).astype(jnp.bfloat16)
    modulation = jnp.dot(cond_pair, mod_weight, preferred_element_type=jnp.float32)
    normed = modulate(latent, norm_gain, modulation[0], model_width)
    normed_ctx = modulate(context, norm_gain, modulation[1], model_width)
    positions = jnp.arange(SEQ, dtype=jnp.int32)
    cos_table, sin_table = rope_tables(positions, HD)
    query_raw = jnp.dot(normed, query_weight, preferred_element_type=jnp.float32).reshape(SEQ, Q_HEADS, HD)
    queries = rotate(head_norm(query_raw, query_gain), cos_table, sin_table).astype(jnp.bfloat16)
    key_raw = jnp.dot(normed, key_weight, preferred_element_type=jnp.float32).reshape(SEQ, KV_HEADS, HD)
    keys = rotate(head_norm(key_raw, key_gain), cos_table, sin_table).astype(jnp.bfloat16)
    values = jnp.dot(normed, value_weight, preferred_element_type=jnp.float32).astype(jnp.bfloat16)
    ctx_raw = jnp.dot(normed_ctx, key_weight, preferred_element_type=jnp.float32).reshape(CTX, KV_HEADS, HD)
    ctx_keys = head_norm(ctx_raw, key_gain).astype(jnp.bfloat16)
    ctx_values = jnp.dot(normed_ctx, value_weight, preferred_element_type=jnp.float32).astype(jnp.bfloat16)
    group_size = Q_HEADS // KV_HEADS
    score_scale = HD ** (-0.5)
    query_heads = queries.reshape(SEQ, KV_HEADS, group_size, HD).transpose(1, 0, 2, 3)
    key_heads = keys.transpose(1, 0, 2)
    value_heads = values.reshape(SEQ, KV_HEADS, HD).transpose(1, 0, 2)
    ctx_key_heads = ctx_keys.transpose(1, 0, 2)
    ctx_value_heads = ctx_values.reshape(CTX, KV_HEADS, HD).transpose(1, 0, 2)
    lift_rows = context_lift.reshape(KV_HEADS, group_size)
    query_block = math.gcd(SEQ, 512)

    def per_head(inputs):
        q_head, k_head, v_head, ck_head, cv_head, lift_row = inputs
        k_wide = k_head.astype(jnp.float32)
        v_wide = v_head.astype(jnp.float32)
        ck_wide = ck_head.astype(jnp.float32)
        cv_wide = cv_head.astype(jnp.float32)
        blocks = q_head.reshape(SEQ // query_block, query_block, group_size, HD)

        def per_block(q_block):
            q_wide = q_block.astype(jnp.float32)
            lat_scores = jnp.einsum('qgd,kd->gqk', q_wide, k_wide) * score_scale
            ctx_scores = jnp.einsum('qgd,kd->gqk', q_wide, ck_wide) * score_scale + lift_row[:, None, None]
            peak = jnp.maximum(lax.optimization_barrier(jnp.max(lat_scores, axis=-1)), lax.optimization_barrier(jnp.max(ctx_scores, axis=-1)))[..., None]
            lat_expo = jnp.exp(lat_scores - peak)
            ctx_expo = jnp.exp(ctx_scores - peak)
            denom = lax.optimization_barrier(jnp.sum(lat_expo, axis=-1)) + lax.optimization_barrier(jnp.sum(ctx_expo, axis=-1))
            lat_probs = lax.optimization_barrier(lat_expo.astype(jnp.bfloat16)).astype(jnp.float32)
            ctx_probs = lax.optimization_barrier(ctx_expo.astype(jnp.bfloat16)).astype(jnp.float32)
            numer = jnp.einsum('gqk,kd->gqd', lat_probs, v_wide) + jnp.einsum('gqk,kd->gqd', ctx_probs, cv_wide)
            return (numer / denom[..., None]).astype(jnp.bfloat16)
        return lax.map(per_block, blocks)
    heads_out = lax.map(per_head, (query_heads, key_heads, value_heads, ctx_key_heads, ctx_value_heads, lift_rows))
    attended = heads_out.transpose(1, 3, 0, 2, 4).reshape(SEQ, Q_HEADS * HD)
    mixed = jnp.dot(attended, out_weight, preferred_element_type=jnp.float32).astype(jnp.bfloat16)
    gate_lat = modulation[0, 2 * model_width:]
    return (latent.astype(jnp.float32) + gate_lat * mixed.astype(jnp.float32)).astype(jnp.bfloat16)
```

```python
import functools

import jax
import jax.numpy as jnp
import numpy as np
from jax import lax
from jax.experimental import pallas as pl
from jax.experimental.pallas import tpu as pltpu
from jax.sharding import PartitionSpec as P

GRID_W = 64
EPS = 1e-06
MESH = pl.DeviceIdType.MESH
ANY = pl.BlockSpec(memory_space=pl.ANY)
VMEM = pl.BlockSpec(memory_space=pltpu.VMEM)
SMEM = pl.BlockSpec(memory_space=pltpu.SMEM)
BF16 = jnp.bfloat16
F32 = jnp.float32


def remote(src, dst, send, recv, index, axis, peer):
    return pltpu.make_async_remote_copy(
        src_ref=src, dst_ref=dst, send_sem=send.at[index], recv_sem=recv.at[index],
        device_id={axis: peer}, device_id_type=MESH,
    )


def greet(peers):
    barrier = pltpu.get_barrier_semaphore()
    for axis, peer in peers:
        pl.semaphore_signal(barrier, inc=1, device_id={axis: peer}, device_id_type=MESH)
    pl.semaphore_wait(barrier, len(peers))


def others(axis, count):
    me = lax.axis_index(axis)
    return [(axis, lax.rem(me + step, count)) for step in range(1, count)]


def gather_sems(count):
    return 13 if count == 8 else max(count - 1, 1)


class Gather:
    def __init__(self, count, own, full, send, recv):
        self.count, self.own, self.full, self.send, self.recv = count, own, full, send, recv
        self.me = lax.axis_index("tp")
        self.half = own.shape[0] // 2
        me = self.me
        if count == 8:
            self.core, self.x, self.y = me % 2, (me // 2) % 2, me // 4
            self.sib = me + 1 - 2 * self.core
            self.step = 1 - 2 * self.core
            self.xn = me + 2 - 4 * self.x
            self.yn = me + 4 - 8 * self.y
            self.dn = self.xn + 4 - 8 * self.y

    def part(self, ref, which):
        return ref if which is None else ref.at[pl.ds(which * self.half, self.half)]

    def copy(self, index):
        me, xn, yn, dn, sib = self.me, self.xn, self.yn, self.dn, self.sib
        origin, half, peer = {
            0: (me, 0, xn), 1: (me, 1, xn), 2: (me, 0, yn), 3: (me, 1, yn), 4: (me, None, sib),
            5: (xn, 1, yn), 6: (yn, 0, xn),
            7: (xn, 0, sib), 8: (xn, 1, sib), 9: (yn, 0, sib), 10: (yn, 1, sib),
            11: (dn, 0, sib), 12: (dn, 1, sib),
        }[index]
        source = self.own if index < 5 else self.full.at[origin]
        return remote(self.part(source, half), self.part(self.full.at[origin], half), self.send, self.recv, index, "tp", peer)

    def wait_recv(self, index):
        xn, yn, dn, sib, step = self.xn, self.yn, self.dn, self.sib, self.step
        origin, half = {
            0: (xn, 0), 1: (xn, 1), 2: (yn, 0), 3: (yn, 1), 4: (sib, None), 5: (dn, 1), 6: (dn, 0),
            7: (xn + step, 0), 8: (xn + step, 1), 9: (yn + step, 0), 10: (yn + step, 1),
            11: (dn + step, 0), 12: (dn + step, 1),
        }[index]
        ref = self.part(self.full.at[origin], half)
        remote(ref, ref, self.send, self.recv, index, "tp", sib).wait_recv()

    def direct(self, step):
        peer = lax.rem(self.me + step, self.count)
        return remote(self.own, self.full.at[self.me], self.send, self.recv, step - 1, "tp", peer)

    def start(self):
        if self.count == 8:
            for index in (1, 2, 4):
                self.copy(index).start()
        else:
            for step in range(1, self.count):
                self.direct(step).start()

    def second(self):
        if self.count == 8:
            for index in (0, 3):
                self.copy(index).start()

    def relay(self):
        if self.count == 8:
            for arrived, then in ((1, (5, 8)), (2, (6, 9))):
                self.wait_recv(arrived)
                for nxt in then:
                    self.copy(nxt).start()

    def before(self, index):
        if self.count != 8:
            @pl.when(index == 0)
            def _():
                for step in range(1, self.count):
                    origin = lax.rem(self.me - step + self.count, self.count)
                    ref = self.full.at[origin]
                    remote(ref, ref, self.send, self.recv, step - 1, "tp", origin).wait_recv()
            return

        @pl.when(index == 0)
        def _():
            self.wait_recv(4)

        @pl.when(index == 1)
        def _():
            for arrived, nxt in ((0, 7), (3, 10)):
                self.wait_recv(arrived)
                self.copy(nxt).start()
            self.wait_recv(7)
            self.wait_recv(8)

        @pl.when(index == 2)
        def _():
            self.wait_recv(9)
            self.wait_recv(10)

        @pl.when(index == 3)
        def _():
            self.wait_recv(5)
            self.copy(12).start()
            self.wait_recv(6)
            self.copy(11).start()
            self.wait_recv(12)
            self.wait_recv(11)

    def chip(self, index):
        if self.count == 8:
            return ((self.y + index // 2) % 2) * 2 + (self.x + index) % 2
        return index

    def finish(self):
        if self.count == 8:
            for index in range(13):
                self.copy(index).wait_send()
        else:
            for step in range(1, self.count):
                self.direct(step).wait_send()


def front_kernel(sp, tp, heads, kv_heads, head, stacked, lat, ctx, cond, mod_weight, gain, cos, sin, q_gain, k_gain, lift, *rest):
    weights, rest = rest[: 1 if stacked else 3], rest[1 if stacked else 3 :]
    (attended, gate, full, normed, wide, mod_wide, parts, partial, total, mod, gsc, shf, gains, q_all, kvs, top, acc,
     send, recv, psend, precv, msend, mrecv, zsend, zrecv, local) = rest
    s, f = lax.axis_index("sp"), lax.axis_index("tp")
    rows, model = lat.shape
    width = wide.shape[2]
    slots = wide.shape[0]
    groups = slots - 2
    tile = 2 * rows
    lat_rows = rows * tp
    keys = kvs.shape[2]
    mcols = partial.shape[1]
    tiles = tp // 2 + 1
    scale = head ** -0.5
    mod_in = pltpu.make_async_copy(mod_weight, mod_wide, local.at[slots + 3])
    mod_in.start()
    copies = []
    if stacked:
        copies.append(pltpu.make_async_copy(weights[0], wide, local.at[0]))
    else:
        for n in range(groups):
            copies.append(pltpu.make_async_copy(weights[0].at[:, n * width : (n + 1) * width], wide.at[n], local.at[n]))
        copies.append(pltpu.make_async_copy(weights[1], wide.at[groups], local.at[groups]))
        copies.append(pltpu.make_async_copy(weights[2], wide.at[groups + 1], local.at[groups + 1]))
    own = pltpu.make_async_copy(lat, full.at[f], local.at[slots])
    ctx_in = [
        pltpu.make_async_copy(ctx.at[pl.ds(n * rows, rows)], full.at[tp + n], local.at[slots + 1 + n]) for n in range(2)
    ]
    greet(others("tp", tp) + others("sp", sp))
    gather = Gather(tp, lat, full, send, recv)
    gather.start()
    for item in ctx_in + [own] + copies[::-1]:
        item.start()
    mod_in.wait()
    first_sum = jnp.dot(cond[...], mod_wide[...], preferred_element_type=F32)
    partial[...] = first_sum
    parts[s] = first_sum
    sends = []
    for step in range(1, sp):
        sends.append(remote(partial, parts.at[s], psend, precv, step - 1, "sp", lax.rem(s + step, sp)))
    for item in sends:
        item.start()
    for n in range(slots):
        row = q_gain[...] * scale if n < groups else k_gain[...]
        gains[n] = jnp.concatenate([row] * (width // head), axis=1) if width > head else row
    for step in range(1, sp):
        origin = lax.rem(s - step + sp, sp)
        remote(parts.at[origin], parts.at[origin], psend, precv, step - 1, "sp", origin).wait_recv()
    summed = parts[0]
    for n in range(1, sp):
        summed = summed + parts[n]
    total[...] = summed
    here = pl.ds(pl.multiple_of(f * mcols, mcols), mcols)
    mod[:, here] = summed
    outs = []
    for step in range(1, tp):
        outs.append(remote(total, mod.at[:, here], msend, mrecv, step - 1, "tp", lax.rem(f + step, tp)))
    for item in outs:
        item.start()
    gather.second()
    top[...] = jnp.full(top.shape, -1e30, F32)
    acc[...] = jnp.zeros(acc.shape, F32)
    for step in range(1, tp):
        origin = lax.rem(f - step + tp, tp)
        ref = mod.at[:, pl.ds(pl.multiple_of(origin * mcols, mcols), mcols)]
        remote(ref, ref, msend, mrecv, step - 1, "tp", origin).wait_recv()
    for r in range(2):
        gsc[r] = gain[...] * (1.0 + mod[r : r + 1, model : 2 * model])
        shf[r] = mod[r : r + 1, :model]
    gate[...] = mod[0:1, 2 * model :]
    gather.relay()
    for item in ctx_in + copies:
        item.wait()
    own.wait()

    ring = sp == 4
    right, left, far = (s + 1) % sp, (s + sp - 1) % sp, (s + 2) % sp

    def tile_first(number):
        if isinstance(number, int):
            return lat_rows if number == 0 else pl.multiple_of(gather.chip(number - 1) * tile, tile)
        chip = jnp.where(number == 0, tp // 2, gather.chip(jnp.maximum(number - 1, 0)))
        return pl.multiple_of(chip * tile, tile)

    def ring_copy(number, index):
        which, origin, peer = {
            0: (0, s, right), 1: (1, s, right), 2: (1, s, left), 3: (0, s, left), 4: (0, left, right), 5: (1, right, left),
        }[index]
        ref = kvs.at[origin, which, pl.ds(tile_first(number), tile)]
        return remote(ref, ref, zsend, zrecv, number * 6 + index, "sp", peer)

    def ring_wait(number, index):
        which, origin = {0: (0, left), 1: (1, left), 2: (1, right), 3: (0, right), 4: (0, far), 5: (1, far)}[index]
        ref = kvs.at[origin, which, pl.ds(tile_first(number), tile)]
        remote(ref, ref, zsend, zrecv, number * 6 + index, "sp", right).wait_recv()

    def forward(number):
        ring_wait(number, 0)
        ring_copy(number, 4).start()
        ring_wait(number, 2)
        ring_copy(number, 5).start()

    def direct(step):
        return remote(kvs.at[s], kvs.at[s], zsend, zrecv, step - 1, "sp", lax.rem(s + step, sp))

    even = lax.broadcasted_iota(jnp.int32, (tile, width), 1) % 2 == 0
    same = (
        lax.broadcasted_iota(jnp.int32, (width, width), 0) // head
        == lax.broadcasted_iota(jnp.int32, (width, width), 1) // head
    )
    ones = jnp.where(same, 1.0, 0.0).astype(BF16)
    by_row = (lax.broadcasted_iota(jnp.int32, (1, 2 * head), 1) % head) // 2 < head // 4
    grid_rows = cos.shape[0] - GRID_W
    part = min(tile, GRID_W)
    step_rows = 16

    def roll(v, by):
        if width % 128 == 0:
            return pltpu.roll(v, by % width, axis=1)
        return jnp.concatenate([v[:, width - by % width :], v[:, : width - by % width]], axis=1)

    def table(ref, first, is_ctx, fill):
        pieces = []
        for k in range(tile // part):
            at = jnp.where(is_ctx == 1, 0, first + k * part)
            row = ref[pl.ds(at // GRID_W, 1), :]
            col = ref[pl.ds(pl.multiple_of(grid_rows + at % GRID_W, 8), part), :]
            pieces.append(jnp.where(by_row, row, col))
        v = jnp.concatenate(pieces, axis=0) if len(pieces) > 1 else pieces[0]
        v = jnp.where(is_ctx == 1, fill, v)
        if width > v.shape[1]:
            return jnp.concatenate([v] * (width // v.shape[1]), axis=1)
        return v[:, :width]

    def one_tile(number, unused):
        @pl.when(number > 0)
        def _():
            gather.before(number - 1)

        is_ctx = jnp.where(number == 0, 1, 0)
        first = tile_first(number)
        base = first // rows

        def norm_rows(j, unused):
            slot = base + (j * step_rows) // rows
            row = pl.multiple_of((j * step_rows) % rows, step_rows)
            v = full[slot, pl.ds(row, step_rows), :].astype(F32)
            inv = lax.rsqrt(jnp.mean(v * v, axis=-1, keepdims=True) + EPS)
            out = v * inv * gsc[is_ctx] + shf[is_ctx]
            normed[pl.ds(pl.multiple_of(j * step_rows, step_rows), step_rows), :] = out.astype(BF16)
            return unused

        lax.fori_loop(0, tile // step_rows, norm_rows, 0)

        def turned(y, n):
            sq = y * y
            hi = sq.astype(BF16)
            lo = (sq - hi.astype(F32)).astype(BF16)
            mean = jnp.dot(hi, ones, preferred_element_type=F32) + jnp.dot(lo, ones, preferred_element_type=F32)
            u = y * lax.rsqrt(mean * (1.0 / head) + EPS) * gains[n]
            other = jnp.where(even, roll(u, -1), roll(u, 1))
            return (u * table(cos, first, is_ctx, 1.0) + other * table(sin, first, is_ctx, 0.0)).astype(BF16)

        def one_slot(m, unused):
            n = (m + groups) % slots
            y = jnp.dot(normed[...], wide[n], preferred_element_type=F32)

            @pl.when(m == 1)
            def _():
                kvs[s, 1, pl.ds(first, tile), :] = y.astype(BF16)
                if ring:
                    for index in (0, 2, 1, 3):
                        ring_copy(number, index).start()

            @pl.when(m == 0)
            def _():
                kvs[s, 0, pl.ds(first, tile), :] = turned(y, n)

            @pl.when(m > 1)
            def _():
                q_all[n, pl.ds(first, tile), :] = turned(y, n)

            return unused

        lax.fori_loop(0, jnp.where(number == 0, 2, slots), one_slot, 0)
        return unused

    lax.fori_loop(0, tiles, one_tile, 0)

    if not ring:
        for step in range(1, sp):
            direct(step).start()
    group = heads // kv_heads
    q_tile = min(256, lat_rows)
    q_tiles = lat_rows // q_tile

    def block(b, unused):
        if ring:
            @pl.when(b == 0)
            def _():
                for number in range(tiles - 2):
                    forward(number)

            @pl.when(b == 1)
            def _():
                forward(tiles - 1)
                for number in range(tiles):
                    ring_wait(number, 1)

            @pl.when(b == 2)
            def _():
                for number in range(tiles):
                    ring_wait(number, 3)

            @pl.when(b == 3)
            def _():
                for number in range(tiles):
                    ring_wait(number, 4)
                    ring_wait(number, 5)

            origin = (s + jnp.where(b == 1, sp - 1, jnp.where(b == 2, 1, jnp.where(b == 3, 2, 0)))) % sp
        else:
            @pl.when(b == 1)
            def _():
                for step in range(1, sp):
                    source = lax.rem(s - step + sp, sp)
                    remote(kvs.at[source], kvs.at[source], zsend, zrecv, step - 1, "sp", source).wait_recv()

            origin = (s + b) % sp

        def q_rows(t, unused):
            if ring:
                @pl.when((b == 0) & (t == q_tiles - 1))
                def _():
                    forward(tiles - 2)

            at = pl.ds(pl.multiple_of(t * q_tile, q_tile), q_tile)
            for h in range(kv_heads):
                k = kvs[origin, 0, :, h * head : (h + 1) * head]
                v = kvs[origin, 1, :, h * head : (h + 1) * head]
                v_wide = jnp.concatenate([v, jnp.ones((keys, head), BF16)], axis=1)
                for g in range(group):
                    n = h * group + g
                    slot, lane = (n * head) // width, (n * head) % width
                    q = q_all[slot, at, lane : lane + head]
                    scores = lax.dot_general(q, k, (((1,), (1,)), ((), ())), preferred_element_type=F32)
                    scores = jnp.concatenate([scores[:, :lat_rows], scores[:, lat_rows:] + lift[n]], axis=1)
                    before = top[n, at, :]
                    now = jnp.maximum(before, jnp.max(scores, axis=-1, keepdims=True))
                    expo = jnp.exp(scores - now)
                    keep = jnp.exp(before - now)
                    top[n, at, :] = now
                    acc[n, at, :] = acc[n, at, :] * keep + jnp.dot(expo.astype(BF16), v_wide, preferred_element_type=F32)
            return unused

        lax.fori_loop(0, q_tiles, q_rows, 0)
        return unused

    lax.fori_loop(0, sp, block, 0)

    def close(t, unused):
        at = pl.ds(pl.multiple_of(t * q_tile, q_tile), q_tile)
        for pair in range(heads // 2):
            two = [acc[2 * pair + n, at, :] for n in range(2)]
            two = [v[:, :head] / v[:, head:] for v in two]
            attended[at, pair * 2 * head : (pair + 1) * 2 * head] = jnp.concatenate(two, axis=1).astype(BF16)
        return unused

    lax.fori_loop(0, q_tiles, close, 0)
    if ring:
        for number in range(tiles):
            for index in range(6):
                ring_copy(number, index).wait_send()
    else:
        for step in range(1, sp):
            direct(step).wait_send()
    for item in sends + outs:
        item.wait_send()
    gather.finish()


def back_kernel(tp, att, weight, out, full, wide, total, mixed, landed, send, recv, asend, arecv, local):
    f = lax.axis_index("tp")
    rows, cols = att.shape
    own_rows = out.shape[0]
    out_cols = weight.shape[1]
    load = pltpu.make_async_copy(weight, wide, local.at[0])
    load.start()
    mine = pltpu.make_async_copy(att, full.at[f], local.at[1])
    mine.start()
    greet(others("tp", tp))
    gather = Gather(tp, att, full, send, recv)
    gather.start()
    gather.second()
    total[...] = jnp.zeros(total.shape, F32)
    gather.relay()
    mine.wait()
    load.wait()
    r_tile = min(256, rows)

    def chip_step(index, unused):
        gather.before(index)
        chip = gather.chip(index)

        def row_step(t, unused):
            at = pl.ds(pl.multiple_of(t * r_tile, r_tile), r_tile)
            value = total[at, :]
            for n in range(2):
                source = chip * 2 + n
                depth = pl.ds(pl.multiple_of(source * cols, cols), cols)
                value = value + jnp.dot(full[source, at, :], wide[depth, :], preferred_element_type=F32)
            total[at, :] = value
            return unused

        lax.fori_loop(0, rows // r_tile, row_step, 0)
        return unused

    lax.fori_loop(0, tp // 2, chip_step, 0)
    for peer in range(tp):
        mixed[peer] = total[peer * own_rows : (peer + 1) * own_rows, :].astype(BF16)
    sends = []
    for step in range(1, tp):
        peer = lax.rem(f + step, tp)
        sends.append(remote(mixed.at[peer], landed.at[f], asend, arecv, step - 1, "tp", peer))
    for item in sends:
        item.start()
    landed[f] = mixed[f]
    for step in range(1, tp):
        origin = lax.rem(f - step + tp, tp)
        remote(landed.at[origin], landed.at[origin], asend, arecv, step - 1, "tp", origin).wait_recv()
    for n in range(tp):
        out[:, n * out_cols : (n + 1) * out_cols] = landed[n]
    for item in sends:
        item.wait_send()
    gather.finish()


def tables(first, count, head):
    freqs = head // 4
    lane = jnp.arange(2 * head, dtype=jnp.int32) % head
    inverse = 10000.0 ** (-(lane // 2 % freqs).astype(F32) / freqs)
    sign = jnp.where(lane % 2 == 0, -1.0, 1.0)
    grid_rows = -(-(count // GRID_W) // 8) * 8
    index = jnp.arange(grid_rows + GRID_W, dtype=jnp.int32)
    spot = jnp.where(index < grid_rows, index + first // GRID_W, index - grid_rows)
    angles = spot.astype(F32)[:, None] * inverse
    return jnp.cos(angles), jnp.sin(angles) * sign


def local(sp, tp, latent, context, condition, context_cond, mod_weight, norm_gain, query_weight, key_weight,
          value_weight, out_weight, query_gain, key_gain, context_lift):
    rows, model = latent.shape
    ctx_rows = context.shape[0]
    head = query_gain.shape[0]
    heads = query_weight.shape[1] // head
    kv_heads = key_weight.shape[1] // head
    width = key_weight.shape[1]
    slots = query_weight.shape[1] // width + 2
    block = rows * tp
    keys = block + ctx_rows
    limit = 60 * 1024 * 1024
    cond_pair = jax.nn.silu(jnp.stack([condition, context_cond])).astype(BF16)
    mcols = mod_weight.shape[1]
    cos, sin = tables(lax.axis_index("sp") * block, block, head)
    stacked = width % 128 != 0
    weights = [query_weight, key_weight, value_weight]
    if stacked:
        weights = [jnp.stack([query_weight[:, n * width : (n + 1) * width] for n in range(slots - 2)] + weights[1:])]
    dma = pltpu.SemaphoreType.DMA
    count = gather_sems(tp)
    pieces = (tp // 2 + 1) * 6 if sp == 4 else sp - 1
    attended, gate = pl.pallas_call(
        functools.partial(front_kernel, sp, tp, heads, kv_heads, head, stacked),
        name="front",
        out_shape=(jax.ShapeDtypeStruct((block, heads * head), BF16), jax.ShapeDtypeStruct((1, model), F32)),
        in_specs=[ANY, ANY, VMEM, ANY, VMEM, VMEM, VMEM, VMEM, VMEM, SMEM] + [ANY] * len(weights),
        out_specs=(VMEM, VMEM),
        scratch_shapes=[
            pltpu.VMEM((tp + 2, rows, model), BF16),
            pltpu.VMEM((2 * rows, model), BF16),
            pltpu.VMEM((slots, model, width), BF16),
            pltpu.VMEM(mod_weight.shape, BF16),
            pltpu.VMEM((sp, 2, mcols), F32),
            pltpu.VMEM((2, mcols), F32),
            pltpu.VMEM((2, mcols), F32),
            pltpu.VMEM((2, mcols * tp), F32),
            pltpu.VMEM((2, 1, model), F32),
            pltpu.VMEM((2, 1, model), F32),
            pltpu.VMEM((slots, 1, width), F32),
            pltpu.VMEM((slots - 2, block, width), BF16),
            pltpu.VMEM((sp, 2, keys, width), BF16),
            pltpu.VMEM((heads, block, 1), F32),
            pltpu.VMEM((heads, block, 2 * head), F32),
            dma((count,)), dma((count,)), dma((sp - 1,)), dma((sp - 1,)), dma((tp - 1,)), dma((tp - 1,)),
            dma((pieces,)), dma((pieces,)),
            dma((slots + 4,)),
        ],
        compiler_params=pltpu.CompilerParams(collective_id=0, has_side_effects=True, vmem_limit_bytes=limit),
    )(latent, context, cond_pair, mod_weight, norm_gain.reshape(1, model), cos, sin, query_gain.reshape(1, head),
      key_gain.reshape(1, head), context_lift, *weights)
    mixed = pl.pallas_call(
        functools.partial(back_kernel, tp),
        name="back",
        out_shape=jax.ShapeDtypeStruct((rows, model), BF16),
        in_specs=[VMEM, ANY],
        out_specs=VMEM,
        scratch_shapes=[
            pltpu.VMEM((tp, block, heads * head), BF16),
            pltpu.VMEM(out_weight.shape, BF16),
            pltpu.VMEM((block, out_weight.shape[1]), F32),
            pltpu.VMEM((tp, rows, out_weight.shape[1]), BF16),
            pltpu.VMEM((tp, rows, out_weight.shape[1]), BF16),
            dma((count,)), dma((count,)), dma((tp - 1,)), dma((tp - 1,)), dma((2,)),
        ],
        compiler_params=pltpu.CompilerParams(collective_id=2, has_side_effects=True, vmem_limit_bytes=limit),
    )(attended, out_weight)
    return (latent.astype(F32) + gate * mixed.astype(F32)).astype(BF16)


def partner(s, order):
    return jnp.where(order == 0, s, jnp.where(order == 1, 3 - s, jnp.where(order == 2, (s + 2) % 4, s + 1 - 2 * (s % 2))))


class Square:
    def __init__(self, own, full, send, recv, base):
        self.own, self.full, self.send, self.recv, self.base = own, full, send, recv, base
        me = lax.axis_index("tp")
        self.me = me
        self.half = own.shape[0] // 2
        core, x, y = me % 2, (me // 2) % 2, me // 4
        self.sib = me + 1 - 2 * core
        self.step = 1 - 2 * core
        self.xn = me + 2 - 4 * x
        self.yn = me + 4 - 8 * y
        self.dn = self.xn + 4 - 8 * y

    def part(self, ref, which):
        return ref if which is None else ref.at[pl.ds(which * self.half, self.half)]

    def copy(self, index):
        me, xn, yn, dn, sib = self.me, self.xn, self.yn, self.dn, self.sib
        origin, half, peer = {
            0: (me, 0, xn), 1: (me, 1, xn), 2: (me, 0, yn), 3: (me, 1, yn), 4: (me, None, sib),
            5: (xn, 1, yn), 6: (yn, 0, xn),
            7: (xn, 0, sib), 8: (xn, 1, sib), 9: (yn, 0, sib), 10: (yn, 1, sib),
            11: (dn, 0, sib), 12: (dn, 1, sib),
        }[index]
        source = self.own if index < 5 else self.full.at[origin]
        return remote(self.part(source, half), self.part(self.full.at[origin], half), self.send, self.recv,
                      self.base + index, "tp", peer)

    def start(self, *indices):
        for index in indices:
            self.copy(index).start()

    def arrived(self, *indices):
        xn, yn, dn, sib, step = self.xn, self.yn, self.dn, self.sib, self.step
        for index in indices:
            origin, half = {
                0: (xn, 0), 1: (xn, 1), 2: (yn, 0), 3: (yn, 1), 4: (sib, None), 5: (dn, 1), 6: (dn, 0),
                7: (xn + step, 0), 8: (xn + step, 1), 9: (yn + step, 0), 10: (yn + step, 1),
                11: (dn + step, 0), 12: (dn + step, 1),
            }[index]
            ref = self.part(self.full.at[origin], half)
            remote(ref, ref, self.send, self.recv, self.base + index, "tp", sib).wait_recv()

    def finish(self):
        for index in range(13):
            self.copy(index).wait_send()


def whole_kernel(head, lat, ctx, cond, ctx_cond, mod_weight, gain, cos_in, sin_in, q_gain, k_gain, lift, wq, wk, wv, wo_in, out,
                 full, normed, wide, mod_wide, wo, parts, partial, total_mod, mod, gsc, shf, gains, cos, sin,
                 kv_out, kv_in, v_ones, q_out, q_in, o_out, att, total, mixed, landed, result,
                 send, recv, psend, precv, msend, mrecv, ksend, krecv, qsend, qrecv, osend, orecv, asend, arecv,
                 bsend, brecv, local):
    sp, tp = 4, 8
    s, f = lax.axis_index("sp"), lax.axis_index("tp")
    rows, model = lat.shape
    tile = 2 * rows
    block = rows * tp
    ctx_rows = ctx.shape[0]
    mcols = partial.shape[1]
    half_rows = rows // 2
    width = wk.shape[1]
    pack = 2 * head
    chunk = block // 2
    scale = head ** -0.5

    mod_in = pltpu.make_async_copy(mod_weight, mod_wide, local.at[0])
    mod_in.start()
    barrier = pltpu.get_barrier_semaphore()
    peers = others("tp", tp) + others("sp", sp)
    for axis, peer in peers:
        pl.semaphore_signal(barrier, inc=1, device_id={axis: peer}, device_id_type=MESH)
    ctx_in = [pltpu.make_async_copy(ctx.at[pl.ds(n * rows, rows)], full.at[tp + n], local.at[1 + n]) for n in range(2)]
    own = pltpu.make_async_copy(lat, full.at[f], local.at[3])
    weights = [
        pltpu.make_async_copy(wk, wide.at[0, :, pl.ds(0, width)], local.at[4]),
        pltpu.make_async_copy(wv, wide.at[0, :, pl.ds(width, width)], local.at[5]),
        pltpu.make_async_copy(wq, wide.at[1], local.at[6]),
    ]
    tabs = [pltpu.make_async_copy(cos_in, cos, local.at[7]), pltpu.make_async_copy(sin_in, sin, local.at[8])]
    out_w = [pltpu.make_async_copy(wo_in.at[:, n], wo.at[n], local.at[9 + n]) for n in range(sp)]
    pl.semaphore_wait(barrier, len(peers))
    gather = Square(lat, full, send, recv, 0)
    gather.start(1, 2, 4)
    for item in ctx_in + [own] + weights + tabs + out_w:
        item.start()
    pair = jnp.concatenate([cond[...], ctx_cond[...]], axis=0)
    pair = (pair / (1.0 + jnp.exp(-pair))).astype(BF16)
    mod_in.wait()
    first_sum = jnp.dot(pair, mod_wide[...], preferred_element_type=F32)
    partial[...] = first_sum
    parts[s] = first_sum
    sends = [remote(partial, parts.at[s], psend, precv, n - 1, "sp", partner(s, n)) for n in range(1, sp)]
    for item in sends:
        item.start()
    gains[0] = jnp.concatenate([k_gain[...]] * (width // head), axis=1)
    gains[1] = jnp.concatenate([q_gain[...] * scale] * (width // head), axis=1)
    total[...] = jnp.zeros(total.shape, F32)
    for n in range(1, sp):
        origin = partner(s, n)
        remote(parts.at[origin], parts.at[origin], psend, precv, n - 1, "sp", origin).wait_recv()
    summed = parts[0] + parts[1] + parts[2] + parts[3]
    total_mod[...] = summed
    here = pl.ds(pl.multiple_of(f * mcols, mcols), mcols)
    mod[:, here] = summed
    outs = [remote(total_mod, mod.at[:, here], msend, mrecv, step - 1, "tp", lax.rem(f + step, tp)) for step in range(1, tp)]
    for item in outs:
        item.start()
    gather.start(0, 3)
    for step in range(1, tp):
        origin = lax.rem(f - step + tp, tp)
        ref = mod.at[:, pl.ds(pl.multiple_of(origin * mcols, mcols), mcols)]
        remote(ref, ref, msend, mrecv, step - 1, "tp", origin).wait_recv()
    for r in range(2):
        gsc[r] = gain[...] * (1.0 + mod[r : r + 1, model : 2 * model])
        shf[r] = mod[r : r + 1, :model]
    gather.arrived(1)
    gather.start(5, 8)
    gather.arrived(2)
    gather.start(6, 9)
    for item in ctx_in + [own] + weights + tabs:
        item.wait()

    even = lax.broadcasted_iota(jnp.int32, (tile, width), 1) % 2 == 0
    same = (
        lax.broadcasted_iota(jnp.int32, (width, width), 0) // head
        == lax.broadcasted_iota(jnp.int32, (width, width), 1) // head
    )
    ones = jnp.where(same, 1.0, 0.0).astype(BF16)
    by_row = (lax.broadcasted_iota(jnp.int32, (1, pack), 1) % head) // 2 < head // 4
    low = lax.broadcasted_iota(jnp.int32, (tile, pack), 1) < head
    grid_rows = cos.shape[0] - GRID_W
    step_rows = 16
    steps = half_rows // step_rows

    def chip_at(index):
        x, y = (f // 2) % 2, f // 4
        return ((y + index // 2) % 2) * 2 + (x + index) % 2

    def kv_send(number, n):
        chip = chip_at(jnp.maximum(number - 1, 0))
        at_out = pl.multiple_of(jnp.where(number == 0, block, chip * tile), tile)
        at_in = pl.multiple_of(jnp.where(number == 0, sp * block + s * ctx_rows, s * block + chip * tile), tile)
        peer = partner(s, n)
        return remote(kv_out.at[peer, pl.ds(at_out, tile)], kv_in.at[pl.ds(at_in, tile)], ksend, krecv,
                      number * 3 + n - 1, "sp", peer)

    def kv_wait(number, n):
        chip = chip_at(jnp.maximum(number - 1, 0))
        origin = partner(s, n)
        at_in = pl.multiple_of(jnp.where(number == 0, sp * block + origin * ctx_rows, origin * block + chip * tile), tile)
        ref = kv_in.at[pl.ds(at_in, tile)]
        remote(ref, ref, ksend, krecv, number * 3 + n - 1, "sp", origin).wait_recv()

    def one_tile(number, unused):
        @pl.when(number == 1)
        def _():
            gather.arrived(4)

        @pl.when(number == 2)
        def _():
            gather.arrived(0)
            gather.start(7)
            gather.arrived(3)
            gather.start(10)
            gather.arrived(7, 8)

        @pl.when(number == 3)
        def _():
            gather.arrived(9, 10)

        @pl.when(number == 4)
        def _():
            gather.arrived(5)
            gather.start(12)
            gather.arrived(6)
            gather.start(11)
            gather.arrived(12, 11)

        is_ctx = jnp.where(number == 0, 1, 0)
        chip = chip_at(jnp.maximum(number - 1, 0))
        base = jnp.where(number == 0, tp, chip * 2)

        def norm_rows(j, unused):
            slot = base + (j // steps) % 2
            row = pl.multiple_of((j // (2 * steps)) * half_rows + (j % steps) * step_rows, step_rows)
            v = full[slot, pl.ds(row, step_rows), :].astype(F32)
            inv = lax.rsqrt(jnp.mean(v * v, axis=-1, keepdims=True) + EPS)
            value = v * inv * gsc[is_ctx] + shf[is_ctx]
            normed[pl.ds(pl.multiple_of(j * step_rows, step_rows), step_rows), :] = value.astype(BF16)
            return unused

        lax.fori_loop(0, tile // step_rows, norm_rows, 0)

        def table(ref, fill):
            pieces = []
            for c in range(2):
                for owner in range(2):
                    row = ref[pl.ds(s * tp + chip * 2 + owner, 1), :]
                    col = ref[grid_rows + c * half_rows : grid_rows + (c + 1) * half_rows, :]
                    pieces.append(jnp.where(by_row, row, col))
            v = jnp.concatenate(pieces, axis=0)
            v = jnp.where(is_ctx == 1, fill, v)
            return jnp.concatenate([v] * (width // pack), axis=1)

        cos_t, sin_t = table(cos, 1.0), table(sin, 0.0)

        def turned(y, row):
            sq = y * y
            hi = sq.astype(BF16)
            lo = (sq - hi.astype(F32)).astype(BF16)
            mean = jnp.dot(hi, ones, preferred_element_type=F32) + jnp.dot(lo, ones, preferred_element_type=F32)
            u = y * lax.rsqrt(mean * (1.0 / head) + EPS) * row
            other = jnp.where(even, pltpu.roll(u, width - 1, axis=1), pltpu.roll(u, 1, axis=1))
            return u * cos_t + other * sin_t

        y = jnp.dot(normed[...], wide[0], preferred_element_type=F32)
        k, v = turned(y[:, :width], gains[0]), y[:, width:]
        at_out = pl.ds(pl.multiple_of(jnp.where(number == 0, block, chip * tile), tile), tile)
        at_in = pl.ds(pl.multiple_of(jnp.where(number == 0, sp * block + s * ctx_rows, s * block + chip * tile), tile), tile)
        for n in range(width // pack):
            kc, vc = k[:, n * pack : (n + 1) * pack], v[:, n * pack : (n + 1) * pack]
            kv_out[2 * n, at_out, :] = jnp.where(low, kc, pltpu.roll(vc, head, axis=1)).astype(BF16)
            kv_out[2 * n + 1, at_out, :] = jnp.where(low, pltpu.roll(kc, head, axis=1), vc).astype(BF16)
        for n in range(1, sp):
            kv_send(number, n).start()
        kv_in[at_in, :] = kv_out[s, at_out, :]

        @pl.when(number > 0)
        def _():
            y = jnp.dot(normed[...], wide[1], preferred_element_type=F32)
            for n in range(2):
                q = turned(y[:, n * width : (n + 1) * width], gains[1]).astype(BF16)
                for m in range(2):
                    for c in range(2):
                        q_out[2 * n + m, c, pl.ds(pl.multiple_of(chip * rows, rows), rows), :] = (
                            q[c * rows : (c + 1) * rows, m * pack : (m + 1) * pack])

        return unused

    lax.fori_loop(0, tp // 2 + 1, one_tile, 0)

    def q_send(n, c):
        peer = partner(s, n)
        return remote(q_out.at[peer, c], q_in.at[n, c], qsend, qrecv, (n - 1) * 2 + c, "sp", peer)

    for n in range(1, sp):
        for c in range(2):
            q_send(n, c).start()
    q_in[0] = q_out[s]

    def wait_kv(number, unused):
        for n in range(1, sp):
            kv_wait(number, n)
        return unused

    lax.fori_loop(0, tp // 2 + 1, wait_kv, 0)
    keys = kv_in.shape[0]
    v_ones[...] = jnp.concatenate([kv_in[:, head:], jnp.ones((keys, head), BF16)], axis=1)
    for item in out_w:
        item.wait()
    lat_keys = sp * block
    pieces = 2 * sp
    lag = 2

    def o_send(order, c):
        return remote(o_out.at[order - 1, c], att.at[order, c, f], osend, orecv, (order - 1) * 2 + c, "sp", partner(s, order))

    def piece_of(p):
        order, c = p // 2, p % 2
        return Square(att.at[order, c, f], att.at[order, c], asend, arecv, p * 13)

    def back_send(c, step):
        peer = lax.rem(f + step, tp)
        return remote(mixed.at[c, peer], landed.at[c, f], bsend, brecv, c * (tp - 1) + step - 1, "tp", peer)

    def one_step(i, unused):
        @pl.when(i < pieces)
        def _():
            order, c = i // 2, i % 2

            @pl.when(order > 0)
            def _():
                ref = q_in.at[order, c]
                remote(ref, ref, qsend, qrecv, (order - 1) * 2 + c, "sp", partner(s, order)).wait_recv()

            results = []
            for g in range(2):
                q = q_in[order, c, :, g * head : (g + 1) * head]
                scores = lax.dot_general(q, kv_in[:, :head], (((1,), (1,)), ((), ())), preferred_element_type=F32)
                scores = jnp.concatenate([scores[:, :lat_keys], scores[:, lat_keys:] + lift[2 * s + g]], axis=1)
                peak = jnp.max(scores, axis=-1, keepdims=True)
                expo = jnp.exp(scores - peak).astype(BF16)
                acc = jnp.dot(expo, v_ones[...], preferred_element_type=F32)
                results.append(acc[:, :head] / acc[:, head:])
            value = jnp.concatenate(results, axis=1).astype(BF16)

            @pl.when(order == 0)
            def _():
                att[0, c, f] = value

            @pl.when(order > 0)
            def _():
                o_out[order - 1, c] = value
                o_send(order, c).start()

        def stage(delay):
            p = i - lag - delay
            return p, pl.when((p >= 0) & (p < pieces))

        p0, guard = stage(0)

        @guard
        def _():
            @pl.when(p0 >= 2)
            def _():
                order, c = p0 // 2, p0 % 2
                ref = att.at[order, c, f]
                remote(ref, ref, osend, orecv, (order - 1) * 2 + c, "sp", partner(s, order)).wait_recv()

            piece_of(p0).start(1, 2, 4, 0, 3)

        p1, guard = stage(1)

        @guard
        def _():
            piece = piece_of(p1)
            piece.arrived(1)
            piece.start(5, 8)
            piece.arrived(2)
            piece.start(6, 9)
            piece.arrived(0)
            piece.start(7)
            piece.arrived(3)
            piece.start(10)

        p2, guard = stage(2)

        @guard
        def _():
            piece = piece_of(p2)
            piece.arrived(5)
            piece.start(12)
            piece.arrived(6)
            piece.start(11)

        p3, guard = stage(3)

        @guard
        def _():
            piece_of(p3).arrived(4, 7, 8, 9, 10, 11, 12)
            order, c = p3 // 2, p3 % 2
            left = jnp.concatenate([att[order, c, n] for n in range(tp)], axis=1)
            total[c] += jnp.dot(left, wo[partner(s, order)].reshape(tp * pack, wo.shape[3]), preferred_element_type=F32)

            @pl.when(order == sp - 1)
            def _():
                for n in range(tp):
                    mixed[c, n] = total[c, n * half_rows : (n + 1) * half_rows, :].astype(BF16)
                for step in range(1, tp):
                    back_send(c, step).start()
                landed[c, f] = mixed[c, f]

        return unused

    lax.fori_loop(0, pieces + lag + 3, one_step, 0)
    cols = wo.shape[3]
    writes = []
    for c in range(2):
        for step in range(1, tp):
            origin = lax.rem(f - step + tp, tp)
            ref = landed.at[c, origin]
            remote(ref, ref, bsend, brecv, c * (tp - 1) + step - 1, "tp", origin).wait_recv()
        at = slice(c * half_rows, (c + 1) * half_rows)
        for n in range(tp):
            there = slice(n * cols, (n + 1) * cols)
            gate = mod[0:1, 2 * model + n * cols : 2 * model + (n + 1) * cols]
            result[at, there] = (full[f, at, there].astype(F32) + gate * landed[c, n].astype(F32)).astype(BF16)
        writes.append(pltpu.make_async_copy(result.at[pl.ds(c * half_rows, half_rows)], out.at[pl.ds(c * half_rows, half_rows)],
                                            local.at[9 + sp + c]))
        writes[-1].start()
    for item in sends + outs:
        item.wait_send()
    gather.finish()

    def drain_kv(number, unused):
        for n in range(1, sp):
            kv_send(number, n).wait_send()
        return unused

    lax.fori_loop(0, tp // 2 + 1, drain_kv, 0)
    for n in range(1, sp):
        for c in range(2):
            q_send(n, c).wait_send()
            o_send(n, c).wait_send()

    def drain_pieces(p, unused):
        piece_of(p).finish()
        return unused

    lax.fori_loop(0, pieces, drain_pieces, 0)
    for c in range(2):
        for step in range(1, tp):
            back_send(c, step).wait_send()
    for item in writes:
        item.wait()


def all_tables(count, head):
    freqs = head // 4
    lane = np.arange(2 * head) % head
    inverse = (10000.0 ** (-(lane // 2 % freqs).astype(np.float32) / freqs)).astype(np.float32)
    sign = np.where(lane % 2 == 0, -1.0, 1.0).astype(np.float32)
    spot = np.concatenate([np.arange(count // GRID_W), np.arange(GRID_W)]).astype(np.float32)
    angles = (spot[:, None] * inverse).astype(np.float32)
    return np.cos(angles).astype(np.float32), (np.sin(angles) * sign).astype(np.float32)


def whole(sp, tp, latent, context, condition, context_cond, mod_weight, norm_gain, query_weight, key_weight,
          value_weight, out_weight, query_gain, key_gain, context_lift):
    rows, model = latent.shape
    head = query_gain.shape[0]
    block = rows * tp
    ctx_rows = context.shape[0]
    width = key_weight.shape[1]
    mcols = mod_weight.shape[1]
    out_cols = out_weight.shape[1]
    pack = 2 * head
    chunk = block // 2
    keys = sp * (block + ctx_rows)
    cos, sin = all_tables(sp * block, head)
    dma = lambda *shape: pltpu.SemaphoreType.DMA(shape)
    vm = pltpu.VMEM
    tiles = tp // 2 + 1
    return pl.pallas_call(
        functools.partial(whole_kernel, head),
        name="whole",
        out_shape=jax.ShapeDtypeStruct((rows, model), BF16),
        in_specs=[ANY, ANY, VMEM, VMEM, ANY, VMEM, ANY, ANY, VMEM, VMEM, SMEM, ANY, ANY, ANY, ANY],
        out_specs=ANY,
        scratch_shapes=[
            vm((tp + 2, rows, model), BF16),
            vm((2 * rows, model), BF16),
            vm((2, model, 2 * width), BF16),
            vm(mod_weight.shape, BF16),
            vm((sp, tp, pack, out_cols), BF16),
            vm((sp, 2, mcols), F32),
            vm((2, mcols), F32),
            vm((2, mcols), F32),
            vm((2, mcols * tp), F32),
            vm((2, 1, model), F32),
            vm((2, 1, model), F32),
            vm((2, 1, width), F32),
            vm(cos.shape, F32),
            vm(sin.shape, F32),
            vm((sp, block + ctx_rows, pack), BF16),
            vm((keys, pack), BF16),
            vm((keys, pack), BF16),
            vm((sp, 2, chunk, pack), BF16),
            vm((sp, 2, chunk, pack), BF16),
            vm((sp - 1, 2, chunk, pack), BF16),
            vm((sp, 2, tp, chunk, pack), BF16),
            vm((2, chunk, out_cols), F32),
            vm((2, tp, rows // 2, out_cols), BF16),
            vm((2, tp, rows // 2, out_cols), BF16),
            vm((rows, model), BF16),
            dma(13), dma(13), dma(sp - 1), dma(sp - 1), dma(tp - 1), dma(tp - 1),
            dma(tiles * 3), dma(tiles * 3), dma(6), dma(6), dma(6), dma(6),
            dma(13 * 8), dma(13 * 8), dma(2 * (tp - 1)), dma(2 * (tp - 1)),
            dma(9 + sp + 2),
        ],
        compiler_params=pltpu.CompilerParams(collective_id=1, has_side_effects=True, vmem_limit_bytes=62 * 1024 * 1024),
    )(latent, context, condition.reshape(1, -1), context_cond.reshape(1, -1), mod_weight, norm_gain.reshape(1, model),
      cos, sin, query_gain.reshape(1, head), key_gain.reshape(1, head), context_lift, query_weight, key_weight,
      value_weight, out_weight.reshape(tp, sp, pack, out_cols))


def fits(sp, tp, latent, context, key_weight, query_weight, query_gain):
    head = query_gain.shape[0]
    return (
        sp == 4 and tp == 8 and latent.shape[0] == GRID_W and context.shape[0] == 2 * latent.shape[0]
        and 2 * head == 128 and key_weight.shape[1] == sp * head and query_weight.shape[1] == 2 * sp * head
    )


def chosen(sp, tp, *args):
    latent, context, query_weight, key_weight, query_gain = args[0], args[1], args[6], args[7], args[10]
    if fits(sp, tp, latent, context, key_weight, query_weight, query_gain):
        return whole(sp, tp, *args)
    return local(sp, tp, *args)


def solution(mesh):
    return jax.shard_map(
        functools.partial(chosen, mesh.shape["sp"], mesh.shape["tp"]),
        mesh=mesh,
        in_specs=(
            P(("sp", "tp"), None),
            P("sp", None),
            P("sp"),
            P("sp"),
            P("sp", "tp"),
            P(),
            P(None, "tp"),
            P(None, "tp"),
            P(None, "tp"),
            P(None, "tp"),
            P(),
            P(),
            P("tp"),
        ),
        out_specs=P(("sp", "tp"), None),
        check_vma=False,
    )
```

```python
import functools

import jax
import jax.numpy as jnp
import numpy as np
from jax import lax
from jax.experimental import pallas as pl
from jax.experimental.pallas import tpu as pltpu
from jax.sharding import PartitionSpec as P

GRID_W = 64
EPS = 1e-06
MESH = pl.DeviceIdType.MESH
ANY = pl.BlockSpec(memory_space=pl.ANY)
VMEM = pl.BlockSpec(memory_space=pltpu.VMEM)
SMEM = pl.BlockSpec(memory_space=pltpu.SMEM)
BF16 = jnp.bfloat16
F32 = jnp.float32


def remote(src, dst, send, recv, index, axis, peer):
    return pltpu.make_async_remote_copy(
        src_ref=src, dst_ref=dst, send_sem=send.at[index], recv_sem=recv.at[index],
        device_id={axis: peer}, device_id_type=MESH,
    )


def greet(peers):
    barrier = pltpu.get_barrier_semaphore()
    for axis, peer in peers:
        pl.semaphore_signal(barrier, inc=1, device_id={axis: peer}, device_id_type=MESH)
    pl.semaphore_wait(barrier, len(peers))


def others(axis, count):
    me = lax.axis_index(axis)
    return [(axis, lax.rem(me + step, count)) for step in range(1, count)]


def gather_sems(count):
    return 13 if count == 8 else max(count - 1, 1)


class Gather:
    def __init__(self, count, own, full, send, recv):
        self.count, self.own, self.full, self.send, self.recv = count, own, full, send, recv
        self.me = lax.axis_index("tp")
        self.half = own.shape[0] // 2
        me = self.me
        if count == 8:
            self.core, self.x, self.y = me % 2, (me // 2) % 2, me // 4
            self.sib = me + 1 - 2 * self.core
            self.step = 1 - 2 * self.core
            self.xn = me + 2 - 4 * self.x
            self.yn = me + 4 - 8 * self.y
            self.dn = self.xn + 4 - 8 * self.y

    def part(self, ref, which):
        return ref if which is None else ref.at[pl.ds(which * self.half, self.half)]

    def copy(self, index):
        me, xn, yn, dn, sib = self.me, self.xn, self.yn, self.dn, self.sib
        origin, half, peer = {
            0: (me, 0, xn), 1: (me, 1, xn), 2: (me, 0, yn), 3: (me, 1, yn), 4: (me, None, sib),
            5: (xn, 1, yn), 6: (yn, 0, xn),
            7: (xn, 0, sib), 8: (xn, 1, sib), 9: (yn, 0, sib), 10: (yn, 1, sib),
            11: (dn, 0, sib), 12: (dn, 1, sib),
        }[index]
        source = self.own if index < 5 else self.full.at[origin]
        return remote(self.part(source, half), self.part(self.full.at[origin], half), self.send, self.recv, index, "tp", peer)

    def wait_recv(self, index):
        xn, yn, dn, sib, step = self.xn, self.yn, self.dn, self.sib, self.step
        origin, half = {
            0: (xn, 0), 1: (xn, 1), 2: (yn, 0), 3: (yn, 1), 4: (sib, None), 5: (dn, 1), 6: (dn, 0),
            7: (xn + step, 0), 8: (xn + step, 1), 9: (yn + step, 0), 10: (yn + step, 1),
            11: (dn + step, 0), 12: (dn + step, 1),
        }[index]
        ref = self.part(self.full.at[origin], half)
        remote(ref, ref, self.send, self.recv, index, "tp", sib).wait_recv()

    def direct(self, step):
        peer = lax.rem(self.me + step, self.count)
        return remote(self.own, self.full.at[self.me], self.send, self.recv, step - 1, "tp", peer)

    def start(self):
        if self.count == 8:
            for index in (1, 2, 4):
                self.copy(index).start()
        else:
            for step in range(1, self.count):
                self.direct(step).start()

    def second(self):
        if self.count == 8:
            for index in (0, 3):
                self.copy(index).start()

    def relay(self):
        if self.count == 8:
            for arrived, then in ((1, (5, 8)), (2, (6, 9))):
                self.wait_recv(arrived)
                for nxt in then:
                    self.copy(nxt).start()

    def before(self, index):
        if self.count != 8:
            @pl.when(index == 0)
            def _():
                for step in range(1, self.count):
                    origin = lax.rem(self.me - step + self.count, self.count)
                    ref = self.full.at[origin]
                    remote(ref, ref, self.send, self.recv, step - 1, "tp", origin).wait_recv()
            return

        @pl.when(index == 0)
        def _():
            self.wait_recv(4)

        @pl.when(index == 1)
        def _():
            for arrived, nxt in ((0, 7), (3, 10)):
                self.wait_recv(arrived)
                self.copy(nxt).start()
            self.wait_recv(7)
            self.wait_recv(8)

        @pl.when(index == 2)
        def _():
            self.wait_recv(9)
            self.wait_recv(10)

        @pl.when(index == 3)
        def _():
            self.wait_recv(5)
            self.copy(12).start()
            self.wait_recv(6)
            self.copy(11).start()
            self.wait_recv(12)
            self.wait_recv(11)

    def chip(self, index):
        if self.count == 8:
            return ((self.y + index // 2) % 2) * 2 + (self.x + index) % 2
        return index

    def finish(self):
        if self.count == 8:
            for index in range(13):
                self.copy(index).wait_send()
        else:
            for step in range(1, self.count):
                self.direct(step).wait_send()


def front_kernel(sp, tp, heads, kv_heads, head, stacked, lat, ctx, cond, mod_weight, gain, cos, sin, q_gain, k_gain, lift, *rest):
    weights, rest = rest[: 1 if stacked else 3], rest[1 if stacked else 3 :]
    (attended, gate, full, normed, wide, mod_wide, parts, partial, total, mod, gsc, shf, gains, q_all, kvs, top, acc,
     send, recv, psend, precv, msend, mrecv, zsend, zrecv, local) = rest
    s, f = lax.axis_index("sp"), lax.axis_index("tp")
    rows, model = lat.shape
    width = wide.shape[2]
    slots = wide.shape[0]
    groups = slots - 2
    tile = 2 * rows
    lat_rows = rows * tp
    keys = kvs.shape[2]
    mcols = partial.shape[1]
    tiles = tp // 2 + 1
    scale = head ** -0.5
    mod_in = pltpu.make_async_copy(mod_weight, mod_wide, local.at[slots + 3])
    mod_in.start()
    copies = []
    if stacked:
        copies.append(pltpu.make_async_copy(weights[0], wide, local.at[0]))
    else:
        for n in range(groups):
            copies.append(pltpu.make_async_copy(weights[0].at[:, n * width : (n + 1) * width], wide.at[n], local.at[n]))
        copies.append(pltpu.make_async_copy(weights[1], wide.at[groups], local.at[groups]))
        copies.append(pltpu.make_async_copy(weights[2], wide.at[groups + 1], local.at[groups + 1]))
    own = pltpu.make_async_copy(lat, full.at[f], local.at[slots])
    ctx_in = [
        pltpu.make_async_copy(ctx.at[pl.ds(n * rows, rows)], full.at[tp + n], local.at[slots + 1 + n]) for n in range(2)
    ]
    greet(others("tp", tp) + others("sp", sp))
    gather = Gather(tp, lat, full, send, recv)
    gather.start()
    for item in ctx_in + [own] + copies[::-1]:
        item.start()
    mod_in.wait()
    first_sum = jnp.dot(cond[...], mod_wide[...], preferred_element_type=F32)
    partial[...] = first_sum
    parts[s] = first_sum
    sends = []
    for step in range(1, sp):
        sends.append(remote(partial, parts.at[s], psend, precv, step - 1, "sp", lax.rem(s + step, sp)))
    for item in sends:
        item.start()
    for n in range(slots):
        row = q_gain[...] * scale if n < groups else k_gain[...]
        gains[n] = jnp.concatenate([row] * (width // head), axis=1) if width > head else row
    for step in range(1, sp):
        origin = lax.rem(s - step + sp, sp)
        remote(parts.at[origin], parts.at[origin], psend, precv, step - 1, "sp", origin).wait_recv()
    summed = parts[0]
    for n in range(1, sp):
        summed = summed + parts[n]
    total[...] = summed
    here = pl.ds(pl.multiple_of(f * mcols, mcols), mcols)
    mod[:, here] = summed
    outs = []
    for step in range(1, tp):
        outs.append(remote(total, mod.at[:, here], msend, mrecv, step - 1, "tp", lax.rem(f + step, tp)))
    for item in outs:
        item.start()
    gather.second()
    top[...] = jnp.full(top.shape, -1e30, F32)
    acc[...] = jnp.zeros(acc.shape, F32)
    for step in range(1, tp):
        origin = lax.rem(f - step + tp, tp)
        ref = mod.at[:, pl.ds(pl.multiple_of(origin * mcols, mcols), mcols)]
        remote(ref, ref, msend, mrecv, step - 1, "tp", origin).wait_recv()
    for r in range(2):
        gsc[r] = gain[...] * (1.0 + mod[r : r + 1, model : 2 * model])
        shf[r] = mod[r : r + 1, :model]
    gate[...] = mod[0:1, 2 * model :]
    gather.relay()
    for item in ctx_in + copies:
        item.wait()
    own.wait()

    ring = sp == 4
    right, left, far = (s + 1) % sp, (s + sp - 1) % sp, (s + 2) % sp

    def tile_first(number):
        if isinstance(number, int):
            return lat_rows if number == 0 else pl.multiple_of(gather.chip(number - 1) * tile, tile)
        chip = jnp.where(number == 0, tp // 2, gather.chip(jnp.maximum(number - 1, 0)))
        return pl.multiple_of(chip * tile, tile)

    def ring_copy(number, index):
        which, origin, peer = {
            0: (0, s, right), 1: (1, s, right), 2: (1, s, left), 3: (0, s, left), 4: (0, left, right), 5: (1, right, left),
        }[index]
        ref = kvs.at[origin, which, pl.ds(tile_first(number), tile)]
        return remote(ref, ref, zsend, zrecv, number * 6 + index, "sp", peer)

    def ring_wait(number, index):
        which, origin = {0: (0, left), 1: (1, left), 2: (1, right), 3: (0, right), 4: (0, far), 5: (1, far)}[index]
        ref = kvs.at[origin, which, pl.ds(tile_first(number), tile)]
        remote(ref, ref, zsend, zrecv, number * 6 + index, "sp", right).wait_recv()

    def forward(number):
        ring_wait(number, 0)
        ring_copy(number, 4).start()
        ring_wait(number, 2)
        ring_copy(number, 5).start()

    def direct(step):
        return remote(kvs.at[s], kvs.at[s], zsend, zrecv, step - 1, "sp", lax.rem(s + step, sp))

    even = lax.broadcasted_iota(jnp.int32, (tile, width), 1) % 2 == 0
    same = (
        lax.broadcasted_iota(jnp.int32, (width, width), 0) // head
        == lax.broadcasted_iota(jnp.int32, (width, width), 1) // head
    )
    ones = jnp.where(same, 1.0, 0.0).astype(BF16)
    by_row = (lax.broadcasted_iota(jnp.int32, (1, 2 * head), 1) % head) // 2 < head // 4
    grid_rows = cos.shape[0] - GRID_W
    part = min(tile, GRID_W)
    step_rows = 16

    def roll(v, by):
        if width % 128 == 0:
            return pltpu.roll(v, by % width, axis=1)
        return jnp.concatenate([v[:, width - by % width :], v[:, : width - by % width]], axis=1)

    def table(ref, first, is_ctx, fill):
        pieces = []
        for k in range(tile // part):
            at = jnp.where(is_ctx == 1, 0, first + k * part)
            row = ref[pl.ds(at // GRID_W, 1), :]
            col = ref[pl.ds(pl.multiple_of(grid_rows + at % GRID_W, 8), part), :]
            pieces.append(jnp.where(by_row, row, col))
        v = jnp.concatenate(pieces, axis=0) if len(pieces) > 1 else pieces[0]
        v = jnp.where(is_ctx == 1, fill, v)
        if width > v.shape[1]:
            return jnp.concatenate([v] * (width // v.shape[1]), axis=1)
        return v[:, :width]

    def one_tile(number, unused):
        @pl.when(number > 0)
        def _():
            gather.before(number - 1)

        is_ctx = jnp.where(number == 0, 1, 0)
        first = tile_first(number)
        base = first // rows

        def norm_rows(j, unused):
            slot = base + (j * step_rows) // rows
            row = pl.multiple_of((j * step_rows) % rows, step_rows)
            v = full[slot, pl.ds(row, step_rows), :].astype(F32)
            inv = lax.rsqrt(jnp.mean(v * v, axis=-1, keepdims=True) + EPS)
            out = v * inv * gsc[is_ctx] + shf[is_ctx]
            normed[pl.ds(pl.multiple_of(j * step_rows, step_rows), step_rows), :] = out.astype(BF16)
            return unused

        lax.fori_loop(0, tile // step_rows, norm_rows, 0)

        def turned(y, n):
            sq = y * y
            hi = sq.astype(BF16)
            lo = (sq - hi.astype(F32)).astype(BF16)
            mean = jnp.dot(hi, ones, preferred_element_type=F32) + jnp.dot(lo, ones, preferred_element_type=F32)
            u = y * lax.rsqrt(mean * (1.0 / head) + EPS) * gains[n]
            other = jnp.where(even, roll(u, -1), roll(u, 1))
            return (u * table(cos, first, is_ctx, 1.0) + other * table(sin, first, is_ctx, 0.0)).astype(BF16)

        def one_slot(m, unused):
            n = (m + groups) % slots
            y = jnp.dot(normed[...], wide[n], preferred_element_type=F32)

            @pl.when(m == 1)
            def _():
                kvs[s, 1, pl.ds(first, tile), :] = y.astype(BF16)
                if ring:
                    for index in (0, 2, 1, 3):
                        ring_copy(number, index).start()

            @pl.when(m == 0)
            def _():
                kvs[s, 0, pl.ds(first, tile), :] = turned(y, n)

            @pl.when(m > 1)
            def _():
                q_all[n, pl.ds(first, tile), :] = turned(y, n)

            return unused

        lax.fori_loop(0, jnp.where(number == 0, 2, slots), one_slot, 0)
        return unused

    lax.fori_loop(0, tiles, one_tile, 0)

    if not ring:
        for step in range(1, sp):
            direct(step).start()
    group = heads // kv_heads
    q_tile = min(256, lat_rows)
    q_tiles = lat_rows // q_tile

    def block(b, unused):
        if ring:
            @pl.when(b == 0)
            def _():
                for number in range(tiles - 2):
                    forward(number)

            @pl.when(b == 1)
            def _():
                forward(tiles - 1)
                for number in range(tiles):
                    ring_wait(number, 1)

            @pl.when(b == 2)
            def _():
                for number in range(tiles):
                    ring_wait(number, 3)

            @pl.when(b == 3)
            def _():
                for number in range(tiles):
                    ring_wait(number, 4)
                    ring_wait(number, 5)

            origin = (s + jnp.where(b == 1, sp - 1, jnp.where(b == 2, 1, jnp.where(b == 3, 2, 0)))) % sp
        else:
            @pl.when(b == 1)
            def _():
                for step in range(1, sp):
                    source = lax.rem(s - step + sp, sp)
                    remote(kvs.at[source], kvs.at[source], zsend, zrecv, step - 1, "sp", source).wait_recv()

            origin = (s + b) % sp

        def q_rows(t, unused):
            if ring:
                @pl.when((b == 0) & (t == q_tiles - 1))
                def _():
                    forward(tiles - 2)

            at = pl.ds(pl.multiple_of(t * q_tile, q_tile), q_tile)
            for h in range(kv_heads):
                k = kvs[origin, 0, :, h * head : (h + 1) * head]
                v = kvs[origin, 1, :, h * head : (h + 1) * head]
                v_wide = jnp.concatenate([v, jnp.ones((keys, head), BF16)], axis=1)
                for g in range(group):
                    n = h * group + g
                    slot, lane = (n * head) // width, (n * head) % width
                    q = q_all[slot, at, lane : lane + head]
                    scores = lax.dot_general(q, k, (((1,), (1,)), ((), ())), preferred_element_type=F32)
                    scores = jnp.concatenate([scores[:, :lat_rows], scores[:, lat_rows:] + lift[n]], axis=1)
                    before = top[n, at, :]
                    now = jnp.maximum(before, jnp.max(scores, axis=-1, keepdims=True))
                    expo = jnp.exp(scores - now)
                    keep = jnp.exp(before - now)
                    top[n, at, :] = now
                    acc[n, at, :] = acc[n, at, :] * keep + jnp.dot(expo.astype(BF16), v_wide, preferred_element_type=F32)
            return unused

        lax.fori_loop(0, q_tiles, q_rows, 0)
        return unused

    lax.fori_loop(0, sp, block, 0)

    def close(t, unused):
        at = pl.ds(pl.multiple_of(t * q_tile, q_tile), q_tile)
        for pair in range(heads // 2):
            two = [acc[2 * pair + n, at, :] for n in range(2)]
            two = [v[:, :head] / v[:, head:] for v in two]
            attended[at, pair * 2 * head : (pair + 1) * 2 * head] = jnp.concatenate(two, axis=1).astype(BF16)
        return unused

    lax.fori_loop(0, q_tiles, close, 0)
    if ring:
        for number in range(tiles):
            for index in range(6):
                ring_copy(number, index).wait_send()
    else:
        for step in range(1, sp):
            direct(step).wait_send()
    for item in sends + outs:
        item.wait_send()
    gather.finish()


def back_kernel(tp, att, weight, out, full, wide, total, mixed, landed, send, recv, asend, arecv, local):
    f = lax.axis_index("tp")
    rows, cols = att.shape
    own_rows = out.shape[0]
    out_cols = weight.shape[1]
    load = pltpu.make_async_copy(weight, wide, local.at[0])
    load.start()
    mine = pltpu.make_async_copy(att, full.at[f], local.at[1])
    mine.start()
    greet(others("tp", tp))
    gather = Gather(tp, att, full, send, recv)
    gather.start()
    gather.second()
    total[...] = jnp.zeros(total.shape, F32)
    gather.relay()
    mine.wait()
    load.wait()
    r_tile = min(256, rows)

    def chip_step(index, unused):
        gather.before(index)
        chip = gather.chip(index)

        def row_step(t, unused):
            at = pl.ds(pl.multiple_of(t * r_tile, r_tile), r_tile)
            value = total[at, :]
            for n in range(2):
                source = chip * 2 + n
                depth = pl.ds(pl.multiple_of(source * cols, cols), cols)
                value = value + jnp.dot(full[source, at, :], wide[depth, :], preferred_element_type=F32)
            total[at, :] = value
            return unused

        lax.fori_loop(0, rows // r_tile, row_step, 0)
        return unused

    lax.fori_loop(0, tp // 2, chip_step, 0)
    for peer in range(tp):
        mixed[peer] = total[peer * own_rows : (peer + 1) * own_rows, :].astype(BF16)
    sends = []
    for step in range(1, tp):
        peer = lax.rem(f + step, tp)
        sends.append(remote(mixed.at[peer], landed.at[f], asend, arecv, step - 1, "tp", peer))
    for item in sends:
        item.start()
    landed[f] = mixed[f]
    for step in range(1, tp):
        origin = lax.rem(f - step + tp, tp)
        remote(landed.at[origin], landed.at[origin], asend, arecv, step - 1, "tp", origin).wait_recv()
    for n in range(tp):
        out[:, n * out_cols : (n + 1) * out_cols] = landed[n]
    for item in sends:
        item.wait_send()
    gather.finish()


def tables(first, count, head):
    freqs = head // 4
    lane = jnp.arange(2 * head, dtype=jnp.int32) % head
    inverse = 10000.0 ** (-(lane // 2 % freqs).astype(F32) / freqs)
    sign = jnp.where(lane % 2 == 0, -1.0, 1.0)
    grid_rows = -(-(count // GRID_W) // 8) * 8
    index = jnp.arange(grid_rows + GRID_W, dtype=jnp.int32)
    spot = jnp.where(index < grid_rows, index + first // GRID_W, index - grid_rows)
    angles = spot.astype(F32)[:, None] * inverse
    return jnp.cos(angles), jnp.sin(angles) * sign


def local(sp, tp, latent, context, condition, context_cond, mod_weight, norm_gain, query_weight, key_weight,
          value_weight, out_weight, query_gain, key_gain, context_lift):
    rows, model = latent.shape
    ctx_rows = context.shape[0]
    head = query_gain.shape[0]
    heads = query_weight.shape[1] // head
    kv_heads = key_weight.shape[1] // head
    width = key_weight.shape[1]
    slots = query_weight.shape[1] // width + 2
    block = rows * tp
    keys = block + ctx_rows
    limit = 60 * 1024 * 1024
    cond_pair = jax.nn.silu(jnp.stack([condition, context_cond])).astype(BF16)
    mcols = mod_weight.shape[1]
    cos, sin = tables(lax.axis_index("sp") * block, block, head)
    stacked = width % 128 != 0
    weights = [query_weight, key_weight, value_weight]
    if stacked:
        weights = [jnp.stack([query_weight[:, n * width : (n + 1) * width] for n in range(slots - 2)] + weights[1:])]
    dma = pltpu.SemaphoreType.DMA
    count = gather_sems(tp)
    pieces = (tp // 2 + 1) * 6 if sp == 4 else sp - 1
    attended, gate = pl.pallas_call(
        functools.partial(front_kernel, sp, tp, heads, kv_heads, head, stacked),
        name="front",
        out_shape=(jax.ShapeDtypeStruct((block, heads * head), BF16), jax.ShapeDtypeStruct((1, model), F32)),
        in_specs=[ANY, ANY, VMEM, ANY, VMEM, VMEM, VMEM, VMEM, VMEM, SMEM] + [ANY] * len(weights),
        out_specs=(VMEM, VMEM),
        scratch_shapes=[
            pltpu.VMEM((tp + 2, rows, model), BF16),
            pltpu.VMEM((2 * rows, model), BF16),
            pltpu.VMEM((slots, model, width), BF16),
            pltpu.VMEM(mod_weight.shape, BF16),
            pltpu.VMEM((sp, 2, mcols), F32),
            pltpu.VMEM((2, mcols), F32),
            pltpu.VMEM((2, mcols), F32),
            pltpu.VMEM((2, mcols * tp), F32),
            pltpu.VMEM((2, 1, model), F32),
            pltpu.VMEM((2, 1, model), F32),
            pltpu.VMEM((slots, 1, width), F32),
            pltpu.VMEM((slots - 2, block, width), BF16),
            pltpu.VMEM((sp, 2, keys, width), BF16),
            pltpu.VMEM((heads, block, 1), F32),
            pltpu.VMEM((heads, block, 2 * head), F32),
            dma((count,)), dma((count,)), dma((sp - 1,)), dma((sp - 1,)), dma((tp - 1,)), dma((tp - 1,)),
            dma((pieces,)), dma((pieces,)),
            dma((slots + 4,)),
        ],
        compiler_params=pltpu.CompilerParams(collective_id=0, has_side_effects=True, vmem_limit_bytes=limit),
    )(latent, context, cond_pair, mod_weight, norm_gain.reshape(1, model), cos, sin, query_gain.reshape(1, head),
      key_gain.reshape(1, head), context_lift, *weights)
    mixed = pl.pallas_call(
        functools.partial(back_kernel, tp),
        name="back",
        out_shape=jax.ShapeDtypeStruct((rows, model), BF16),
        in_specs=[VMEM, ANY],
        out_specs=VMEM,
        scratch_shapes=[
            pltpu.VMEM((tp, block, heads * head), BF16),
            pltpu.VMEM(out_weight.shape, BF16),
            pltpu.VMEM((block, out_weight.shape[1]), F32),
            pltpu.VMEM((tp, rows, out_weight.shape[1]), BF16),
            pltpu.VMEM((tp, rows, out_weight.shape[1]), BF16),
            dma((count,)), dma((count,)), dma((tp - 1,)), dma((tp - 1,)), dma((2,)),
        ],
        compiler_params=pltpu.CompilerParams(collective_id=2, has_side_effects=True, vmem_limit_bytes=limit),
    )(attended, out_weight)
    return (latent.astype(F32) + gate * mixed.astype(F32)).astype(BF16)


def partner(s, order):
    return jnp.where(order == 0, s, jnp.where(order == 1, 3 - s, jnp.where(order == 2, (s + 2) % 4, s + 1 - 2 * (s % 2))))


class Square:
    def __init__(self, own, full, send, recv, base):
        self.own, self.full, self.send, self.recv, self.base = own, full, send, recv, base
        me = lax.axis_index("tp")
        self.me = me
        self.half = own.shape[0] // 2
        core, x, y = me % 2, (me // 2) % 2, me // 4
        self.sib = me + 1 - 2 * core
        self.step = 1 - 2 * core
        self.xn = me + 2 - 4 * x
        self.yn = me + 4 - 8 * y
        self.dn = self.xn + 4 - 8 * y

    def part(self, ref, which):
        return ref if which is None else ref.at[pl.ds(which * self.half, self.half)]

    def copy(self, index):
        me, xn, yn, dn, sib = self.me, self.xn, self.yn, self.dn, self.sib
        origin, half, peer = {
            0: (me, 0, xn), 1: (me, 1, xn), 2: (me, 0, yn), 3: (me, 1, yn), 4: (me, None, sib),
            5: (xn, 1, yn), 6: (yn, 0, xn),
            7: (xn, 0, sib), 8: (xn, 1, sib), 9: (yn, 0, sib), 10: (yn, 1, sib),
            11: (dn, 0, sib), 12: (dn, 1, sib),
        }[index]
        source = self.own if index < 5 else self.full.at[origin]
        return remote(self.part(source, half), self.part(self.full.at[origin], half), self.send, self.recv,
                      self.base + index, "tp", peer)

    def start(self, *indices):
        for index in indices:
            self.copy(index).start()

    def arrived(self, *indices):
        xn, yn, dn, sib, step = self.xn, self.yn, self.dn, self.sib, self.step
        for index in indices:
            origin, half = {
                0: (xn, 0), 1: (xn, 1), 2: (yn, 0), 3: (yn, 1), 4: (sib, None), 5: (dn, 1), 6: (dn, 0),
                7: (xn + step, 0), 8: (xn + step, 1), 9: (yn + step, 0), 10: (yn + step, 1),
                11: (dn + step, 0), 12: (dn + step, 1),
            }[index]
            ref = self.part(self.full.at[origin], half)
            remote(ref, ref, self.send, self.recv, self.base + index, "tp", sib).wait_recv()

    def finish(self):
        for index in range(13):
            self.copy(index).wait_send()


def whole_kernel(head, lat, ctx, cond, ctx_cond, mod_weight, gain, cos_in, sin_in, q_gain, k_gain, lift, wq, wk, wv, wo_in, out,
                 full, normed, wide, mod_wide, wo, parts, partial, total_mod, mod, gsc, shf, gains, cos, sin,
                 kv_out, kv_in, v_ones, q_out, q_in, o_out, att, total, mixed, landed, result,
                 send, recv, psend, precv, msend, mrecv, ksend, krecv, qsend, qrecv, osend, orecv, asend, arecv,
                 bsend, brecv, local):
    sp, tp = 4, 8
    s, f = lax.axis_index("sp"), lax.axis_index("tp")
    rows, model = lat.shape
    tile = 2 * rows
    block = rows * tp
    ctx_rows = ctx.shape[0]
    mcols = partial.shape[1]
    half_rows = rows // 2
    width = wk.shape[1]
    pack = 2 * head
    chunk = block // 2
    scale = head ** -0.5

    mod_in = pltpu.make_async_copy(mod_weight, mod_wide, local.at[0])
    mod_in.start()
    barrier = pltpu.get_barrier_semaphore()
    peers = others("tp", tp) + others("sp", sp)
    for axis, peer in peers:
        pl.semaphore_signal(barrier, inc=1, device_id={axis: peer}, device_id_type=MESH)
    ctx_in = [pltpu.make_async_copy(ctx.at[pl.ds(n * rows, rows)], full.at[tp + n], local.at[1 + n]) for n in range(2)]
    own = pltpu.make_async_copy(lat, full.at[f], local.at[3])
    weights = [
        pltpu.make_async_copy(wk, wide.at[0, :, pl.ds(0, width)], local.at[4]),
        pltpu.make_async_copy(wv, wide.at[0, :, pl.ds(width, width)], local.at[5]),
        pltpu.make_async_copy(wq, wide.at[1], local.at[6]),
    ]
    tabs = [pltpu.make_async_copy(cos_in, cos, local.at[7]), pltpu.make_async_copy(sin_in, sin, local.at[8])]
    out_w = [pltpu.make_async_copy(wo_in.at[:, n], wo.at[n], local.at[9 + n]) for n in range(sp)]
    pl.semaphore_wait(barrier, len(peers))
    gather = Square(lat, full, send, recv, 0)
    gather.start(1, 2, 4)
    for item in ctx_in + [own] + weights + tabs + out_w:
        item.start()
    pair = jnp.concatenate([cond[...], ctx_cond[...]], axis=0)
    pair = (pair / (1.0 + jnp.exp(-pair))).astype(BF16)
    mod_in.wait()
    first_sum = jnp.dot(pair, mod_wide[...], preferred_element_type=F32)
    partial[...] = first_sum
    parts[s] = first_sum
    sends = [remote(partial, parts.at[s], psend, precv, n - 1, "sp", partner(s, n)) for n in range(1, sp)]
    for item in sends:
        item.start()
    gains[0] = jnp.concatenate([k_gain[...]] * (width // head), axis=1)
    gains[1] = jnp.concatenate([q_gain[...] * scale] * (width // head), axis=1)
    total[...] = jnp.zeros(total.shape, F32)
    for n in range(1, sp):
        origin = partner(s, n)
        remote(parts.at[origin], parts.at[origin], psend, precv, n - 1, "sp", origin).wait_recv()
    summed = parts[0] + parts[1] + parts[2] + parts[3]
    total_mod[...] = summed
    here = pl.ds(pl.multiple_of(f * mcols, mcols), mcols)
    mod[:, here] = summed
    outs = [remote(total_mod, mod.at[:, here], msend, mrecv, step - 1, "tp", lax.rem(f + step, tp)) for step in range(1, tp)]
    for item in outs:
        item.start()
    gather.start(0, 3)
    for step in range(1, tp):
        origin = lax.rem(f - step + tp, tp)
        ref = mod.at[:, pl.ds(pl.multiple_of(origin * mcols, mcols), mcols)]
        remote(ref, ref, msend, mrecv, step - 1, "tp", origin).wait_recv()
    for r in range(2):
        gsc[r] = gain[...] * (1.0 + mod[r : r + 1, model : 2 * model])
        shf[r] = mod[r : r + 1, :model]
    gather.arrived(1)
    gather.start(5, 8)
    gather.arrived(2)
    gather.start(6, 9)
    for item in ctx_in + [own] + weights + tabs:
        item.wait()

    even = lax.broadcasted_iota(jnp.int32, (tile, width), 1) % 2 == 0
    same = (
        lax.broadcasted_iota(jnp.int32, (width, width), 0) // head
        == lax.broadcasted_iota(jnp.int32, (width, width), 1) // head
    )
    ones = jnp.where(same, 1.0, 0.0).astype(BF16)
    by_row = (lax.broadcasted_iota(jnp.int32, (1, pack), 1) % head) // 2 < head // 4
    low = lax.broadcasted_iota(jnp.int32, (tile, pack), 1) < head
    grid_rows = cos.shape[0] - GRID_W
    step_rows, wide_step = 16, 512
    steps = half_rows // step_rows

    def chip_at(index):
        x, y = (f // 2) % 2, f // 4
        return ((y + index // 2) % 2) * 2 + (x + index) % 2

    def kv_send(number, n):
        chip = chip_at(jnp.maximum(number - 1, 0))
        at_out = pl.multiple_of(jnp.where(number == 0, block, chip * tile), tile)
        at_in = pl.multiple_of(jnp.where(number == 0, sp * block + s * ctx_rows, s * block + chip * tile), tile)
        peer = partner(s, n)
        return remote(kv_out.at[peer, pl.ds(at_out, tile)], kv_in.at[pl.ds(at_in, tile)], ksend, krecv,
                      number * 3 + n - 1, "sp", peer)

    def kv_wait(number, n):
        chip = chip_at(jnp.maximum(number - 1, 0))
        origin = partner(s, n)
        at_in = pl.multiple_of(jnp.where(number == 0, sp * block + origin * ctx_rows, origin * block + chip * tile), tile)
        ref = kv_in.at[pl.ds(at_in, tile)]
        remote(ref, ref, ksend, krecv, number * 3 + n - 1, "sp", origin).wait_recv()

    def one_tile(number, unused):
        @pl.when(number == 1)
        def _():
            gather.arrived(4)

        @pl.when(number == 2)
        def _():
            gather.arrived(0)
            gather.start(7)
            gather.arrived(3)
            gather.start(10)
            gather.arrived(7, 8)

        @pl.when(number == 3)
        def _():
            gather.arrived(9, 10)

        @pl.when(number == 4)
        def _():
            gather.arrived(5)
            gather.start(12)
            gather.arrived(6)
            gather.start(11)
            gather.arrived(12, 11)

        is_ctx = jnp.where(number == 0, 1, 0)
        chip = chip_at(jnp.maximum(number - 1, 0))
        base = jnp.where(number == 0, tp, chip * 2)

        def norm_rows(j, unused):
            slot = base + (j // steps) % 2
            row = pl.multiple_of((j // (2 * steps)) * half_rows + (j % steps) * step_rows, step_rows)
            there = pl.ds(pl.multiple_of(j * step_rows, step_rows), step_rows)
            squares = jnp.zeros((step_rows, 128), F32)
            for n in range(model // wide_step):
                v = full[slot, pl.ds(row, step_rows), n * wide_step : (n + 1) * wide_step].astype(F32)
                v = v * v
                for m in range(wide_step // 128):
                    squares = squares + v[:, m * 128 : (m + 1) * 128]
            inv = lax.rsqrt(jnp.sum(squares, axis=-1, keepdims=True) * (1.0 / model) + EPS)
            for n in range(model // wide_step):
                cols = slice(n * wide_step, (n + 1) * wide_step)
                v = full[slot, pl.ds(row, step_rows), cols].astype(F32)
                normed[there, cols] = (v * inv * gsc[is_ctx, :, cols] + shf[is_ctx, :, cols]).astype(BF16)
            return unused

        lax.fori_loop(0, tile // step_rows, norm_rows, 0, unroll=4)

        def table(ref, fill):
            pieces = []
            for c in range(2):
                for owner in range(2):
                    row = ref[pl.ds(s * tp + chip * 2 + owner, 1), :]
                    col = ref[grid_rows + c * half_rows : grid_rows + (c + 1) * half_rows, :]
                    pieces.append(jnp.where(by_row, row, col))
            v = jnp.concatenate(pieces, axis=0)
            v = jnp.where(is_ctx == 1, fill, v)
            return jnp.concatenate([v] * (width // pack), axis=1)

        cos_t, sin_t = table(cos, 1.0), table(sin, 0.0)

        def turned(y, row):
            sq = y * y
            hi = sq.astype(BF16)
            lo = (sq - hi.astype(F32)).astype(BF16)
            mean = jnp.dot(hi, ones, preferred_element_type=F32) + jnp.dot(lo, ones, preferred_element_type=F32)
            u = y * lax.rsqrt(mean * (1.0 / head) + EPS) * row
            other = jnp.where(even, pltpu.roll(u, width - 1, axis=1), pltpu.roll(u, 1, axis=1))
            return u * cos_t + other * sin_t

        y = jnp.dot(normed[...], wide[0], preferred_element_type=F32)
        k, v = turned(y[:, :width], gains[0]), y[:, width:]
        at_out = pl.ds(pl.multiple_of(jnp.where(number == 0, block, chip * tile), tile), tile)
        at_in = pl.ds(pl.multiple_of(jnp.where(number == 0, sp * block + s * ctx_rows, s * block + chip * tile), tile), tile)
        for n in range(width // pack):
            kc, vc = k[:, n * pack : (n + 1) * pack], v[:, n * pack : (n + 1) * pack]
            kv_out[2 * n, at_out, :] = jnp.where(low, kc, pltpu.roll(vc, head, axis=1)).astype(BF16)
            kv_out[2 * n + 1, at_out, :] = jnp.where(low, pltpu.roll(kc, head, axis=1), vc).astype(BF16)
        for n in range(1, sp):
            kv_send(number, n).start()
        kv_in[at_in, :] = kv_out[s, at_out, :]

        @pl.when(number > 0)
        def _():
            y = jnp.dot(normed[...], wide[1], preferred_element_type=F32)
            for n in range(2):
                q = turned(y[:, n * width : (n + 1) * width], gains[1]).astype(BF16)
                for m in range(2):
                    for c in range(2):
                        q_out[2 * n + m, c, pl.ds(pl.multiple_of(chip * rows, rows), rows), :] = (
                            q[c * rows : (c + 1) * rows, m * pack : (m + 1) * pack])

        return unused

    lax.fori_loop(0, tp // 2 + 1, one_tile, 0)

    def q_send(n, c):
        peer = partner(s, n)
        return remote(q_out.at[peer, c], q_in.at[n, c], qsend, qrecv, (n - 1) * 2 + c, "sp", peer)

    for c in range(2):
        for n in range(1, sp):
            q_send(n, c).start()
    q_in[0] = q_out[s]

    def wait_kv(number, unused):
        for n in range(1, sp):
            kv_wait(number, n)
        return unused

    lax.fori_loop(0, tp // 2 + 1, wait_kv, 0)
    keys = kv_in.shape[0]
    v_ones[...] = jnp.concatenate([kv_in[:, head:], jnp.ones((keys, head), BF16)], axis=1)
    for item in out_w:
        item.wait()
    lat_keys = sp * block
    pieces = 2 * sp
    lag = 2

    def step_at(p):
        if isinstance(p, int):
            return (0 if p == pieces - 1 else p if p < sp else p - sp + 1), (0 if p < sp else 1)
        return jnp.where(p == pieces - 1, 0, jnp.where(p < sp, p, p - sp + 1)), jnp.where(p < sp, 0, 1)

    def o_send(order, c):
        return remote(o_out.at[order - 1, c], att.at[order, c, f], osend, orecv, (order - 1) * 2 + c, "sp", partner(s, order))

    def piece_of(p):
        order, c = step_at(p)
        return Square(att.at[order, c, f], att.at[order, c], asend, arecv, p * 13)

    def back_send(c, step):
        peer = lax.rem(f + step, tp)
        return remote(mixed.at[c, peer], landed.at[c, f], bsend, brecv, c * (tp - 1) + step - 1, "tp", peer)

    def stage_zero(p):
        order, c = step_at(p)

        def arrive():
            ref = att.at[order, c, f]
            remote(ref, ref, osend, orecv, (order - 1) * 2 + c, "sp", partner(s, order)).wait_recv()

        if isinstance(p, int):
            if order > 0:
                arrive()
        else:
            pl.when(order > 0)(arrive)
        piece_of(p).start(1, 2, 4, 0, 3)

    def stage_one(p):
        piece = piece_of(p)
        piece.arrived(1)
        piece.start(5, 8)
        piece.arrived(2)
        piece.start(6, 9)
        piece.arrived(0)
        piece.start(7)
        piece.arrived(3)
        piece.start(10)

    def stage_two(p):
        piece = piece_of(p)
        piece.arrived(5)
        piece.start(12)
        piece.arrived(6)
        piece.start(11)

    def stage_three(p):
        piece_of(p).arrived(4, 7, 8, 9, 10, 11, 12)
        order, c = step_at(p)
        left = jnp.concatenate([att[order, c, n] for n in range(tp)], axis=1)
        total[c] += jnp.dot(left, wo[partner(s, order)].reshape(tp * pack, wo.shape[3]), preferred_element_type=F32)

    def back(c):
        for n in range(tp):
            mixed[c, n] = total[c, n * half_rows : (n + 1) * half_rows, :].astype(BF16)
        for step in range(1, tp):
            back_send(c, step).start()
        landed[c, f] = mixed[c, f]

    def one_step(i, unused):
        order, c = step_at(i)

        @pl.when(order > 0)
        def _():
            ref = q_in.at[order, c]
            remote(ref, ref, qsend, qrecv, (order - 1) * 2 + c, "sp", partner(s, order)).wait_recv()

        results = []
        for g in range(2):
            q = q_in[order, c, :, g * head : (g + 1) * head]
            scores = lax.dot_general(q, kv_in[:, :head], (((1,), (1,)), ((), ())), preferred_element_type=F32)
            scores = jnp.concatenate([scores[:, :lat_keys], scores[:, lat_keys:] + lift[2 * s + g]], axis=1)
            peak = jnp.max(scores, axis=-1, keepdims=True)
            expo = jnp.exp(scores - peak).astype(BF16)
            acc = jnp.dot(expo, v_ones[...], preferred_element_type=F32)
            results.append(acc[:, :head] / acc[:, head:])
        value = jnp.concatenate(results, axis=1).astype(BF16)

        @pl.when(order == 0)
        def _():
            att[0, c, f] = value

        @pl.when(order > 0)
        def _():
            o_out[order - 1, c] = value
            o_send(order, c).start()

        for delay, stage in enumerate((stage_zero, stage_one, stage_two, stage_three)):
            p = i - lag - delay
            pl.when(p >= 0)(functools.partial(stage, p))
        return unused

    lax.fori_loop(0, pieces, one_step, 0)
    stage_zero(7)
    stage_three(3)
    back(0)
    stage_two(4)
    stage_one(5)
    stage_zero(6)
    stage_one(7)
    stage_three(4)
    stage_two(5)
    stage_one(6)
    stage_two(7)
    stage_three(5)
    stage_two(6)
    stage_three(7)
    stage_three(6)
    back(1)
    cols = wo.shape[3]
    writes = []
    for c in range(2):
        for step in range(1, tp):
            origin = lax.rem(f - step + tp, tp)
            ref = landed.at[c, origin]
            remote(ref, ref, bsend, brecv, c * (tp - 1) + step - 1, "tp", origin).wait_recv()
        at = slice(c * half_rows, (c + 1) * half_rows)
        for n in range(tp):
            there = slice(n * cols, (n + 1) * cols)
            gate = mod[0:1, 2 * model + n * cols : 2 * model + (n + 1) * cols]
            result[at, there] = (full[f, at, there].astype(F32) + gate * landed[c, n].astype(F32)).astype(BF16)
        writes.append(pltpu.make_async_copy(result.at[pl.ds(c * half_rows, half_rows)], out.at[pl.ds(c * half_rows, half_rows)],
                                            local.at[9 + sp + c]))
        writes[-1].start()
    for item in sends + outs:
        item.wait_send()
    gather.finish()

    def drain_kv(number, unused):
        for n in range(1, sp):
            kv_send(number, n).wait_send()
        return unused

    lax.fori_loop(0, tp // 2 + 1, drain_kv, 0)
    for n in range(1, sp):
        for c in range(2):
            q_send(n, c).wait_send()
            o_send(n, c).wait_send()

    def drain_pieces(p, unused):
        piece_of(p).finish()
        return unused

    lax.fori_loop(0, pieces, drain_pieces, 0)
    for c in range(2):
        for step in range(1, tp):
            back_send(c, step).wait_send()
    for item in writes:
        item.wait()


def all_tables(count, head):
    freqs = head // 4
    lane = np.arange(2 * head) % head
    inverse = (10000.0 ** (-(lane // 2 % freqs).astype(np.float32) / freqs)).astype(np.float32)
    sign = np.where(lane % 2 == 0, -1.0, 1.0).astype(np.float32)
    spot = np.concatenate([np.arange(count // GRID_W), np.arange(GRID_W)]).astype(np.float32)
    angles = (spot[:, None] * inverse).astype(np.float32)
    return np.cos(angles).astype(np.float32), (np.sin(angles) * sign).astype(np.float32)


def whole(sp, tp, latent, context, condition, context_cond, mod_weight, norm_gain, query_weight, key_weight,
          value_weight, out_weight, query_gain, key_gain, context_lift):
    rows, model = latent.shape
    head = query_gain.shape[0]
    block = rows * tp
    ctx_rows = context.shape[0]
    width = key_weight.shape[1]
    mcols = mod_weight.shape[1]
    out_cols = out_weight.shape[1]
    pack = 2 * head
    chunk = block // 2
    keys = sp * (block + ctx_rows)
    cos, sin = all_tables(sp * block, head)
    dma = lambda *shape: pltpu.SemaphoreType.DMA(shape)
    vm = pltpu.VMEM
    tiles = tp // 2 + 1
    return pl.pallas_call(
        functools.partial(whole_kernel, head),
        name="whole",
        out_shape=jax.ShapeDtypeStruct((rows, model), BF16),
        in_specs=[ANY, ANY, VMEM, VMEM, ANY, VMEM, ANY, ANY, VMEM, VMEM, SMEM, ANY, ANY, ANY, ANY],
        out_specs=ANY,
        scratch_shapes=[
            vm((tp + 2, rows, model), BF16),
            vm((2 * rows, model), BF16),
            vm((2, model, 2 * width), BF16),
            vm(mod_weight.shape, BF16),
            vm((sp, tp, pack, out_cols), BF16),
            vm((sp, 2, mcols), F32),
            vm((2, mcols), F32),
            vm((2, mcols), F32),
            vm((2, mcols * tp), F32),
            vm((2, 1, model), F32),
            vm((2, 1, model), F32),
            vm((2, 1, width), F32),
            vm(cos.shape, F32),
            vm(sin.shape, F32),
            vm((sp, block + ctx_rows, pack), BF16),
            vm((keys, pack), BF16),
            vm((keys, pack), BF16),
            vm((sp, 2, chunk, pack), BF16),
            vm((sp, 2, chunk, pack), BF16),
            vm((sp - 1, 2, chunk, pack), BF16),
            vm((sp, 2, tp, chunk, pack), BF16),
            vm((2, chunk, out_cols), F32),
            vm((2, tp, rows // 2, out_cols), BF16),
            vm((2, tp, rows // 2, out_cols), BF16),
            vm((rows, model), BF16),
            dma(13), dma(13), dma(sp - 1), dma(sp - 1), dma(tp - 1), dma(tp - 1),
            dma(tiles * 3), dma(tiles * 3), dma(6), dma(6), dma(6), dma(6),
            dma(13 * 8), dma(13 * 8), dma(2 * (tp - 1)), dma(2 * (tp - 1)),
            dma(9 + sp + 2),
        ],
        compiler_params=pltpu.CompilerParams(collective_id=1, has_side_effects=True, vmem_limit_bytes=62 * 1024 * 1024),
    )(latent, context, condition.reshape(1, -1), context_cond.reshape(1, -1), mod_weight, norm_gain.reshape(1, model),
      cos, sin, query_gain.reshape(1, head), key_gain.reshape(1, head), context_lift, query_weight, key_weight,
      value_weight, out_weight.reshape(tp, sp, pack, out_cols))


def fits(sp, tp, latent, context, key_weight, query_weight, query_gain):
    head = query_gain.shape[0]
    return (
        sp == 4 and tp == 8 and latent.shape[0] == GRID_W and context.shape[0] == 2 * latent.shape[0]
        and 2 * head == 128 and key_weight.shape[1] == sp * head and query_weight.shape[1] == 2 * sp * head
    )


def chosen(sp, tp, *args):
    latent, context, query_weight, key_weight, query_gain = args[0], args[1], args[6], args[7], args[10]
    if fits(sp, tp, latent, context, key_weight, query_weight, query_gain):
        return whole(sp, tp, *args)
    return local(sp, tp, *args)


def solution(mesh):
    return jax.shard_map(
        functools.partial(chosen, mesh.shape["sp"], mesh.shape["tp"]),
        mesh=mesh,
        in_specs=(
            P(("sp", "tp"), None),
            P("sp", None),
            P("sp"),
            P("sp"),
            P("sp", "tp"),
            P(),
            P(None, "tp"),
            P(None, "tp"),
            P(None, "tp"),
            P(None, "tp"),
            P(),
            P(),
            P("tp"),
        ),
        out_specs=P(("sp", "tp"), None),
        check_vma=False,
    )
```

```python
import functools

import jax
import jax.numpy as jnp
import numpy as np
from jax import lax
from jax.experimental import pallas as pl
from jax.experimental.pallas import tpu as pltpu
from jax.sharding import PartitionSpec as P

GRID_W = 64
EPS = 1e-06
MESH = pl.DeviceIdType.MESH
ANY = pl.BlockSpec(memory_space=pl.ANY)
VMEM = pl.BlockSpec(memory_space=pltpu.VMEM)
SMEM = pl.BlockSpec(memory_space=pltpu.SMEM)
BF16 = jnp.bfloat16
F32 = jnp.float32


def remote(src, dst, send, recv, index, axis, peer):
    return pltpu.make_async_remote_copy(
        src_ref=src, dst_ref=dst, send_sem=send.at[index], recv_sem=recv.at[index],
        device_id={axis: peer}, device_id_type=MESH,
    )


def greet(peers):
    barrier = pltpu.get_barrier_semaphore()
    for axis, peer in peers:
        pl.semaphore_signal(barrier, inc=1, device_id={axis: peer}, device_id_type=MESH)
    pl.semaphore_wait(barrier, len(peers))


def others(axis, count):
    me = lax.axis_index(axis)
    return [(axis, lax.rem(me + step, count)) for step in range(1, count)]


def gather_sems(count):
    return 13 if count == 8 else max(count - 1, 1)


class Gather:
    def __init__(self, count, own, full, send, recv):
        self.count, self.own, self.full, self.send, self.recv = count, own, full, send, recv
        self.me = lax.axis_index("tp")
        self.half = own.shape[0] // 2
        me = self.me
        if count == 8:
            self.core, self.x, self.y = me % 2, (me // 2) % 2, me // 4
            self.sib = me + 1 - 2 * self.core
            self.step = 1 - 2 * self.core
            self.xn = me + 2 - 4 * self.x
            self.yn = me + 4 - 8 * self.y
            self.dn = self.xn + 4 - 8 * self.y

    def part(self, ref, which):
        return ref if which is None else ref.at[pl.ds(which * self.half, self.half)]

    def copy(self, index):
        me, xn, yn, dn, sib = self.me, self.xn, self.yn, self.dn, self.sib
        origin, half, peer = {
            0: (me, 0, xn), 1: (me, 1, xn), 2: (me, 0, yn), 3: (me, 1, yn), 4: (me, None, sib),
            5: (xn, 1, yn), 6: (yn, 0, xn),
            7: (xn, 0, sib), 8: (xn, 1, sib), 9: (yn, 0, sib), 10: (yn, 1, sib),
            11: (dn, 0, sib), 12: (dn, 1, sib),
        }[index]
        source = self.own if index < 5 else self.full.at[origin]
        return remote(self.part(source, half), self.part(self.full.at[origin], half), self.send, self.recv, index, "tp", peer)

    def wait_recv(self, index):
        xn, yn, dn, sib, step = self.xn, self.yn, self.dn, self.sib, self.step
        origin, half = {
            0: (xn, 0), 1: (xn, 1), 2: (yn, 0), 3: (yn, 1), 4: (sib, None), 5: (dn, 1), 6: (dn, 0),
            7: (xn + step, 0), 8: (xn + step, 1), 9: (yn + step, 0), 10: (yn + step, 1),
            11: (dn + step, 0), 12: (dn + step, 1),
        }[index]
        ref = self.part(self.full.at[origin], half)
        remote(ref, ref, self.send, self.recv, index, "tp", sib).wait_recv()

    def direct(self, step):
        peer = lax.rem(self.me + step, self.count)
        return remote(self.own, self.full.at[self.me], self.send, self.recv, step - 1, "tp", peer)

    def start(self):
        if self.count == 8:
            for index in (1, 2, 4):
                self.copy(index).start()
        else:
            for step in range(1, self.count):
                self.direct(step).start()

    def second(self):
        if self.count == 8:
            for index in (0, 3):
                self.copy(index).start()

    def relay(self):
        if self.count == 8:
            for arrived, then in ((1, (5, 8)), (2, (6, 9))):
                self.wait_recv(arrived)
                for nxt in then:
                    self.copy(nxt).start()

    def before(self, index):
        if self.count != 8:
            @pl.when(index == 0)
            def _():
                for step in range(1, self.count):
                    origin = lax.rem(self.me - step + self.count, self.count)
                    ref = self.full.at[origin]
                    remote(ref, ref, self.send, self.recv, step - 1, "tp", origin).wait_recv()
            return

        @pl.when(index == 0)
        def _():
            self.wait_recv(4)

        @pl.when(index == 1)
        def _():
            for arrived, nxt in ((0, 7), (3, 10)):
                self.wait_recv(arrived)
                self.copy(nxt).start()
            self.wait_recv(7)
            self.wait_recv(8)

        @pl.when(index == 2)
        def _():
            self.wait_recv(9)
            self.wait_recv(10)

        @pl.when(index == 3)
        def _():
            self.wait_recv(5)
            self.copy(12).start()
            self.wait_recv(6)
            self.copy(11).start()
            self.wait_recv(12)
            self.wait_recv(11)

    def chip(self, index):
        if self.count == 8:
            return ((self.y + index // 2) % 2) * 2 + (self.x + index) % 2
        return index

    def finish(self):
        if self.count == 8:
            for index in range(13):
                self.copy(index).wait_send()
        else:
            for step in range(1, self.count):
                self.direct(step).wait_send()


def front_kernel(sp, tp, heads, kv_heads, head, stacked, lat, ctx, cond, mod_weight, gain, cos, sin, q_gain, k_gain, lift, *rest):
    weights, rest = rest[: 1 if stacked else 3], rest[1 if stacked else 3 :]
    (attended, gate, full, normed, wide, mod_wide, parts, partial, total, mod, gsc, shf, gains, q_all, kvs, top, acc,
     send, recv, psend, precv, msend, mrecv, zsend, zrecv, local) = rest
    s, f = lax.axis_index("sp"), lax.axis_index("tp")
    rows, model = lat.shape
    width = wide.shape[2]
    slots = wide.shape[0]
    groups = slots - 2
    tile = 2 * rows
    lat_rows = rows * tp
    keys = kvs.shape[2]
    mcols = partial.shape[1]
    tiles = tp // 2 + 1
    scale = head ** -0.5
    mod_in = pltpu.make_async_copy(mod_weight, mod_wide, local.at[slots + 3])
    mod_in.start()
    copies = []
    if stacked:
        copies.append(pltpu.make_async_copy(weights[0], wide, local.at[0]))
    else:
        for n in range(groups):
            copies.append(pltpu.make_async_copy(weights[0].at[:, n * width : (n + 1) * width], wide.at[n], local.at[n]))
        copies.append(pltpu.make_async_copy(weights[1], wide.at[groups], local.at[groups]))
        copies.append(pltpu.make_async_copy(weights[2], wide.at[groups + 1], local.at[groups + 1]))
    own = pltpu.make_async_copy(lat, full.at[f], local.at[slots])
    ctx_in = [
        pltpu.make_async_copy(ctx.at[pl.ds(n * rows, rows)], full.at[tp + n], local.at[slots + 1 + n]) for n in range(2)
    ]
    greet(others("tp", tp) + others("sp", sp))
    gather = Gather(tp, lat, full, send, recv)
    gather.start()
    for item in ctx_in + [own] + copies[::-1]:
        item.start()
    mod_in.wait()
    first_sum = jnp.dot(cond[...], mod_wide[...], preferred_element_type=F32)
    partial[...] = first_sum
    parts[s] = first_sum
    sends = []
    for step in range(1, sp):
        sends.append(remote(partial, parts.at[s], psend, precv, step - 1, "sp", lax.rem(s + step, sp)))
    for item in sends:
        item.start()
    for n in range(slots):
        row = q_gain[...] * scale if n < groups else k_gain[...]
        gains[n] = jnp.concatenate([row] * (width // head), axis=1) if width > head else row
    for step in range(1, sp):
        origin = lax.rem(s - step + sp, sp)
        remote(parts.at[origin], parts.at[origin], psend, precv, step - 1, "sp", origin).wait_recv()
    summed = parts[0]
    for n in range(1, sp):
        summed = summed + parts[n]
    total[...] = summed
    here = pl.ds(pl.multiple_of(f * mcols, mcols), mcols)
    mod[:, here] = summed
    outs = []
    for step in range(1, tp):
        outs.append(remote(total, mod.at[:, here], msend, mrecv, step - 1, "tp", lax.rem(f + step, tp)))
    for item in outs:
        item.start()
    gather.second()
    top[...] = jnp.full(top.shape, -1e30, F32)
    acc[...] = jnp.zeros(acc.shape, F32)
    for step in range(1, tp):
        origin = lax.rem(f - step + tp, tp)
        ref = mod.at[:, pl.ds(pl.multiple_of(origin * mcols, mcols), mcols)]
        remote(ref, ref, msend, mrecv, step - 1, "tp", origin).wait_recv()
    for r in range(2):
        gsc[r] = gain[...] * (1.0 + mod[r : r + 1, model : 2 * model])
        shf[r] = mod[r : r + 1, :model]
    gate[...] = mod[0:1, 2 * model :]
    gather.relay()
    for item in ctx_in + copies:
        item.wait()
    own.wait()

    ring = sp == 4
    right, left, far = (s + 1) % sp, (s + sp - 1) % sp, (s + 2) % sp

    def tile_first(number):
        if isinstance(number, int):
            return lat_rows if number == 0 else pl.multiple_of(gather.chip(number - 1) * tile, tile)
        chip = jnp.where(number == 0, tp // 2, gather.chip(jnp.maximum(number - 1, 0)))
        return pl.multiple_of(chip * tile, tile)

    def ring_copy(number, index):
        which, origin, peer = {
            0: (0, s, right), 1: (1, s, right), 2: (1, s, left), 3: (0, s, left), 4: (0, left, right), 5: (1, right, left),
        }[index]
        ref = kvs.at[origin, which, pl.ds(tile_first(number), tile)]
        return remote(ref, ref, zsend, zrecv, number * 6 + index, "sp", peer)

    def ring_wait(number, index):
        which, origin = {0: (0, left), 1: (1, left), 2: (1, right), 3: (0, right), 4: (0, far), 5: (1, far)}[index]
        ref = kvs.at[origin, which, pl.ds(tile_first(number), tile)]
        remote(ref, ref, zsend, zrecv, number * 6 + index, "sp", right).wait_recv()

    def forward(number):
        ring_wait(number, 0)
        ring_copy(number, 4).start()
        ring_wait(number, 2)
        ring_copy(number, 5).start()

    def direct(step):
        return remote(kvs.at[s], kvs.at[s], zsend, zrecv, step - 1, "sp", lax.rem(s + step, sp))

    even = lax.broadcasted_iota(jnp.int32, (tile, width), 1) % 2 == 0
    same = (
        lax.broadcasted_iota(jnp.int32, (width, width), 0) // head
        == lax.broadcasted_iota(jnp.int32, (width, width), 1) // head
    )
    ones = jnp.where(same, 1.0, 0.0).astype(BF16)
    by_row = (lax.broadcasted_iota(jnp.int32, (1, 2 * head), 1) % head) // 2 < head // 4
    grid_rows = cos.shape[0] - GRID_W
    part = min(tile, GRID_W)
    step_rows = 16

    def roll(v, by):
        if width % 128 == 0:
            return pltpu.roll(v, by % width, axis=1)
        return jnp.concatenate([v[:, width - by % width :], v[:, : width - by % width]], axis=1)

    def table(ref, first, is_ctx, fill):
        pieces = []
        for k in range(tile // part):
            at = jnp.where(is_ctx == 1, 0, first + k * part)
            row = ref[pl.ds(at // GRID_W, 1), :]
            col = ref[pl.ds(pl.multiple_of(grid_rows + at % GRID_W, 8), part), :]
            pieces.append(jnp.where(by_row, row, col))
        v = jnp.concatenate(pieces, axis=0) if len(pieces) > 1 else pieces[0]
        v = jnp.where(is_ctx == 1, fill, v)
        if width > v.shape[1]:
            return jnp.concatenate([v] * (width // v.shape[1]), axis=1)
        return v[:, :width]

    def one_tile(number, unused):
        @pl.when(number > 0)
        def _():
            gather.before(number - 1)

        is_ctx = jnp.where(number == 0, 1, 0)
        first = tile_first(number)
        base = first // rows

        def norm_rows(j, unused):
            slot = base + (j * step_rows) // rows
            row = pl.multiple_of((j * step_rows) % rows, step_rows)
            v = full[slot, pl.ds(row, step_rows), :].astype(F32)
            inv = lax.rsqrt(jnp.mean(v * v, axis=-1, keepdims=True) + EPS)
            out = v * inv * gsc[is_ctx] + shf[is_ctx]
            normed[pl.ds(pl.multiple_of(j * step_rows, step_rows), step_rows), :] = out.astype(BF16)
            return unused

        lax.fori_loop(0, tile // step_rows, norm_rows, 0)

        def turned(y, n):
            sq = y * y
            hi = sq.astype(BF16)
            lo = (sq - hi.astype(F32)).astype(BF16)
            mean = jnp.dot(hi, ones, preferred_element_type=F32) + jnp.dot(lo, ones, preferred_element_type=F32)
            u = y * lax.rsqrt(mean * (1.0 / head) + EPS) * gains[n]
            other = jnp.where(even, roll(u, -1), roll(u, 1))
            return (u * table(cos, first, is_ctx, 1.0) + other * table(sin, first, is_ctx, 0.0)).astype(BF16)

        def one_slot(m, unused):
            n = (m + groups) % slots
            y = jnp.dot(normed[...], wide[n], preferred_element_type=F32)

            @pl.when(m == 1)
            def _():
                kvs[s, 1, pl.ds(first, tile), :] = y.astype(BF16)
                if ring:
                    for index in (0, 2, 1, 3):
                        ring_copy(number, index).start()

            @pl.when(m == 0)
            def _():
                kvs[s, 0, pl.ds(first, tile), :] = turned(y, n)

            @pl.when(m > 1)
            def _():
                q_all[n, pl.ds(first, tile), :] = turned(y, n)

            return unused

        lax.fori_loop(0, jnp.where(number == 0, 2, slots), one_slot, 0)
        return unused

    lax.fori_loop(0, tiles, one_tile, 0)

    if not ring:
        for step in range(1, sp):
            direct(step).start()
    group = heads // kv_heads
    q_tile = min(256, lat_rows)
    q_tiles = lat_rows // q_tile

    def block(b, unused):
        if ring:
            @pl.when(b == 0)
            def _():
                for number in range(tiles - 2):
                    forward(number)

            @pl.when(b == 1)
            def _():
                forward(tiles - 1)
                for number in range(tiles):
                    ring_wait(number, 1)

            @pl.when(b == 2)
            def _():
                for number in range(tiles):
                    ring_wait(number, 3)

            @pl.when(b == 3)
            def _():
                for number in range(tiles):
                    ring_wait(number, 4)
                    ring_wait(number, 5)

            origin = (s + jnp.where(b == 1, sp - 1, jnp.where(b == 2, 1, jnp.where(b == 3, 2, 0)))) % sp
        else:
            @pl.when(b == 1)
            def _():
                for step in range(1, sp):
                    source = lax.rem(s - step + sp, sp)
                    remote(kvs.at[source], kvs.at[source], zsend, zrecv, step - 1, "sp", source).wait_recv()

            origin = (s + b) % sp

        def q_rows(t, unused):
            if ring:
                @pl.when((b == 0) & (t == q_tiles - 1))
                def _():
                    forward(tiles - 2)

            at = pl.ds(pl.multiple_of(t * q_tile, q_tile), q_tile)
            for h in range(kv_heads):
                k = kvs[origin, 0, :, h * head : (h + 1) * head]
                v = kvs[origin, 1, :, h * head : (h + 1) * head]
                v_wide = jnp.concatenate([v, jnp.ones((keys, head), BF16)], axis=1)
                for g in range(group):
                    n = h * group + g
                    slot, lane = (n * head) // width, (n * head) % width
                    q = q_all[slot, at, lane : lane + head]
                    scores = lax.dot_general(q, k, (((1,), (1,)), ((), ())), preferred_element_type=F32)
                    scores = jnp.concatenate([scores[:, :lat_rows], scores[:, lat_rows:] + lift[n]], axis=1)
                    before = top[n, at, :]
                    now = jnp.maximum(before, jnp.max(scores, axis=-1, keepdims=True))
                    expo = jnp.exp(scores - now)
                    keep = jnp.exp(before - now)
                    top[n, at, :] = now
                    acc[n, at, :] = acc[n, at, :] * keep + jnp.dot(expo.astype(BF16), v_wide, preferred_element_type=F32)
            return unused

        lax.fori_loop(0, q_tiles, q_rows, 0)
        return unused

    lax.fori_loop(0, sp, block, 0)

    def close(t, unused):
        at = pl.ds(pl.multiple_of(t * q_tile, q_tile), q_tile)
        for pair in range(heads // 2):
            two = [acc[2 * pair + n, at, :] for n in range(2)]
            two = [v[:, :head] / v[:, head:] for v in two]
            attended[at, pair * 2 * head : (pair + 1) * 2 * head] = jnp.concatenate(two, axis=1).astype(BF16)
        return unused

    lax.fori_loop(0, q_tiles, close, 0)
    if ring:
        for number in range(tiles):
            for index in range(6):
                ring_copy(number, index).wait_send()
    else:
        for step in range(1, sp):
            direct(step).wait_send()
    for item in sends + outs:
        item.wait_send()
    gather.finish()


def back_kernel(tp, att, weight, out, full, wide, total, mixed, landed, send, recv, asend, arecv, local):
    f = lax.axis_index("tp")
    rows, cols = att.shape
    own_rows = out.shape[0]
    out_cols = weight.shape[1]
    load = pltpu.make_async_copy(weight, wide, local.at[0])
    load.start()
    mine = pltpu.make_async_copy(att, full.at[f], local.at[1])
    mine.start()
    greet(others("tp", tp))
    gather = Gather(tp, att, full, send, recv)
    gather.start()
    gather.second()
    total[...] = jnp.zeros(total.shape, F32)
    gather.relay()
    mine.wait()
    load.wait()
    r_tile = min(256, rows)

    def chip_step(index, unused):
        gather.before(index)
        chip = gather.chip(index)

        def row_step(t, unused):
            at = pl.ds(pl.multiple_of(t * r_tile, r_tile), r_tile)
            value = total[at, :]
            for n in range(2):
                source = chip * 2 + n
                depth = pl.ds(pl.multiple_of(source * cols, cols), cols)
                value = value + jnp.dot(full[source, at, :], wide[depth, :], preferred_element_type=F32)
            total[at, :] = value
            return unused

        lax.fori_loop(0, rows // r_tile, row_step, 0)
        return unused

    lax.fori_loop(0, tp // 2, chip_step, 0)
    for peer in range(tp):
        mixed[peer] = total[peer * own_rows : (peer + 1) * own_rows, :].astype(BF16)
    sends = []
    for step in range(1, tp):
        peer = lax.rem(f + step, tp)
        sends.append(remote(mixed.at[peer], landed.at[f], asend, arecv, step - 1, "tp", peer))
    for item in sends:
        item.start()
    landed[f] = mixed[f]
    for step in range(1, tp):
        origin = lax.rem(f - step + tp, tp)
        remote(landed.at[origin], landed.at[origin], asend, arecv, step - 1, "tp", origin).wait_recv()
    for n in range(tp):
        out[:, n * out_cols : (n + 1) * out_cols] = landed[n]
    for item in sends:
        item.wait_send()
    gather.finish()


def tables(first, count, head):
    freqs = head // 4
    lane = jnp.arange(2 * head, dtype=jnp.int32) % head
    inverse = 10000.0 ** (-(lane // 2 % freqs).astype(F32) / freqs)
    sign = jnp.where(lane % 2 == 0, -1.0, 1.0)
    grid_rows = -(-(count // GRID_W) // 8) * 8
    index = jnp.arange(grid_rows + GRID_W, dtype=jnp.int32)
    spot = jnp.where(index < grid_rows, index + first // GRID_W, index - grid_rows)
    angles = spot.astype(F32)[:, None] * inverse
    return jnp.cos(angles), jnp.sin(angles) * sign


def local(sp, tp, latent, context, condition, context_cond, mod_weight, norm_gain, query_weight, key_weight,
          value_weight, out_weight, query_gain, key_gain, context_lift):
    rows, model = latent.shape
    ctx_rows = context.shape[0]
    head = query_gain.shape[0]
    heads = query_weight.shape[1] // head
    kv_heads = key_weight.shape[1] // head
    width = key_weight.shape[1]
    slots = query_weight.shape[1] // width + 2
    block = rows * tp
    keys = block + ctx_rows
    limit = 60 * 1024 * 1024
    cond_pair = jax.nn.silu(jnp.stack([condition, context_cond])).astype(BF16)
    mcols = mod_weight.shape[1]
    cos, sin = tables(lax.axis_index("sp") * block, block, head)
    stacked = width % 128 != 0
    weights = [query_weight, key_weight, value_weight]
    if stacked:
        weights = [jnp.stack([query_weight[:, n * width : (n + 1) * width] for n in range(slots - 2)] + weights[1:])]
    dma = pltpu.SemaphoreType.DMA
    count = gather_sems(tp)
    pieces = (tp // 2 + 1) * 6 if sp == 4 else sp - 1
    attended, gate = pl.pallas_call(
        functools.partial(front_kernel, sp, tp, heads, kv_heads, head, stacked),
        name="front",
        out_shape=(jax.ShapeDtypeStruct((block, heads * head), BF16), jax.ShapeDtypeStruct((1, model), F32)),
        in_specs=[ANY, ANY, VMEM, ANY, VMEM, VMEM, VMEM, VMEM, VMEM, SMEM] + [ANY] * len(weights),
        out_specs=(VMEM, VMEM),
        scratch_shapes=[
            pltpu.VMEM((tp + 2, rows, model), BF16),
            pltpu.VMEM((2 * rows, model), BF16),
            pltpu.VMEM((slots, model, width), BF16),
            pltpu.VMEM(mod_weight.shape, BF16),
            pltpu.VMEM((sp, 2, mcols), F32),
            pltpu.VMEM((2, mcols), F32),
            pltpu.VMEM((2, mcols), F32),
            pltpu.VMEM((2, mcols * tp), F32),
            pltpu.VMEM((2, 1, model), F32),
            pltpu.VMEM((2, 1, model), F32),
            pltpu.VMEM((slots, 1, width), F32),
            pltpu.VMEM((slots - 2, block, width), BF16),
            pltpu.VMEM((sp, 2, keys, width), BF16),
            pltpu.VMEM((heads, block, 1), F32),
            pltpu.VMEM((heads, block, 2 * head), F32),
            dma((count,)), dma((count,)), dma((sp - 1,)), dma((sp - 1,)), dma((tp - 1,)), dma((tp - 1,)),
            dma((pieces,)), dma((pieces,)),
            dma((slots + 4,)),
        ],
        compiler_params=pltpu.CompilerParams(collective_id=0, has_side_effects=True, vmem_limit_bytes=limit),
    )(latent, context, cond_pair, mod_weight, norm_gain.reshape(1, model), cos, sin, query_gain.reshape(1, head),
      key_gain.reshape(1, head), context_lift, *weights)
    mixed = pl.pallas_call(
        functools.partial(back_kernel, tp),
        name="back",
        out_shape=jax.ShapeDtypeStruct((rows, model), BF16),
        in_specs=[VMEM, ANY],
        out_specs=VMEM,
        scratch_shapes=[
            pltpu.VMEM((tp, block, heads * head), BF16),
            pltpu.VMEM(out_weight.shape, BF16),
            pltpu.VMEM((block, out_weight.shape[1]), F32),
            pltpu.VMEM((tp, rows, out_weight.shape[1]), BF16),
            pltpu.VMEM((tp, rows, out_weight.shape[1]), BF16),
            dma((count,)), dma((count,)), dma((tp - 1,)), dma((tp - 1,)), dma((2,)),
        ],
        compiler_params=pltpu.CompilerParams(collective_id=2, has_side_effects=True, vmem_limit_bytes=limit),
    )(attended, out_weight)
    return (latent.astype(F32) + gate * mixed.astype(F32)).astype(BF16)


def partner(s, order):
    return jnp.where(order == 0, s, jnp.where(order == 1, s + 1 - 2 * (s % 2), jnp.where(order == 2, 3 - s, (s + 2) % 4)))


class Square:
    def __init__(self, own, full, send, recv, base):
        self.own, self.full, self.send, self.recv, self.base = own, full, send, recv, base
        me = lax.axis_index("tp")
        self.me = me
        self.half = own.shape[0] // 2
        core, x, y = me % 2, (me // 2) % 2, me // 4
        self.sib = me + 1 - 2 * core
        self.step = 1 - 2 * core
        self.xn = me + 2 - 4 * x
        self.yn = me + 4 - 8 * y
        self.dn = self.xn + 4 - 8 * y

    def part(self, ref, which):
        return ref if which is None else ref.at[pl.ds(which * self.half, self.half)]

    def copy(self, index):
        me, xn, yn, dn, sib = self.me, self.xn, self.yn, self.dn, self.sib
        origin, half, peer = {
            0: (me, 0, xn), 1: (me, 1, xn), 2: (me, 0, yn), 3: (me, 1, yn), 4: (me, None, sib),
            5: (xn, 1, yn), 6: (yn, 0, xn),
            7: (xn, 0, sib), 8: (xn, 1, sib), 9: (yn, 0, sib), 10: (yn, 1, sib),
            11: (dn, 0, sib), 12: (dn, 1, sib),
        }[index]
        source = self.own if index < 5 else self.full.at[origin]
        return remote(self.part(source, half), self.part(self.full.at[origin], half), self.send, self.recv,
                      self.base + index, "tp", peer)

    def start(self, *indices):
        for index in indices:
            self.copy(index).start()

    def arrived(self, *indices):
        xn, yn, dn, sib, step = self.xn, self.yn, self.dn, self.sib, self.step
        for index in indices:
            origin, half = {
                0: (xn, 0), 1: (xn, 1), 2: (yn, 0), 3: (yn, 1), 4: (sib, None), 5: (dn, 1), 6: (dn, 0),
                7: (xn + step, 0), 8: (xn + step, 1), 9: (yn + step, 0), 10: (yn + step, 1),
                11: (dn + step, 0), 12: (dn + step, 1),
            }[index]
            ref = self.part(self.full.at[origin], half)
            remote(ref, ref, self.send, self.recv, self.base + index, "tp", sib).wait_recv()

    def finish(self):
        for index in range(13):
            self.copy(index).wait_send()


class Cross(Square):
    def copy(self, index):
        origin, peer = {
            0: (self.me, self.xn), 1: (self.me, self.yn), 2: (self.me, self.dn), 3: (self.me, self.sib),
            4: (self.xn, self.sib), 5: (self.yn, self.sib), 6: (self.dn, self.sib),
        }[index]
        ref = self.full.at[origin]
        return remote(ref, ref, self.send, self.recv, self.base + index, "tp", peer)

    def arrived(self, *indices):
        for index in indices:
            origin = {
                0: self.xn, 1: self.yn, 2: self.dn, 3: self.sib,
                4: self.xn + self.step, 5: self.yn + self.step, 6: self.dn + self.step,
            }[index]
            ref = self.full.at[origin]
            remote(ref, ref, self.send, self.recv, self.base + index, "tp", self.sib).wait_recv()

    def finish(self):
        for index in range(7):
            self.copy(index).wait_send()


def whole_kernel(head, lat, ctx, cond, ctx_cond, mod_weight, gain, cos_in, sin_in, q_gain, k_gain, lift, wq, wk, wv, wo_in, out,
                 full, normed, wide, mod_wide, wo, parts, partial, total_mod, mod, gsc, shf, gains, cos, sin,
                 kv_out, kv_in, v_rows, q_out, q_in, o_out, att, total, mixed, landed, result, sc_a, sc_b, max_a, max_b,
                 send, recv, psend, precv, msend, mrecv, ksend, krecv, qsend, qrecv, osend, orecv, asend, arecv,
                 bsend, brecv, local):
    sp, tp = 4, 8
    s, f = lax.axis_index("sp"), lax.axis_index("tp")
    rows, model = lat.shape
    tile = 2 * rows
    block = rows * tp
    ctx_rows = ctx.shape[0]
    mcols = partial.shape[1]
    half_rows = rows // 2
    width = wk.shape[1]
    pack = 2 * head
    chunk = block // 2
    scale = head ** -0.5

    mod_in = pltpu.make_async_copy(mod_weight, mod_wide, local.at[0])
    mod_in.start()
    barrier = pltpu.get_barrier_semaphore()
    peers = others("tp", tp) + others("sp", sp)
    for axis, peer in peers:
        pl.semaphore_signal(barrier, inc=1, device_id={axis: peer}, device_id_type=MESH)
    ctx_in = [pltpu.make_async_copy(ctx.at[pl.ds(n * rows, rows)], full.at[tp + n], local.at[1 + n]) for n in range(2)]
    own = pltpu.make_async_copy(lat, full.at[f], local.at[3])
    weights = [
        pltpu.make_async_copy(wk, wide.at[0, :, pl.ds(0, width)], local.at[4]),
        pltpu.make_async_copy(wv, wide.at[0, :, pl.ds(width, width)], local.at[5]),
        pltpu.make_async_copy(wq, wide.at[1], local.at[6]),
    ]
    tabs = [pltpu.make_async_copy(cos_in, cos, local.at[7]), pltpu.make_async_copy(sin_in, sin, local.at[8])]
    out_w = [pltpu.make_async_copy(wo_in.at[:, n], wo.at[n], local.at[9 + n]) for n in range(sp)]
    pair = jnp.concatenate([cond[...], ctx_cond[...]], axis=0)
    pair = (pair / (1.0 + jnp.exp(-pair))).astype(BF16)
    pl.semaphore_wait(barrier, len(peers))
    gather = Square(lat, full, send, recv, 0)
    gather.start(1, 2, 4)
    mod_in.wait()
    for item in ctx_in + [own] + weights + tabs + out_w:
        item.start()
    first_sum = jnp.dot(pair, mod_wide[...], preferred_element_type=F32)
    partial[...] = first_sum
    parts[s] = first_sum
    sends = [remote(partial, parts.at[s], psend, precv, n - 1, "sp", partner(s, n)) for n in range(1, sp)]
    for item in sends:
        item.start()
    gains[0] = jnp.concatenate([k_gain[...]] * (width // head), axis=1)
    gains[1] = jnp.concatenate([q_gain[...] * scale] * (width // head), axis=1)
    total[...] = jnp.zeros(total.shape, F32)
    for n in range(1, sp):
        origin = partner(s, n)
        remote(parts.at[origin], parts.at[origin], psend, precv, n - 1, "sp", origin).wait_recv()
    summed = parts[0] + parts[1] + parts[2] + parts[3]
    total_mod[...] = summed
    here = pl.ds(pl.multiple_of(f * mcols, mcols), mcols)
    mod[:, here] = summed
    outs = [remote(total_mod, mod.at[:, here], msend, mrecv, step - 1, "tp", lax.rem(f + step, tp)) for step in range(1, tp)]
    for item in outs:
        item.start()
    gather.start(0, 3)
    for step in range(1, tp):
        origin = lax.rem(f - step + tp, tp)
        ref = mod.at[:, pl.ds(pl.multiple_of(origin * mcols, mcols), mcols)]
        remote(ref, ref, msend, mrecv, step - 1, "tp", origin).wait_recv()
    for r in range(2):
        gsc[r] = gain[...] * (1.0 + mod[r : r + 1, model : 2 * model])
        shf[r] = mod[r : r + 1, :model]
    gather.arrived(1)
    gather.start(5, 8)
    gather.arrived(2)
    gather.start(6, 9)
    for item in ctx_in + [own] + weights + tabs:
        item.wait()

    even = lax.broadcasted_iota(jnp.int32, (tile, width), 1) % 2 == 0
    same = (
        lax.broadcasted_iota(jnp.int32, (width, width), 0) // head
        == lax.broadcasted_iota(jnp.int32, (width, width), 1) // head
    )
    ones = jnp.where(same, 1.0, 0.0).astype(BF16)
    by_row = (lax.broadcasted_iota(jnp.int32, (1, pack), 1) % head) // 2 < head // 4
    low = lax.broadcasted_iota(jnp.int32, (tile, pack), 1) < head
    grid_rows = cos.shape[0] - GRID_W
    step_rows, wide_step = 16, 512
    steps = half_rows // step_rows

    def chip_at(index):
        x, y = (f // 2) % 2, f // 4
        return ((y + index // 2) % 2) * 2 + (x + index) % 2

    odd = s % 2

    def rows_at(number, plane):
        chip = chip_at(jnp.maximum(number - 1, 0))
        at_out = jnp.where(number == 0, block, chip * tile)
        at_in = jnp.where(number == 0, sp * block + plane * ctx_rows, plane * block + chip * tile)
        return pl.ds(pl.multiple_of(at_out, tile), tile), pl.ds(pl.multiple_of(at_in, tile), tile)

    def kv_send(number, a, n):
        at_out, at_in = rows_at(number, s)
        head_pack = 2 * odd + a if n == 3 else 2 * (1 - odd) + a
        return remote(kv_out.at[head_pack, at_out], kv_in.at[a, at_in], ksend, krecv, number * 6 + a * 3 + n - 1, "sp",
                      partner(s, n))

    def kv_wait(number, a, n):
        ref = kv_in.at[a, rows_at(number, partner(s, n))[1]]
        remote(ref, ref, ksend, krecv, number * 6 + a * 3 + n - 1, "sp", partner(s, n)).wait_recv()

    def q_copy(number, a):
        there = pl.ds(pl.multiple_of(chip_at(number - 1) * rows, rows), rows)
        return remote(q_out.at[2 * (1 - odd) + a, :, there], q_in.at[a, 1, :, there], qsend, qrecv, (number - 1) * 2 + a, "sp",
                      partner(s, 1))

    def q_wait(number, a):
        ref = q_in.at[a, 1, :, pl.ds(pl.multiple_of(chip_at(number - 1) * rows, rows), rows)]
        remote(ref, ref, qsend, qrecv, (number - 1) * 2 + a, "sp", partner(s, 1)).wait_recv()

    def one_tile(number, unused):
        @pl.when(number == 1)
        def _():
            gather.arrived(4)

        @pl.when(number == 2)
        def _():
            gather.arrived(0)
            gather.start(7)
            gather.arrived(3)
            gather.start(10)
            gather.arrived(7, 8)

        @pl.when(number == 3)
        def _():
            gather.arrived(9, 10)

        @pl.when(number == 4)
        def _():
            gather.arrived(5)
            gather.start(12)
            gather.arrived(6)
            gather.start(11)
            gather.arrived(12, 11)

        is_ctx = jnp.where(number == 0, 1, 0)
        chip = chip_at(jnp.maximum(number - 1, 0))
        base = jnp.where(number == 0, tp, chip * 2)

        def norm_rows(j, unused):
            slot = base + (j // steps) % 2
            row = pl.multiple_of((j // (2 * steps)) * half_rows + (j % steps) * step_rows, step_rows)
            there = pl.ds(pl.multiple_of(j * step_rows, step_rows), step_rows)
            squares = jnp.zeros((step_rows, 128), F32)
            for n in range(model // wide_step):
                v = full[slot, pl.ds(row, step_rows), n * wide_step : (n + 1) * wide_step].astype(F32)
                v = v * v
                for m in range(wide_step // 128):
                    squares = squares + v[:, m * 128 : (m + 1) * 128]
            inv = lax.rsqrt(jnp.sum(squares, axis=-1, keepdims=True) * (1.0 / model) + EPS)
            for n in range(model // wide_step):
                cols = slice(n * wide_step, (n + 1) * wide_step)
                v = full[slot, pl.ds(row, step_rows), cols].astype(F32)
                normed[there, cols] = (v * inv * gsc[is_ctx, :, cols] + shf[is_ctx, :, cols]).astype(BF16)
            return unused

        lax.fori_loop(0, tile // step_rows, norm_rows, 0, unroll=4)

        def table(ref, fill):
            pieces = []
            for c in range(2):
                for owner in range(2):
                    row = ref[pl.ds(s * tp + chip * 2 + owner, 1), :]
                    col = ref[grid_rows + c * half_rows : grid_rows + (c + 1) * half_rows, :]
                    pieces.append(jnp.where(by_row, row, col))
            v = jnp.concatenate(pieces, axis=0)
            v = jnp.where(is_ctx == 1, fill, v)
            return jnp.concatenate([v] * (width // pack), axis=1)

        cos_t, sin_t = table(cos, 1.0), table(sin, 0.0)

        def turned(y, row):
            sq = y * y
            hi = sq.astype(BF16)
            lo = (sq - hi.astype(F32)).astype(BF16)
            mean = jnp.dot(hi, ones, preferred_element_type=F32) + jnp.dot(lo, ones, preferred_element_type=F32)
            u = y * lax.rsqrt(mean * (1.0 / head) + EPS) * row
            other = jnp.where(even, pltpu.roll(u, width - 1, axis=1), pltpu.roll(u, 1, axis=1))
            return u * cos_t + other * sin_t

        y = jnp.dot(normed[...], wide[0], preferred_element_type=F32)
        k, v = turned(y[:, :width], gains[0]), y[:, width:]
        at_out, at_in = rows_at(number, s)
        for n in range(width // pack):
            kc, vc = k[:, n * pack : (n + 1) * pack], v[:, n * pack : (n + 1) * pack]
            kv_out[2 * n, at_out, :] = jnp.where(low, kc, pltpu.roll(vc, head, axis=1)).astype(BF16)
            kv_out[2 * n + 1, at_out, :] = jnp.where(low, pltpu.roll(kc, head, axis=1), vc).astype(BF16)
        for n in (2, 3, 1):
            kv_send(number, 0, n).start()

        @pl.when(number == 1)
        def _():
            for n in (2, 3, 1):
                kv_send(number - 1, 1, n).start()

        for a in range(2):
            kv_in[a, at_in, :] = kv_out[2 * odd + a, at_out, :]

        @pl.when(number > 0)
        def _():
            y = jnp.dot(normed[...], wide[1], preferred_element_type=F32)
            for n in range(2):
                q = turned(y[:, n * width : (n + 1) * width], gains[1]).astype(BF16)
                for m in range(2):
                    for c in range(2):
                        q_out[2 * n + m, c, pl.ds(pl.multiple_of(chip * rows, rows), rows), :] = (
                            q[c * rows : (c + 1) * rows, m * pack : (m + 1) * pack])
            for a in range(2):
                q_copy(number, a).start()

        return unused

    lax.fori_loop(0, tp // 2 + 1, one_tile, 0)

    def late_kv(number, unused):
        for n in (2, 3, 1):
            kv_send(number, 1, n).start()
        return unused

    lax.fori_loop(1, tp // 2 + 1, late_kv, 0)
    for a in range(2):
        q_in[a, 0] = q_out[2 * odd + a]
    keys = kv_in.shape[1]
    for item in out_w:
        item.wait()
    pieces = 2 * sp

    def step_at(p):
        return p // 4, 1 - p % 2, (p % 4) // 2

    def o_send(a, c):
        return remote(o_out.at[a, c], att.at[a * 4 + 2 * c, f], osend, orecv, a * 2 + c, "sp", partner(s, 1))

    def piece_of(p):
        return Cross(att.at[p, f], att.at[p], asend, arecv, p * 7)

    def back_send(c, step):
        peer = lax.rem(f + step, tp)
        return remote(mixed.at[c, peer], landed.at[c, f], bsend, brecv, c * (tp - 1) + step - 1, "tp", peer)

    def stage_zero(p):
        a, other, c = step_at(p)
        if other:
            ref = att.at[p, f]
            remote(ref, ref, osend, orecv, a * 2 + c, "sp", partner(s, 1)).wait_recv()
        piece_of(p).start(2, 0, 1, 3)

    def stage_one(p):
        piece = piece_of(p)
        piece.arrived(0, 1, 2)
        piece.start(4, 5, 6)

    def stage_three(p):
        piece_of(p).arrived(3, 4, 5, 6)
        a, other, c = step_at(p)
        source = 2 * (1 - odd) + a if other else 2 * odd + a
        left = jnp.concatenate([att[p, n] for n in range(tp)], axis=1)
        total[c] += jnp.dot(left, wo[source].reshape(tp * pack, wo.shape[3]), preferred_element_type=F32)

    def back(c):
        for n in range(tp):
            mixed[c, n] = total[c, n * half_rows : (n + 1) * half_rows, :].astype(BF16)
        for step in range(1, tp):
            back_send(c, step).start()
        landed[c, f] = mixed[c, f]

    key_step = block
    first_head = lax.broadcasted_iota(jnp.int32, (1, 2 * chunk), 1) < chunk

    def advance(a, m, old, old_max, new, new_max):
        if new is not None:
            _, other, c = step_at(m + 1)
            if m + 1 == 0:
                for number in range(1, tp // 2 + 1):
                    q_wait(number, a)
            lifts = jnp.where(first_head, lift[4 * odd + 2 * a], lift[4 * odd + 2 * a + 1])
            q = q_in[a, other, c]
            both = jnp.concatenate([q[:, :head], q[:, head:]], axis=0)
            high = None
        if old is not None:
            peak = jnp.max(old_max[...], axis=0, keepdims=True)
            acc = None
        for n in range(keys // key_step):
            there = slice(n * key_step, (n + 1) * key_step)
            if new is not None:
                scores = lax.dot_general(kv_in[a, there, :head], both, (((1,), (1,)), ((), ())), preferred_element_type=F32)
                if n >= sp:
                    scores = scores + lifts
                new[there, :] = scores
                part = jnp.max(scores.reshape(key_step // 8, 8, 2 * chunk), axis=0)
                high = part if high is None else jnp.maximum(high, part)
            if old is not None:
                expo = jnp.exp(old[there, :] - peak).astype(BF16)
                part = jnp.dot(v_rows[:, there], expo, preferred_element_type=F32)
                acc = part if acc is None else acc + part
        if new is not None:
            new_max[...] = high
        if old is None:
            return
        value = acc[:head] / acc[head : head + 1]
        value = jnp.concatenate([value[:, :chunk], value[:, chunk:]], axis=0).T.astype(BF16)
        _, other, c = step_at(m)
        if other:
            o_out[a, c] = value
            o_send(a, c).start()
        else:
            att[a * 4 + m, f] = value

    def run(a, m, *stages):
        @pl.when(a == m // 4)
        def _():
            for stage, p in stages:
                stage(p)

    zero, one, three = stage_zero, stage_one, stage_three

    def one_head(a, unused):
        def wait_kv(number, unused):
            for n in range(1, sp):
                kv_wait(number, a, n)
            return unused

        run(a, 4, (zero, 2), (one, 1))
        lax.fori_loop(0, tp // 2 + 1, wait_kv, 0)
        v_rows[...] = jnp.concatenate([kv_in[a, :, head:].astype(F32), jnp.ones((keys, head), F32)], axis=1).T.astype(BF16)
        advance(a, -1, None, None, sc_a, max_a)
        advance(a, 0, sc_a, max_a, sc_b, max_b)
        run(a, 4, (one, 0), (one, 3), (three, 1))
        advance(a, 1, sc_b, max_b, sc_a, max_a)
        run(a, 1, (zero, 1))
        run(a, 5, (zero, 5), (one, 2), (three, 0))
        advance(a, 2, sc_a, max_a, sc_b, max_b)
        run(a, 2, (zero, 0))
        run(a, 6, (zero, 4), (three, 3))
        advance(a, 3, sc_b, max_b, None, None)
        run(a, 3, (zero, 3))
        return unused

    lax.fori_loop(0, 2, one_head, 0)
    zero(7)
    one(5)
    three(2)
    zero(6)
    one(4)
    three(5)
    three(4)
    back(0)
    one(7)
    one(6)
    three(7)
    three(6)
    back(1)
    cols = wo.shape[3]
    writes = []
    for c in range(2):
        for step in range(1, tp):
            origin = lax.rem(f - step + tp, tp)
            ref = landed.at[c, origin]
            remote(ref, ref, bsend, brecv, c * (tp - 1) + step - 1, "tp", origin).wait_recv()
        at = slice(c * half_rows, (c + 1) * half_rows)
        for n in range(tp):
            there = slice(n * cols, (n + 1) * cols)
            gate = mod[0:1, 2 * model + n * cols : 2 * model + (n + 1) * cols]
            result[at, there] = (full[f, at, there].astype(F32) + gate * landed[c, n].astype(F32)).astype(BF16)
        writes.append(pltpu.make_async_copy(result.at[pl.ds(c * half_rows, half_rows)], out.at[pl.ds(c * half_rows, half_rows)],
                                            local.at[9 + sp + c]))
        writes[-1].start()
    for item in sends + outs:
        item.wait_send()
    gather.finish()

    def drain_kv(number, unused):
        for a in range(2):
            for n in range(1, sp):
                kv_send(number, a, n).wait_send()
        return unused

    lax.fori_loop(0, tp // 2 + 1, drain_kv, 0)
    for a in range(2):
        for c in range(2):
            o_send(a, c).wait_send()
        for number in range(1, tp // 2 + 1):
            q_copy(number, a).wait_send()

    def drain_pieces(p, unused):
        piece_of(p).finish()
        return unused

    lax.fori_loop(0, pieces, drain_pieces, 0)
    for c in range(2):
        for step in range(1, tp):
            back_send(c, step).wait_send()
    for item in writes:
        item.wait()


def all_tables(count, head):
    freqs = head // 4
    lane = np.arange(2 * head) % head
    inverse = (10000.0 ** (-(lane // 2 % freqs).astype(np.float32) / freqs)).astype(np.float32)
    sign = np.where(lane % 2 == 0, -1.0, 1.0).astype(np.float32)
    spot = np.concatenate([np.arange(count // GRID_W), np.arange(GRID_W)]).astype(np.float32)
    angles = (spot[:, None] * inverse).astype(np.float32)
    return np.cos(angles).astype(np.float32), (np.sin(angles) * sign).astype(np.float32)


def whole(sp, tp, latent, context, condition, context_cond, mod_weight, norm_gain, query_weight, key_weight,
          value_weight, out_weight, query_gain, key_gain, context_lift):
    rows, model = latent.shape
    head = query_gain.shape[0]
    block = rows * tp
    ctx_rows = context.shape[0]
    width = key_weight.shape[1]
    mcols = mod_weight.shape[1]
    out_cols = out_weight.shape[1]
    pack = 2 * head
    chunk = block // 2
    keys = sp * (block + ctx_rows)
    cos, sin = all_tables(sp * block, head)
    dma = lambda *shape: pltpu.SemaphoreType.DMA(shape)
    vm = pltpu.VMEM
    tiles = tp // 2 + 1
    return pl.pallas_call(
        functools.partial(whole_kernel, head),
        name="whole",
        out_shape=jax.ShapeDtypeStruct((rows, model), BF16),
        in_specs=[ANY, ANY, VMEM, VMEM, ANY, VMEM, ANY, ANY, VMEM, VMEM, SMEM, ANY, ANY, ANY, ANY],
        out_specs=ANY,
        scratch_shapes=[
            vm((tp + 2, rows, model), BF16),
            vm((2 * rows, model), BF16),
            vm((2, model, 2 * width), BF16),
            vm(mod_weight.shape, BF16),
            vm((sp, tp, pack, out_cols), BF16),
            vm((sp, 2, mcols), F32),
            vm((2, mcols), F32),
            vm((2, mcols), F32),
            vm((2, mcols * tp), F32),
            vm((2, 1, model), F32),
            vm((2, 1, model), F32),
            vm((2, 1, width), F32),
            vm(cos.shape, F32),
            vm(sin.shape, F32),
            vm((sp, block + ctx_rows, pack), BF16),
            vm((2, keys, pack), BF16),
            vm((pack, keys), BF16),
            vm((sp, 2, chunk, pack), BF16),
            vm((2, 2, 2, chunk, pack), BF16),
            vm((2, 2, chunk, pack), BF16),
            vm((2 * sp, tp, chunk, pack), BF16),
            vm((2, chunk, out_cols), F32),
            vm((2, tp, rows // 2, out_cols), BF16),
            vm((2, tp, rows // 2, out_cols), BF16),
            vm((rows, model), BF16),
            vm((keys, 2 * chunk), F32),
            vm((keys, 2 * chunk), F32),
            vm((8, 2 * chunk), F32),
            vm((8, 2 * chunk), F32),
            dma(13), dma(13), dma(sp - 1), dma(sp - 1), dma(tp - 1), dma(tp - 1),
            dma(tiles * 6), dma(tiles * 6), dma(8), dma(8), dma(4), dma(4),
            dma(7 * 8), dma(7 * 8), dma(2 * (tp - 1)), dma(2 * (tp - 1)),
            dma(9 + sp + 2),
        ],
        compiler_params=pltpu.CompilerParams(collective_id=1, has_side_effects=True, vmem_limit_bytes=62 * 1024 * 1024),
    )(latent, context, condition.reshape(1, -1), context_cond.reshape(1, -1), mod_weight, norm_gain.reshape(1, model),
      cos, sin, query_gain.reshape(1, head), key_gain.reshape(1, head), context_lift, query_weight, key_weight,
      value_weight, out_weight.reshape(tp, sp, pack, out_cols))


def fits(sp, tp, latent, context, key_weight, query_weight, query_gain):
    head = query_gain.shape[0]
    return (
        sp == 4 and tp == 8 and latent.shape[0] == GRID_W and context.shape[0] == 2 * latent.shape[0]
        and 2 * head == 128 and key_weight.shape[1] == sp * head and query_weight.shape[1] == 2 * sp * head
    )


def chosen(sp, tp, *args):
    latent, context, query_weight, key_weight, query_gain = args[0], args[1], args[6], args[7], args[10]
    if fits(sp, tp, latent, context, key_weight, query_weight, query_gain):
        return whole(sp, tp, *args)
    return local(sp, tp, *args)


def solution(mesh):
    return jax.shard_map(
        functools.partial(chosen, mesh.shape["sp"], mesh.shape["tp"]),
        mesh=mesh,
        in_specs=(
            P(("sp", "tp"), None),
            P("sp", None),
            P("sp"),
            P("sp"),
            P("sp", "tp"),
            P(),
            P(None, "tp"),
            P(None, "tp"),
            P(None, "tp"),
            P(None, "tp"),
            P(),
            P(),
            P("tp"),
        ),
        out_specs=P(("sp", "tp"), None),
        check_vma=False,
    )
```

```python
import functools

import jax
import jax.numpy as jnp
import numpy as np
from jax import lax
from jax.experimental import pallas as pl
from jax.experimental.pallas import tpu as pltpu
from jax.sharding import PartitionSpec as P

GRID_W = 64
EPS = 1e-06
MESH = pl.DeviceIdType.MESH
ANY = pl.BlockSpec(memory_space=pl.ANY)
VMEM = pl.BlockSpec(memory_space=pltpu.VMEM)
SMEM = pl.BlockSpec(memory_space=pltpu.SMEM)
BF16 = jnp.bfloat16
F32 = jnp.float32


def remote(src, dst, send, recv, index, axis, peer):
    return pltpu.make_async_remote_copy(
        src_ref=src, dst_ref=dst, send_sem=send.at[index], recv_sem=recv.at[index],
        device_id={axis: peer}, device_id_type=MESH,
    )


def greet(peers):
    barrier = pltpu.get_barrier_semaphore()
    for axis, peer in peers:
        pl.semaphore_signal(barrier, inc=1, device_id={axis: peer}, device_id_type=MESH)
    pl.semaphore_wait(barrier, len(peers))


def others(axis, count):
    me = lax.axis_index(axis)
    return [(axis, lax.rem(me + step, count)) for step in range(1, count)]


def gather_sems(count):
    return 13 if count == 8 else max(count - 1, 1)


class Gather:
    def __init__(self, count, own, full, send, recv):
        self.count, self.own, self.full, self.send, self.recv = count, own, full, send, recv
        self.me = lax.axis_index("tp")
        self.half = own.shape[0] // 2
        me = self.me
        if count == 8:
            self.core, self.x, self.y = me % 2, (me // 2) % 2, me // 4
            self.sib = me + 1 - 2 * self.core
            self.step = 1 - 2 * self.core
            self.xn = me + 2 - 4 * self.x
            self.yn = me + 4 - 8 * self.y
            self.dn = self.xn + 4 - 8 * self.y

    def part(self, ref, which):
        return ref if which is None else ref.at[pl.ds(which * self.half, self.half)]

    def copy(self, index):
        me, xn, yn, dn, sib = self.me, self.xn, self.yn, self.dn, self.sib
        origin, half, peer = {
            0: (me, 0, xn), 1: (me, 1, xn), 2: (me, 0, yn), 3: (me, 1, yn), 4: (me, None, sib),
            5: (xn, 1, yn), 6: (yn, 0, xn),
            7: (xn, 0, sib), 8: (xn, 1, sib), 9: (yn, 0, sib), 10: (yn, 1, sib),
            11: (dn, 0, sib), 12: (dn, 1, sib),
        }[index]
        source = self.own if index < 5 else self.full.at[origin]
        return remote(self.part(source, half), self.part(self.full.at[origin], half), self.send, self.recv, index, "tp", peer)

    def wait_recv(self, index):
        xn, yn, dn, sib, step = self.xn, self.yn, self.dn, self.sib, self.step
        origin, half = {
            0: (xn, 0), 1: (xn, 1), 2: (yn, 0), 3: (yn, 1), 4: (sib, None), 5: (dn, 1), 6: (dn, 0),
            7: (xn + step, 0), 8: (xn + step, 1), 9: (yn + step, 0), 10: (yn + step, 1),
            11: (dn + step, 0), 12: (dn + step, 1),
        }[index]
        ref = self.part(self.full.at[origin], half)
        remote(ref, ref, self.send, self.recv, index, "tp", sib).wait_recv()

    def direct(self, step):
        peer = lax.rem(self.me + step, self.count)
        return remote(self.own, self.full.at[self.me], self.send, self.recv, step - 1, "tp", peer)

    def start(self):
        if self.count == 8:
            for index in (1, 2, 4):
                self.copy(index).start()
        else:
            for step in range(1, self.count):
                self.direct(step).start()

    def second(self):
        if self.count == 8:
            for index in (0, 3):
                self.copy(index).start()

    def relay(self):
        if self.count == 8:
            for arrived, then in ((1, (5, 8)), (2, (6, 9))):
                self.wait_recv(arrived)
                for nxt in then:
                    self.copy(nxt).start()

    def before(self, index):
        if self.count != 8:
            @pl.when(index == 0)
            def _():
                for step in range(1, self.count):
                    origin = lax.rem(self.me - step + self.count, self.count)
                    ref = self.full.at[origin]
                    remote(ref, ref, self.send, self.recv, step - 1, "tp", origin).wait_recv()
            return

        @pl.when(index == 0)
        def _():
            self.wait_recv(4)

        @pl.when(index == 1)
        def _():
            for arrived, nxt in ((0, 7), (3, 10)):
                self.wait_recv(arrived)
                self.copy(nxt).start()
            self.wait_recv(7)
            self.wait_recv(8)

        @pl.when(index == 2)
        def _():
            self.wait_recv(9)
            self.wait_recv(10)

        @pl.when(index == 3)
        def _():
            self.wait_recv(5)
            self.copy(12).start()
            self.wait_recv(6)
            self.copy(11).start()
            self.wait_recv(12)
            self.wait_recv(11)

    def chip(self, index):
        if self.count == 8:
            return ((self.y + index // 2) % 2) * 2 + (self.x + index) % 2
        return index

    def finish(self):
        if self.count == 8:
            for index in range(13):
                self.copy(index).wait_send()
        else:
            for step in range(1, self.count):
                self.direct(step).wait_send()


def front_kernel(sp, tp, heads, kv_heads, head, stacked, lat, ctx, cond, mod_weight, gain, cos, sin, q_gain, k_gain, lift, *rest):
    weights, rest = rest[: 1 if stacked else 3], rest[1 if stacked else 3 :]
    (attended, gate, full, normed, wide, mod_wide, parts, partial, total, mod, gsc, shf, gains, q_all, kvs, top, acc,
     send, recv, psend, precv, msend, mrecv, zsend, zrecv, local) = rest
    s, f = lax.axis_index("sp"), lax.axis_index("tp")
    rows, model = lat.shape
    width = wide.shape[2]
    slots = wide.shape[0]
    groups = slots - 2
    tile = 2 * rows
    lat_rows = rows * tp
    keys = kvs.shape[2]
    mcols = partial.shape[1]
    tiles = tp // 2 + 1
    scale = head ** -0.5
    mod_in = pltpu.make_async_copy(mod_weight, mod_wide, local.at[slots + 3])
    mod_in.start()
    copies = []
    if stacked:
        copies.append(pltpu.make_async_copy(weights[0], wide, local.at[0]))
    else:
        for n in range(groups):
            copies.append(pltpu.make_async_copy(weights[0].at[:, n * width : (n + 1) * width], wide.at[n], local.at[n]))
        copies.append(pltpu.make_async_copy(weights[1], wide.at[groups], local.at[groups]))
        copies.append(pltpu.make_async_copy(weights[2], wide.at[groups + 1], local.at[groups + 1]))
    own = pltpu.make_async_copy(lat, full.at[f], local.at[slots])
    ctx_in = [
        pltpu.make_async_copy(ctx.at[pl.ds(n * rows, rows)], full.at[tp + n], local.at[slots + 1 + n]) for n in range(2)
    ]
    greet(others("tp", tp) + others("sp", sp))
    gather = Gather(tp, lat, full, send, recv)
    gather.start()
    for item in ctx_in + [own] + copies[::-1]:
        item.start()
    mod_in.wait()
    first_sum = jnp.dot(cond[...], mod_wide[...], preferred_element_type=F32)
    partial[...] = first_sum
    parts[s] = first_sum
    sends = []
    for step in range(1, sp):
        sends.append(remote(partial, parts.at[s], psend, precv, step - 1, "sp", lax.rem(s + step, sp)))
    for item in sends:
        item.start()
    for n in range(slots):
        row = q_gain[...] * scale if n < groups else k_gain[...]
        gains[n] = jnp.concatenate([row] * (width // head), axis=1) if width > head else row
    for step in range(1, sp):
        origin = lax.rem(s - step + sp, sp)
        remote(parts.at[origin], parts.at[origin], psend, precv, step - 1, "sp", origin).wait_recv()
    summed = parts[0]
    for n in range(1, sp):
        summed = summed + parts[n]
    total[...] = summed
    here = pl.ds(pl.multiple_of(f * mcols, mcols), mcols)
    mod[:, here] = summed
    outs = []
    for step in range(1, tp):
        outs.append(remote(total, mod.at[:, here], msend, mrecv, step - 1, "tp", lax.rem(f + step, tp)))
    for item in outs:
        item.start()
    gather.second()
    top[...] = jnp.full(top.shape, -1e30, F32)
    acc[...] = jnp.zeros(acc.shape, F32)
    for step in range(1, tp):
        origin = lax.rem(f - step + tp, tp)
        ref = mod.at[:, pl.ds(pl.multiple_of(origin * mcols, mcols), mcols)]
        remote(ref, ref, msend, mrecv, step - 1, "tp", origin).wait_recv()
    for r in range(2):
        gsc[r] = gain[...] * (1.0 + mod[r : r + 1, model : 2 * model])
        shf[r] = mod[r : r + 1, :model]
    gate[...] = mod[0:1, 2 * model :]
    gather.relay()
    for item in ctx_in + copies:
        item.wait()
    own.wait()

    ring = sp == 4
    right, left, far = (s + 1) % sp, (s + sp - 1) % sp, (s + 2) % sp

    def tile_first(number):
        if isinstance(number, int):
            return lat_rows if number == 0 else pl.multiple_of(gather.chip(number - 1) * tile, tile)
        chip = jnp.where(number == 0, tp // 2, gather.chip(jnp.maximum(number - 1, 0)))
        return pl.multiple_of(chip * tile, tile)

    def ring_copy(number, index):
        which, origin, peer = {
            0: (0, s, right), 1: (1, s, right), 2: (1, s, left), 3: (0, s, left), 4: (0, left, right), 5: (1, right, left),
        }[index]
        ref = kvs.at[origin, which, pl.ds(tile_first(number), tile)]
        return remote(ref, ref, zsend, zrecv, number * 6 + index, "sp", peer)

    def ring_wait(number, index):
        which, origin = {0: (0, left), 1: (1, left), 2: (1, right), 3: (0, right), 4: (0, far), 5: (1, far)}[index]
        ref = kvs.at[origin, which, pl.ds(tile_first(number), tile)]
        remote(ref, ref, zsend, zrecv, number * 6 + index, "sp", right).wait_recv()

    def forward(number):
        ring_wait(number, 0)
        ring_copy(number, 4).start()
        ring_wait(number, 2)
        ring_copy(number, 5).start()

    def direct(step):
        return remote(kvs.at[s], kvs.at[s], zsend, zrecv, step - 1, "sp", lax.rem(s + step, sp))

    even = lax.broadcasted_iota(jnp.int32, (tile, width), 1) % 2 == 0
    same = (
        lax.broadcasted_iota(jnp.int32, (width, width), 0) // head
        == lax.broadcasted_iota(jnp.int32, (width, width), 1) // head
    )
    ones = jnp.where(same, 1.0, 0.0).astype(BF16)
    by_row = (lax.broadcasted_iota(jnp.int32, (1, 2 * head), 1) % head) // 2 < head // 4
    grid_rows = cos.shape[0] - GRID_W
    part = min(tile, GRID_W)
    step_rows = 16

    def roll(v, by):
        if width % 128 == 0:
            return pltpu.roll(v, by % width, axis=1)
        return jnp.concatenate([v[:, width - by % width :], v[:, : width - by % width]], axis=1)

    def table(ref, first, is_ctx, fill):
        pieces = []
        for k in range(tile // part):
            at = jnp.where(is_ctx == 1, 0, first + k * part)
            row = ref[pl.ds(at // GRID_W, 1), :]
            col = ref[pl.ds(pl.multiple_of(grid_rows + at % GRID_W, 8), part), :]
            pieces.append(jnp.where(by_row, row, col))
        v = jnp.concatenate(pieces, axis=0) if len(pieces) > 1 else pieces[0]
        v = jnp.where(is_ctx == 1, fill, v)
        if width > v.shape[1]:
            return jnp.concatenate([v] * (width // v.shape[1]), axis=1)
        return v[:, :width]

    def one_tile(number, unused):
        @pl.when(number > 0)
        def _():
            gather.before(number - 1)

        is_ctx = jnp.where(number == 0, 1, 0)
        first = tile_first(number)
        base = first // rows

        def norm_rows(j, unused):
            slot = base + (j * step_rows) // rows
            row = pl.multiple_of((j * step_rows) % rows, step_rows)
            v = full[slot, pl.ds(row, step_rows), :].astype(F32)
            inv = lax.rsqrt(jnp.mean(v * v, axis=-1, keepdims=True) + EPS)
            out = v * inv * gsc[is_ctx] + shf[is_ctx]
            normed[pl.ds(pl.multiple_of(j * step_rows, step_rows), step_rows), :] = out.astype(BF16)
            return unused

        lax.fori_loop(0, tile // step_rows, norm_rows, 0)

        def turned(y, n):
            sq = y * y
            hi = sq.astype(BF16)
            lo = (sq - hi.astype(F32)).astype(BF16)
            mean = jnp.dot(hi, ones, preferred_element_type=F32) + jnp.dot(lo, ones, preferred_element_type=F32)
            u = y * lax.rsqrt(mean * (1.0 / head) + EPS) * gains[n]
            other = jnp.where(even, roll(u, -1), roll(u, 1))
            return (u * table(cos, first, is_ctx, 1.0) + other * table(sin, first, is_ctx, 0.0)).astype(BF16)

        def one_slot(m, unused):
            n = (m + groups) % slots
            y = jnp.dot(normed[...], wide[n], preferred_element_type=F32)

            @pl.when(m == 1)
            def _():
                kvs[s, 1, pl.ds(first, tile), :] = y.astype(BF16)
                if ring:
                    for index in (0, 2, 1, 3):
                        ring_copy(number, index).start()

            @pl.when(m == 0)
            def _():
                kvs[s, 0, pl.ds(first, tile), :] = turned(y, n)

            @pl.when(m > 1)
            def _():
                q_all[n, pl.ds(first, tile), :] = turned(y, n)

            return unused

        lax.fori_loop(0, jnp.where(number == 0, 2, slots), one_slot, 0)
        return unused

    lax.fori_loop(0, tiles, one_tile, 0)

    if not ring:
        for step in range(1, sp):
            direct(step).start()
    group = heads // kv_heads
    q_tile = min(256, lat_rows)
    q_tiles = lat_rows // q_tile

    def block(b, unused):
        if ring:
            @pl.when(b == 0)
            def _():
                for number in range(tiles - 2):
                    forward(number)

            @pl.when(b == 1)
            def _():
                forward(tiles - 1)
                for number in range(tiles):
                    ring_wait(number, 1)

            @pl.when(b == 2)
            def _():
                for number in range(tiles):
                    ring_wait(number, 3)

            @pl.when(b == 3)
            def _():
                for number in range(tiles):
                    ring_wait(number, 4)
                    ring_wait(number, 5)

            origin = (s + jnp.where(b == 1, sp - 1, jnp.where(b == 2, 1, jnp.where(b == 3, 2, 0)))) % sp
        else:
            @pl.when(b == 1)
            def _():
                for step in range(1, sp):
                    source = lax.rem(s - step + sp, sp)
                    remote(kvs.at[source], kvs.at[source], zsend, zrecv, step - 1, "sp", source).wait_recv()

            origin = (s + b) % sp

        def q_rows(t, unused):
            if ring:
                @pl.when((b == 0) & (t == q_tiles - 1))
                def _():
                    forward(tiles - 2)

            at = pl.ds(pl.multiple_of(t * q_tile, q_tile), q_tile)
            for h in range(kv_heads):
                k = kvs[origin, 0, :, h * head : (h + 1) * head]
                v = kvs[origin, 1, :, h * head : (h + 1) * head]
                v_wide = jnp.concatenate([v, jnp.ones((keys, head), BF16)], axis=1)
                for g in range(group):
                    n = h * group + g
                    slot, lane = (n * head) // width, (n * head) % width
                    q = q_all[slot, at, lane : lane + head]
                    scores = lax.dot_general(q, k, (((1,), (1,)), ((), ())), preferred_element_type=F32)
                    scores = jnp.concatenate([scores[:, :lat_rows], scores[:, lat_rows:] + lift[n]], axis=1)
                    before = top[n, at, :]
                    now = jnp.maximum(before, jnp.max(scores, axis=-1, keepdims=True))
                    expo = jnp.exp(scores - now)
                    keep = jnp.exp(before - now)
                    top[n, at, :] = now
                    acc[n, at, :] = acc[n, at, :] * keep + jnp.dot(expo.astype(BF16), v_wide, preferred_element_type=F32)
            return unused

        lax.fori_loop(0, q_tiles, q_rows, 0)
        return unused

    lax.fori_loop(0, sp, block, 0)

    def close(t, unused):
        at = pl.ds(pl.multiple_of(t * q_tile, q_tile), q_tile)
        for pair in range(heads // 2):
            two = [acc[2 * pair + n, at, :] for n in range(2)]
            two = [v[:, :head] / v[:, head:] for v in two]
            attended[at, pair * 2 * head : (pair + 1) * 2 * head] = jnp.concatenate(two, axis=1).astype(BF16)
        return unused

    lax.fori_loop(0, q_tiles, close, 0)
    if ring:
        for number in range(tiles):
            for index in range(6):
                ring_copy(number, index).wait_send()
    else:
        for step in range(1, sp):
            direct(step).wait_send()
    for item in sends + outs:
        item.wait_send()
    gather.finish()


def back_kernel(tp, att, weight, out, full, wide, total, mixed, landed, send, recv, asend, arecv, local):
    f = lax.axis_index("tp")
    rows, cols = att.shape
    own_rows = out.shape[0]
    out_cols = weight.shape[1]
    load = pltpu.make_async_copy(weight, wide, local.at[0])
    load.start()
    mine = pltpu.make_async_copy(att, full.at[f], local.at[1])
    mine.start()
    greet(others("tp", tp))
    gather = Gather(tp, att, full, send, recv)
    gather.start()
    gather.second()
    total[...] = jnp.zeros(total.shape, F32)
    gather.relay()
    mine.wait()
    load.wait()
    r_tile = min(256, rows)

    def chip_step(index, unused):
        gather.before(index)
        chip = gather.chip(index)

        def row_step(t, unused):
            at = pl.ds(pl.multiple_of(t * r_tile, r_tile), r_tile)
            value = total[at, :]
            for n in range(2):
                source = chip * 2 + n
                depth = pl.ds(pl.multiple_of(source * cols, cols), cols)
                value = value + jnp.dot(full[source, at, :], wide[depth, :], preferred_element_type=F32)
            total[at, :] = value
            return unused

        lax.fori_loop(0, rows // r_tile, row_step, 0)
        return unused

    lax.fori_loop(0, tp // 2, chip_step, 0)
    for peer in range(tp):
        mixed[peer] = total[peer * own_rows : (peer + 1) * own_rows, :].astype(BF16)
    sends = []
    for step in range(1, tp):
        peer = lax.rem(f + step, tp)
        sends.append(remote(mixed.at[peer], landed.at[f], asend, arecv, step - 1, "tp", peer))
    for item in sends:
        item.start()
    landed[f] = mixed[f]
    for step in range(1, tp):
        origin = lax.rem(f - step + tp, tp)
        remote(landed.at[origin], landed.at[origin], asend, arecv, step - 1, "tp", origin).wait_recv()
    for n in range(tp):
        out[:, n * out_cols : (n + 1) * out_cols] = landed[n]
    for item in sends:
        item.wait_send()
    gather.finish()


def tables(first, count, head):
    freqs = head // 4
    lane = jnp.arange(2 * head, dtype=jnp.int32) % head
    inverse = 10000.0 ** (-(lane // 2 % freqs).astype(F32) / freqs)
    sign = jnp.where(lane % 2 == 0, -1.0, 1.0)
    grid_rows = -(-(count // GRID_W) // 8) * 8
    index = jnp.arange(grid_rows + GRID_W, dtype=jnp.int32)
    spot = jnp.where(index < grid_rows, index + first // GRID_W, index - grid_rows)
    angles = spot.astype(F32)[:, None] * inverse
    return jnp.cos(angles), jnp.sin(angles) * sign


def local(sp, tp, latent, context, condition, context_cond, mod_weight, norm_gain, query_weight, key_weight,
          value_weight, out_weight, query_gain, key_gain, context_lift):
    rows, model = latent.shape
    ctx_rows = context.shape[0]
    head = query_gain.shape[0]
    heads = query_weight.shape[1] // head
    kv_heads = key_weight.shape[1] // head
    width = key_weight.shape[1]
    slots = query_weight.shape[1] // width + 2
    block = rows * tp
    keys = block + ctx_rows
    limit = 60 * 1024 * 1024
    cond_pair = jax.nn.silu(jnp.stack([condition, context_cond])).astype(BF16)
    mcols = mod_weight.shape[1]
    cos, sin = tables(lax.axis_index("sp") * block, block, head)
    stacked = width % 128 != 0
    weights = [query_weight, key_weight, value_weight]
    if stacked:
        weights = [jnp.stack([query_weight[:, n * width : (n + 1) * width] for n in range(slots - 2)] + weights[1:])]
    dma = pltpu.SemaphoreType.DMA
    count = gather_sems(tp)
    pieces = (tp // 2 + 1) * 6 if sp == 4 else sp - 1
    attended, gate = pl.pallas_call(
        functools.partial(front_kernel, sp, tp, heads, kv_heads, head, stacked),
        name="front",
        out_shape=(jax.ShapeDtypeStruct((block, heads * head), BF16), jax.ShapeDtypeStruct((1, model), F32)),
        in_specs=[ANY, ANY, VMEM, ANY, VMEM, VMEM, VMEM, VMEM, VMEM, SMEM] + [ANY] * len(weights),
        out_specs=(VMEM, VMEM),
        scratch_shapes=[
            pltpu.VMEM((tp + 2, rows, model), BF16),
            pltpu.VMEM((2 * rows, model), BF16),
            pltpu.VMEM((slots, model, width), BF16),
            pltpu.VMEM(mod_weight.shape, BF16),
            pltpu.VMEM((sp, 2, mcols), F32),
            pltpu.VMEM((2, mcols), F32),
            pltpu.VMEM((2, mcols), F32),
            pltpu.VMEM((2, mcols * tp), F32),
            pltpu.VMEM((2, 1, model), F32),
            pltpu.VMEM((2, 1, model), F32),
            pltpu.VMEM((slots, 1, width), F32),
            pltpu.VMEM((slots - 2, block, width), BF16),
            pltpu.VMEM((sp, 2, keys, width), BF16),
            pltpu.VMEM((heads, block, 1), F32),
            pltpu.VMEM((heads, block, 2 * head), F32),
            dma((count,)), dma((count,)), dma((sp - 1,)), dma((sp - 1,)), dma((tp - 1,)), dma((tp - 1,)),
            dma((pieces,)), dma((pieces,)),
            dma((slots + 4,)),
        ],
        compiler_params=pltpu.CompilerParams(collective_id=0, has_side_effects=True, vmem_limit_bytes=limit),
    )(latent, context, cond_pair, mod_weight, norm_gain.reshape(1, model), cos, sin, query_gain.reshape(1, head),
      key_gain.reshape(1, head), context_lift, *weights)
    mixed = pl.pallas_call(
        functools.partial(back_kernel, tp),
        name="back",
        out_shape=jax.ShapeDtypeStruct((rows, model), BF16),
        in_specs=[VMEM, ANY],
        out_specs=VMEM,
        scratch_shapes=[
            pltpu.VMEM((tp, block, heads * head), BF16),
            pltpu.VMEM(out_weight.shape, BF16),
            pltpu.VMEM((block, out_weight.shape[1]), F32),
            pltpu.VMEM((tp, rows, out_weight.shape[1]), BF16),
            pltpu.VMEM((tp, rows, out_weight.shape[1]), BF16),
            dma((count,)), dma((count,)), dma((tp - 1,)), dma((tp - 1,)), dma((2,)),
        ],
        compiler_params=pltpu.CompilerParams(collective_id=2, has_side_effects=True, vmem_limit_bytes=limit),
    )(attended, out_weight)
    return (latent.astype(F32) + gate * mixed.astype(F32)).astype(BF16)


def partner(s, order):
    return jnp.where(order == 0, s, jnp.where(order == 1, s + 1 - 2 * (s % 2), jnp.where(order == 2, 3 - s, (s + 2) % 4)))


class Square:
    def __init__(self, own, full, send, recv, base):
        self.own, self.full, self.send, self.recv, self.base = own, full, send, recv, base
        me = lax.axis_index("tp")
        self.me = me
        self.half = own.shape[0] // 2
        core, x, y = me % 2, (me // 2) % 2, me // 4
        self.sib = me + 1 - 2 * core
        self.step = 1 - 2 * core
        self.xn = me + 2 - 4 * x
        self.yn = me + 4 - 8 * y
        self.dn = self.xn + 4 - 8 * y

    def part(self, ref, which):
        return ref if which is None else ref.at[pl.ds(which * self.half, self.half)]

    def copy(self, index):
        me, xn, yn, dn, sib = self.me, self.xn, self.yn, self.dn, self.sib
        origin, half, peer = {
            0: (me, 0, xn), 1: (me, 1, xn), 2: (me, 0, yn), 3: (me, 1, yn), 4: (me, None, sib),
            5: (xn, 1, yn), 6: (yn, 0, xn),
            7: (xn, 0, sib), 8: (xn, 1, sib), 9: (yn, 0, sib), 10: (yn, 1, sib),
            11: (dn, 0, sib), 12: (dn, 1, sib),
        }[index]
        source = self.own if index < 5 else self.full.at[origin]
        return remote(self.part(source, half), self.part(self.full.at[origin], half), self.send, self.recv,
                      self.base + index, "tp", peer)

    def start(self, *indices):
        for index in indices:
            self.copy(index).start()

    def arrived(self, *indices):
        xn, yn, dn, sib, step = self.xn, self.yn, self.dn, self.sib, self.step
        for index in indices:
            origin, half = {
                0: (xn, 0), 1: (xn, 1), 2: (yn, 0), 3: (yn, 1), 4: (sib, None), 5: (dn, 1), 6: (dn, 0),
                7: (xn + step, 0), 8: (xn + step, 1), 9: (yn + step, 0), 10: (yn + step, 1),
                11: (dn + step, 0), 12: (dn + step, 1),
            }[index]
            ref = self.part(self.full.at[origin], half)
            remote(ref, ref, self.send, self.recv, self.base + index, "tp", sib).wait_recv()

    def finish(self):
        for index in range(13):
            self.copy(index).wait_send()


class Cross(Square):
    def copy(self, index):
        origin, peer = {
            0: (self.me, self.xn), 1: (self.me, self.yn), 2: (self.me, self.dn), 3: (self.me, self.sib),
            4: (self.xn, self.sib), 5: (self.yn, self.sib), 6: (self.dn, self.sib),
        }[index]
        ref = self.full.at[origin]
        return remote(ref, ref, self.send, self.recv, self.base + index, "tp", peer)

    def arrived(self, *indices):
        for index in indices:
            origin = {
                0: self.xn, 1: self.yn, 2: self.dn, 3: self.sib,
                4: self.xn + self.step, 5: self.yn + self.step, 6: self.dn + self.step,
            }[index]
            ref = self.full.at[origin]
            remote(ref, ref, self.send, self.recv, self.base + index, "tp", self.sib).wait_recv()

    def finish(self):
        for index in range(7):
            self.copy(index).wait_send()


def whole_kernel(head, lat, ctx, cond_in, ctx_cond_in, mod_weight, gain_in, cos_in, sin_in, q_gain_in, k_gain_in, lift_in, wq, wk, wv, wo_in, out,
                 full, normed, wide, mod_wide, wo, parts, partial, total_mod, mod, gsc, shf, gains, cos, sin,
                 kv_out, kv_in, v_rows, q_out, q_in, o_out, att, total, mixed, landed, result, sc_a, sc_b, max_a, max_b,
                 cond, ctx_cond, gain, q_gain, k_gain, lift,
                 send, recv, psend, precv, msend, mrecv, ksend, krecv, qsend, qrecv, osend, orecv, asend, arecv,
                 bsend, brecv, local):
    sp, tp = 4, 8
    s, f = lax.axis_index("sp"), lax.axis_index("tp")
    rows, model = lat.shape
    tile = 2 * rows
    block = rows * tp
    ctx_rows = ctx.shape[0]
    mcols = partial.shape[1]
    half_rows = rows // 2
    width = wk.shape[1]
    pack = 2 * head
    chunk = block // 2
    scale = head ** -0.5

    mod_in = pltpu.make_async_copy(mod_weight, mod_wide, local.at[0])
    mod_in.start()
    small = [
        pltpu.make_async_copy(src, dst, local.at[9 + 4 + 2 + n])
        for n, (src, dst) in enumerate((
            (cond_in, cond), (ctx_cond_in, ctx_cond), (gain_in, gain), (q_gain_in, q_gain), (k_gain_in, k_gain), (lift_in, lift),
        ))
    ]
    for item in small:
        item.start()
    barrier = pltpu.get_barrier_semaphore()
    peers = others("tp", tp) + others("sp", sp)
    for axis, peer in peers:
        pl.semaphore_signal(barrier, inc=1, device_id={axis: peer}, device_id_type=MESH)
    ctx_in = [pltpu.make_async_copy(ctx.at[pl.ds(n * rows, rows)], full.at[tp + n], local.at[1 + n]) for n in range(2)]
    own = pltpu.make_async_copy(lat, full.at[f], local.at[3])
    weights = [
        pltpu.make_async_copy(wk, wide.at[0, :, pl.ds(0, width)], local.at[4]),
        pltpu.make_async_copy(wv, wide.at[0, :, pl.ds(width, width)], local.at[5]),
        pltpu.make_async_copy(wq, wide.at[1], local.at[6]),
    ]
    tabs = [pltpu.make_async_copy(cos_in, cos, local.at[7]), pltpu.make_async_copy(sin_in, sin, local.at[8])]
    out_w = [pltpu.make_async_copy(wo_in.at[:, n], wo.at[n], local.at[9 + n]) for n in range(sp)]
    pl.semaphore_wait(barrier, len(peers))
    gather = Square(lat, full, send, recv, 0)
    gather.start(1, 2, 4)
    for item in small:
        item.wait()
    pair = jnp.concatenate([cond[...], ctx_cond[...]], axis=0)
    pair = (pair / (1.0 + jnp.exp(-pair))).astype(BF16)
    mod_in.wait()
    for item in ctx_in + [own] + weights + tabs + out_w:
        item.start()
    first_sum = jnp.dot(pair, mod_wide[...], preferred_element_type=F32)
    partial[...] = first_sum
    parts[s] = first_sum
    sends = [remote(partial, parts.at[s], psend, precv, n - 1, "sp", partner(s, n)) for n in range(1, sp)]
    for item in sends:
        item.start()
    gains[0] = jnp.concatenate([k_gain[...]] * (width // head), axis=1)
    gains[1] = jnp.concatenate([q_gain[...] * scale] * (width // head), axis=1)
    total[...] = jnp.zeros(total.shape, F32)
    for n in range(1, sp):
        origin = partner(s, n)
        remote(parts.at[origin], parts.at[origin], psend, precv, n - 1, "sp", origin).wait_recv()
    summed = parts[0] + parts[1] + parts[2] + parts[3]
    total_mod[...] = summed
    here = pl.ds(pl.multiple_of(f * mcols, mcols), mcols)
    mod[:, here] = summed
    outs = [remote(total_mod, mod.at[:, here], msend, mrecv, step - 1, "tp", lax.rem(f + step, tp)) for step in range(1, tp)]
    for item in outs:
        item.start()
    gather.start(0, 3)
    for step in range(1, tp):
        origin = lax.rem(f - step + tp, tp)
        ref = mod.at[:, pl.ds(pl.multiple_of(origin * mcols, mcols), mcols)]
        remote(ref, ref, msend, mrecv, step - 1, "tp", origin).wait_recv()
    for r in range(2):
        gsc[r] = gain[...] * (1.0 + mod[r : r + 1, model : 2 * model])
        shf[r] = mod[r : r + 1, :model]
    gather.arrived(1)
    gather.start(5, 8)
    gather.arrived(2)
    gather.start(6, 9)
    for item in ctx_in + [own] + weights + tabs:
        item.wait()

    even = lax.broadcasted_iota(jnp.int32, (tile, width), 1) % 2 == 0
    same = (
        lax.broadcasted_iota(jnp.int32, (width, width), 0) // head
        == lax.broadcasted_iota(jnp.int32, (width, width), 1) // head
    )
    ones = jnp.where(same, 1.0, 0.0).astype(BF16)
    by_row = (lax.broadcasted_iota(jnp.int32, (1, pack), 1) % head) // 2 < head // 4
    low = lax.broadcasted_iota(jnp.int32, (tile, pack), 1) < head
    grid_rows = cos.shape[0] - GRID_W
    step_rows, wide_step = 16, 512
    steps = half_rows // step_rows

    def chip_at(index):
        x, y = (f // 2) % 2, f // 4
        return ((y + index // 2) % 2) * 2 + (x + index) % 2

    odd = s % 2

    def rows_at(number, plane):
        chip = chip_at(jnp.maximum(number - 1, 0))
        at_out = jnp.where(number == 0, block, chip * tile)
        at_in = jnp.where(number == 0, sp * block + plane * ctx_rows, plane * block + chip * tile)
        return pl.ds(pl.multiple_of(at_out, tile), tile), pl.ds(pl.multiple_of(at_in, tile), tile)

    def kv_send(number, a, n):
        at_out, at_in = rows_at(number, s)
        head_pack = 2 * odd + a if n == 3 else 2 * (1 - odd) + a
        return remote(kv_out.at[head_pack, at_out], kv_in.at[a, at_in], ksend, krecv, number * 6 + a * 3 + n - 1, "sp",
                      partner(s, n))

    def kv_wait(number, a, n):
        ref = kv_in.at[a, rows_at(number, partner(s, n))[1]]
        remote(ref, ref, ksend, krecv, number * 6 + a * 3 + n - 1, "sp", partner(s, n)).wait_recv()

    def q_copy(number, a):
        there = pl.ds(pl.multiple_of(chip_at(number - 1) * rows, rows), rows)
        return remote(q_out.at[2 * (1 - odd) + a, :, there], q_in.at[a, 1, :, there], qsend, qrecv, (number - 1) * 2 + a, "sp",
                      partner(s, 1))

    def q_wait(number, a):
        ref = q_in.at[a, 1, :, pl.ds(pl.multiple_of(chip_at(number - 1) * rows, rows), rows)]
        remote(ref, ref, qsend, qrecv, (number - 1) * 2 + a, "sp", partner(s, 1)).wait_recv()

    def one_tile(number, unused):
        @pl.when(number == 1)
        def _():
            gather.arrived(4)

        @pl.when(number == 2)
        def _():
            gather.arrived(0)
            gather.start(7)
            gather.arrived(3)
            gather.start(10)
            gather.arrived(7, 8)

        @pl.when(number == 3)
        def _():
            gather.arrived(9, 10)

        @pl.when(number == 4)
        def _():
            gather.arrived(5)
            gather.start(12)
            gather.arrived(6)
            gather.start(11)
            gather.arrived(12, 11)

        is_ctx = jnp.where(number == 0, 1, 0)
        chip = chip_at(jnp.maximum(number - 1, 0))
        base = jnp.where(number == 0, tp, chip * 2)

        def norm_rows(j, unused):
            slot = base + (j // steps) % 2
            row = pl.multiple_of((j // (2 * steps)) * half_rows + (j % steps) * step_rows, step_rows)
            there = pl.ds(pl.multiple_of(j * step_rows, step_rows), step_rows)
            squares = jnp.zeros((step_rows, 128), F32)
            for n in range(model // wide_step):
                v = full[slot, pl.ds(row, step_rows), n * wide_step : (n + 1) * wide_step].astype(F32)
                v = v * v
                for m in range(wide_step // 128):
                    squares = squares + v[:, m * 128 : (m + 1) * 128]
            inv = lax.rsqrt(jnp.sum(squares, axis=-1, keepdims=True) * (1.0 / model) + EPS)
            for n in range(model // wide_step):
                cols = slice(n * wide_step, (n + 1) * wide_step)
                v = full[slot, pl.ds(row, step_rows), cols].astype(F32)
                normed[there, cols] = (v * inv * gsc[is_ctx, :, cols] + shf[is_ctx, :, cols]).astype(BF16)
            return unused

        lax.fori_loop(0, tile // step_rows, norm_rows, 0, unroll=4)

        def table(ref, fill):
            pieces = []
            for c in range(2):
                for owner in range(2):
                    row = ref[pl.ds(s * tp + chip * 2 + owner, 1), :]
                    col = ref[grid_rows + c * half_rows : grid_rows + (c + 1) * half_rows, :]
                    pieces.append(jnp.where(by_row, row, col))
            v = jnp.concatenate(pieces, axis=0)
            v = jnp.where(is_ctx == 1, fill, v)
            return jnp.concatenate([v] * (width // pack), axis=1)

        cos_t, sin_t = table(cos, 1.0), table(sin, 0.0)

        def turned(y, row):
            sq = y * y
            hi = sq.astype(BF16)
            lo = (sq - hi.astype(F32)).astype(BF16)
            mean = jnp.dot(hi, ones, preferred_element_type=F32) + jnp.dot(lo, ones, preferred_element_type=F32)
            u = y * lax.rsqrt(mean * (1.0 / head) + EPS) * row
            other = jnp.where(even, pltpu.roll(u, width - 1, axis=1), pltpu.roll(u, 1, axis=1))
            return u * cos_t + other * sin_t

        y = jnp.dot(normed[...], wide[0], preferred_element_type=F32)
        k, v = turned(y[:, :width], gains[0]), y[:, width:]
        at_out, at_in = rows_at(number, s)
        for n in range(width // pack):
            kc, vc = k[:, n * pack : (n + 1) * pack], v[:, n * pack : (n + 1) * pack]
            kv_out[2 * n, at_out, :] = jnp.where(low, kc, pltpu.roll(vc, head, axis=1)).astype(BF16)
            kv_out[2 * n + 1, at_out, :] = jnp.where(low, pltpu.roll(kc, head, axis=1), vc).astype(BF16)
        for n in (2, 3, 1):
            kv_send(number, 0, n).start()

        @pl.when(number == 1)
        def _():
            for n in (2, 3, 1):
                kv_send(number - 1, 1, n).start()

        for a in range(2):
            kv_in[a, at_in, :] = kv_out[2 * odd + a, at_out, :]

        @pl.when(number > 0)
        def _():
            y = jnp.dot(normed[...], wide[1], preferred_element_type=F32)
            for n in range(2):
                q = turned(y[:, n * width : (n + 1) * width], gains[1]).astype(BF16)
                for m in range(2):
                    for c in range(2):
                        q_out[2 * n + m, c, pl.ds(pl.multiple_of(chip * rows, rows), rows), :] = (
                            q[c * rows : (c + 1) * rows, m * pack : (m + 1) * pack])
            for a in range(2):
                q_copy(number, a).start()

        return unused

    lax.fori_loop(0, tp // 2 + 1, one_tile, 0)

    def late_kv(number, unused):
        for n in (2, 3, 1):
            kv_send(number, 1, n).start()
        return unused

    lax.fori_loop(1, tp // 2 + 1, late_kv, 0)
    for a in range(2):
        q_in[a, 0] = q_out[2 * odd + a]
    keys = kv_in.shape[1]
    for item in out_w:
        item.wait()
    pieces = 2 * sp

    def step_at(p):
        return p // 4, (p % 4) // 2, p % 2

    def o_send(a, c):
        return remote(o_out.at[a, c], att.at[a * 4 + 2 + c, f], osend, orecv, a * 2 + c, "sp", partner(s, 1))

    def piece_of(p):
        return Cross(att.at[p, f], att.at[p], asend, arecv, p * 7)

    def back_send(c, step):
        peer = lax.rem(f + step, tp)
        return remote(mixed.at[c, peer], landed.at[c, f], bsend, brecv, c * (tp - 1) + step - 1, "tp", peer)

    def stage_zero(p):
        a, other, c = step_at(p)
        if other:
            ref = att.at[p, f]
            remote(ref, ref, osend, orecv, a * 2 + c, "sp", partner(s, 1)).wait_recv()
        piece_of(p).start(2, 0, 1, 3)

    def stage_one(p):
        piece = piece_of(p)
        piece.arrived(0, 1, 2)
        piece.start(4, 5, 6)

    def stage_three(p):
        piece_of(p).arrived(3, 4, 5, 6)
        a, other, c = step_at(p)
        source = 2 * (1 - odd) + a if other else 2 * odd + a
        left = jnp.concatenate([att[p, n] for n in range(tp)], axis=1)
        total[c] += jnp.dot(left, wo[source].reshape(tp * pack, wo.shape[3]), preferred_element_type=F32)

    def back(c):
        for n in range(tp):
            mixed[c, n] = total[c, n * half_rows : (n + 1) * half_rows, :].astype(BF16)
        for step in range(1, tp):
            back_send(c, step).start()
        landed[c, f] = mixed[c, f]

    key_step = block
    first_head = lax.broadcasted_iota(jnp.int32, (1, 2 * chunk), 1) < chunk

    def advance(a, m, old, old_max, new, new_max):
        if new is not None:
            _, other, c = step_at(m + 1)
            if m + 1 == 2:
                for number in range(1, tp // 2 + 1):
                    q_wait(number, a)
            lifts = jnp.where(first_head, lift[4 * odd + 2 * a], lift[4 * odd + 2 * a + 1])
            q = q_in[a, other, c]
            both = jnp.concatenate([q[:, :head], q[:, head:]], axis=0)
            high = None
        if old is not None:
            peak = jnp.max(old_max[...], axis=0, keepdims=True)
            acc = None
        for n in range(keys // key_step):
            there = slice(n * key_step, (n + 1) * key_step)
            if new is not None:
                scores = lax.dot_general(kv_in[a, there, :head], both, (((1,), (1,)), ((), ())), preferred_element_type=F32)
                if n >= sp:
                    scores = scores + lifts
                new[there, :] = scores
                part = jnp.max(scores.reshape(key_step // 8, 8, 2 * chunk), axis=0)
                high = part if high is None else jnp.maximum(high, part)
            if old is not None:
                expo = jnp.exp(old[there, :] - peak).astype(BF16)
                part = jnp.dot(v_rows[:, there], expo, preferred_element_type=F32)
                acc = part if acc is None else acc + part
        if new is not None:
            new_max[...] = high
        if old is None:
            return
        value = acc[:head] / acc[head : head + 1]
        value = jnp.concatenate([value[:, :chunk], value[:, chunk:]], axis=0).T.astype(BF16)
        _, other, c = step_at(m)
        if other:
            o_out[a, c] = value
            o_send(a, c).start()
        else:
            att[a * 4 + m, f] = value

    def run(a, m, *stages):
        @pl.when(a == m // 4)
        def _():
            for stage, p in stages:
                stage(p)

    zero, one, three = stage_zero, stage_one, stage_three

    def one_head(a, unused):
        def wait_kv(number, unused):
            for n in range(1, sp):
                kv_wait(number, a, n)
            return unused

        run(a, 4, (one, 0), (zero, 2), (zero, 3), (one, 1))
        lax.fori_loop(0, tp // 2 + 1, wait_kv, 0)
        v_rows[...] = jnp.concatenate([kv_in[a, :, head:].astype(F32), jnp.ones((keys, head), F32)], axis=1).T.astype(BF16)
        advance(a, -1, None, None, sc_a, max_a)
        advance(a, 0, sc_a, max_a, sc_b, max_b)
        run(a, 0, (zero, 0))
        run(a, 4, (zero, 4), (three, 0), (three, 1))
        advance(a, 1, sc_b, max_b, sc_a, max_a)
        run(a, 1, (zero, 1))
        run(a, 5, (zero, 5), (one, 2))
        advance(a, 2, sc_a, max_a, sc_b, max_b)
        run(a, 6, (three, 2))
        advance(a, 3, sc_b, max_b, None, None)
        return unused

    lax.fori_loop(0, 2, one_head, 0)
    one(3)
    zero(6)
    zero(7)
    three(3)
    one(4)
    one(5)
    three(4)
    one(6)
    three(5)
    three(6)
    back(0)
    one(7)
    three(7)
    back(1)
    cols = wo.shape[3]
    writes = []
    for c in range(2):
        for step in range(1, tp):
            origin = lax.rem(f - step + tp, tp)
            ref = landed.at[c, origin]
            remote(ref, ref, bsend, brecv, c * (tp - 1) + step - 1, "tp", origin).wait_recv()
        at = slice(c * half_rows, (c + 1) * half_rows)
        for n in range(tp):
            there = slice(n * cols, (n + 1) * cols)
            gate = mod[0:1, 2 * model + n * cols : 2 * model + (n + 1) * cols]
            result[at, there] = (full[f, at, there].astype(F32) + gate * landed[c, n].astype(F32)).astype(BF16)
        writes.append(pltpu.make_async_copy(result.at[pl.ds(c * half_rows, half_rows)], out.at[pl.ds(c * half_rows, half_rows)],
                                            local.at[9 + sp + c]))
        writes[-1].start()
    for item in sends + outs:
        item.wait_send()
    gather.finish()

    def drain_kv(number, unused):
        for a in range(2):
            for n in range(1, sp):
                kv_send(number, a, n).wait_send()
        return unused

    lax.fori_loop(0, tp // 2 + 1, drain_kv, 0)
    for a in range(2):
        for c in range(2):
            o_send(a, c).wait_send()
        for number in range(1, tp // 2 + 1):
            q_copy(number, a).wait_send()

    def drain_pieces(p, unused):
        piece_of(p).finish()
        return unused

    lax.fori_loop(0, pieces, drain_pieces, 0)
    for c in range(2):
        for step in range(1, tp):
            back_send(c, step).wait_send()
    for item in writes:
        item.wait()


def all_tables(count, head):
    freqs = head // 4
    lane = np.arange(2 * head) % head
    inverse = (10000.0 ** (-(lane // 2 % freqs).astype(np.float32) / freqs)).astype(np.float32)
    sign = np.where(lane % 2 == 0, -1.0, 1.0).astype(np.float32)
    spot = np.concatenate([np.arange(count // GRID_W), np.arange(GRID_W)]).astype(np.float32)
    angles = (spot[:, None] * inverse).astype(np.float32)
    return np.cos(angles).astype(np.float32), (np.sin(angles) * sign).astype(np.float32)


def whole(sp, tp, latent, context, condition, context_cond, mod_weight, norm_gain, query_weight, key_weight,
          value_weight, out_weight, query_gain, key_gain, context_lift):
    rows, model = latent.shape
    head = query_gain.shape[0]
    block = rows * tp
    ctx_rows = context.shape[0]
    width = key_weight.shape[1]
    mcols = mod_weight.shape[1]
    out_cols = out_weight.shape[1]
    pack = 2 * head
    chunk = block // 2
    keys = sp * (block + ctx_rows)
    cos, sin = all_tables(sp * block, head)
    dma = lambda *shape: pltpu.SemaphoreType.DMA(shape)
    vm = pltpu.VMEM
    tiles = tp // 2 + 1
    return pl.pallas_call(
        functools.partial(whole_kernel, head),
        name="whole",
        out_shape=jax.ShapeDtypeStruct((rows, model), BF16),
        in_specs=[ANY] * 15,
        out_specs=ANY,
        scratch_shapes=[
            vm((tp + 2, rows, model), BF16),
            vm((2 * rows, model), BF16),
            vm((2, model, 2 * width), BF16),
            vm(mod_weight.shape, BF16),
            vm((sp, tp, pack, out_cols), BF16),
            vm((sp, 2, mcols), F32),
            vm((2, mcols), F32),
            vm((2, mcols), F32),
            vm((2, mcols * tp), F32),
            vm((2, 1, model), F32),
            vm((2, 1, model), F32),
            vm((2, 1, width), F32),
            vm(cos.shape, F32),
            vm(sin.shape, F32),
            vm((sp, block + ctx_rows, pack), BF16),
            vm((2, keys, pack), BF16),
            vm((pack, keys), BF16),
            vm((sp, 2, chunk, pack), BF16),
            vm((2, 2, 2, chunk, pack), BF16),
            vm((2, 2, chunk, pack), BF16),
            vm((2 * sp, tp, chunk, pack), BF16),
            vm((2, chunk, out_cols), F32),
            vm((2, tp, rows // 2, out_cols), BF16),
            vm((2, tp, rows // 2, out_cols), BF16),
            vm((rows, model), BF16),
            vm((keys, 2 * chunk), F32),
            vm((keys, 2 * chunk), F32),
            vm((8, 2 * chunk), F32),
            vm((8, 2 * chunk), F32),
            vm((1, condition.shape[0]), F32),
            vm((1, condition.shape[0]), F32),
            vm((1, model), F32),
            vm((1, head), F32),
            vm((1, head), F32),
            pltpu.SMEM(context_lift.shape, F32),
            dma(13), dma(13), dma(sp - 1), dma(sp - 1), dma(tp - 1), dma(tp - 1),
            dma(tiles * 6), dma(tiles * 6), dma(8), dma(8), dma(4), dma(4),
            dma(7 * 8), dma(7 * 8), dma(2 * (tp - 1)), dma(2 * (tp - 1)),
            dma(9 + sp + 8),
        ],
        compiler_params=pltpu.CompilerParams(collective_id=1, has_side_effects=True, vmem_limit_bytes=62 * 1024 * 1024),
    )(latent, context, condition.reshape(1, -1), context_cond.reshape(1, -1), mod_weight, norm_gain.reshape(1, model),
      cos, sin, query_gain.reshape(1, head), key_gain.reshape(1, head), context_lift, query_weight, key_weight,
      value_weight, out_weight.reshape(tp, sp, pack, out_cols))


def fits(sp, tp, latent, context, key_weight, query_weight, query_gain):
    head = query_gain.shape[0]
    return (
        sp == 4 and tp == 8 and latent.shape[0] == GRID_W and context.shape[0] == 2 * latent.shape[0]
        and 2 * head == 128 and key_weight.shape[1] == sp * head and query_weight.shape[1] == 2 * sp * head
    )


def chosen(sp, tp, *args):
    latent, context, query_weight, key_weight, query_gain = args[0], args[1], args[6], args[7], args[10]
    if fits(sp, tp, latent, context, key_weight, query_weight, query_gain):
        return whole(sp, tp, *args)
    return local(sp, tp, *args)


def solution(mesh):
    return jax.shard_map(
        functools.partial(chosen, mesh.shape["sp"], mesh.shape["tp"]),
        mesh=mesh,
        in_specs=(
            P(("sp", "tp"), None),
            P("sp", None),
            P("sp"),
            P("sp"),
            P("sp", "tp"),
            P(),
            P(None, "tp"),
            P(None, "tp"),
            P(None, "tp"),
            P(None, "tp"),
            P(),
            P(),
            P("tp"),
        ),
        out_specs=P(("sp", "tp"), None),
        check_vma=False,
    )
```

```python
import functools

import jax
import jax.numpy as jnp
import numpy as np
from jax import lax
from jax.experimental import pallas as pl
from jax.experimental.pallas import tpu as pltpu
from jax.sharding import PartitionSpec as P

GRID_W = 64
EPS = 1e-06
MESH = pl.DeviceIdType.MESH
ANY = pl.BlockSpec(memory_space=pl.ANY)
VMEM = pl.BlockSpec(memory_space=pltpu.VMEM)
SMEM = pl.BlockSpec(memory_space=pltpu.SMEM)
BF16 = jnp.bfloat16
F32 = jnp.float32


def remote(src, dst, send, recv, index, axis, peer):
    return pltpu.make_async_remote_copy(
        src_ref=src, dst_ref=dst, send_sem=send.at[index], recv_sem=recv.at[index],
        device_id={axis: peer}, device_id_type=MESH,
    )


def greet(peers):
    barrier = pltpu.get_barrier_semaphore()
    for axis, peer in peers:
        pl.semaphore_signal(barrier, inc=1, device_id={axis: peer}, device_id_type=MESH)
    pl.semaphore_wait(barrier, len(peers))


def others(axis, count):
    me = lax.axis_index(axis)
    return [(axis, lax.rem(me + step, count)) for step in range(1, count)]


def gather_sems(count):
    return 13 if count == 8 else max(count - 1, 1)


class Gather:
    def __init__(self, count, own, full, send, recv):
        self.count, self.own, self.full, self.send, self.recv = count, own, full, send, recv
        self.me = lax.axis_index("tp")
        self.half = own.shape[0] // 2
        me = self.me
        if count == 8:
            self.core, self.x, self.y = me % 2, (me // 2) % 2, me // 4
            self.sib = me + 1 - 2 * self.core
            self.step = 1 - 2 * self.core
            self.xn = me + 2 - 4 * self.x
            self.yn = me + 4 - 8 * self.y
            self.dn = self.xn + 4 - 8 * self.y

    def part(self, ref, which):
        return ref if which is None else ref.at[pl.ds(which * self.half, self.half)]

    def copy(self, index):
        me, xn, yn, dn, sib = self.me, self.xn, self.yn, self.dn, self.sib
        origin, half, peer = {
            0: (me, 0, xn), 1: (me, 1, xn), 2: (me, 0, yn), 3: (me, 1, yn), 4: (me, None, sib),
            5: (xn, 1, yn), 6: (yn, 0, xn),
            7: (xn, 0, sib), 8: (xn, 1, sib), 9: (yn, 0, sib), 10: (yn, 1, sib),
            11: (dn, 0, sib), 12: (dn, 1, sib),
        }[index]
        source = self.own if index < 5 else self.full.at[origin]
        return remote(self.part(source, half), self.part(self.full.at[origin], half), self.send, self.recv, index, "tp", peer)

    def wait_recv(self, index):
        xn, yn, dn, sib, step = self.xn, self.yn, self.dn, self.sib, self.step
        origin, half = {
            0: (xn, 0), 1: (xn, 1), 2: (yn, 0), 3: (yn, 1), 4: (sib, None), 5: (dn, 1), 6: (dn, 0),
            7: (xn + step, 0), 8: (xn + step, 1), 9: (yn + step, 0), 10: (yn + step, 1),
            11: (dn + step, 0), 12: (dn + step, 1),
        }[index]
        ref = self.part(self.full.at[origin], half)
        remote(ref, ref, self.send, self.recv, index, "tp", sib).wait_recv()

    def direct(self, step):
        peer = lax.rem(self.me + step, self.count)
        return remote(self.own, self.full.at[self.me], self.send, self.recv, step - 1, "tp", peer)

    def start(self):
        if self.count == 8:
            for index in (1, 2, 4):
                self.copy(index).start()
        else:
            for step in range(1, self.count):
                self.direct(step).start()

    def second(self):
        if self.count == 8:
            for index in (0, 3):
                self.copy(index).start()

    def relay(self):
        if self.count == 8:
            for arrived, then in ((1, (5, 8)), (2, (6, 9))):
                self.wait_recv(arrived)
                for nxt in then:
                    self.copy(nxt).start()

    def before(self, index):
        if self.count != 8:
            @pl.when(index == 0)
            def _():
                for step in range(1, self.count):
                    origin = lax.rem(self.me - step + self.count, self.count)
                    ref = self.full.at[origin]
                    remote(ref, ref, self.send, self.recv, step - 1, "tp", origin).wait_recv()
            return

        @pl.when(index == 0)
        def _():
            self.wait_recv(4)

        @pl.when(index == 1)
        def _():
            for arrived, nxt in ((0, 7), (3, 10)):
                self.wait_recv(arrived)
                self.copy(nxt).start()
            self.wait_recv(7)
            self.wait_recv(8)

        @pl.when(index == 2)
        def _():
            self.wait_recv(9)
            self.wait_recv(10)

        @pl.when(index == 3)
        def _():
            self.wait_recv(5)
            self.copy(12).start()
            self.wait_recv(6)
            self.copy(11).start()
            self.wait_recv(12)
            self.wait_recv(11)

    def chip(self, index):
        if self.count == 8:
            return ((self.y + index // 2) % 2) * 2 + (self.x + index) % 2
        return index

    def finish(self):
        if self.count == 8:
            for index in range(13):
                self.copy(index).wait_send()
        else:
            for step in range(1, self.count):
                self.direct(step).wait_send()


def front_kernel(sp, tp, heads, kv_heads, head, stacked, lat, ctx, cond, mod_weight, gain, cos, sin, q_gain, k_gain, lift, *rest):
    weights, rest = rest[: 1 if stacked else 3], rest[1 if stacked else 3 :]
    (attended, gate, full, normed, wide, mod_wide, parts, partial, total, mod, gsc, shf, gains, q_all, kvs, top, acc,
     send, recv, psend, precv, msend, mrecv, zsend, zrecv, local) = rest
    s, f = lax.axis_index("sp"), lax.axis_index("tp")
    rows, model = lat.shape
    width = wide.shape[2]
    slots = wide.shape[0]
    groups = slots - 2
    tile = 2 * rows
    lat_rows = rows * tp
    keys = kvs.shape[2]
    mcols = partial.shape[1]
    tiles = tp // 2 + 1
    scale = head ** -0.5
    mod_in = pltpu.make_async_copy(mod_weight, mod_wide, local.at[slots + 3])
    mod_in.start()
    copies = []
    if stacked:
        copies.append(pltpu.make_async_copy(weights[0], wide, local.at[0]))
    else:
        for n in range(groups):
            copies.append(pltpu.make_async_copy(weights[0].at[:, n * width : (n + 1) * width], wide.at[n], local.at[n]))
        copies.append(pltpu.make_async_copy(weights[1], wide.at[groups], local.at[groups]))
        copies.append(pltpu.make_async_copy(weights[2], wide.at[groups + 1], local.at[groups + 1]))
    own = pltpu.make_async_copy(lat, full.at[f], local.at[slots])
    ctx_in = [
        pltpu.make_async_copy(ctx.at[pl.ds(n * rows, rows)], full.at[tp + n], local.at[slots + 1 + n]) for n in range(2)
    ]
    greet(others("tp", tp) + others("sp", sp))
    gather = Gather(tp, lat, full, send, recv)
    gather.start()
    for item in ctx_in + [own] + copies[::-1]:
        item.start()
    mod_in.wait()
    first_sum = jnp.dot(cond[...], mod_wide[...], preferred_element_type=F32)
    partial[...] = first_sum
    parts[s] = first_sum
    sends = []
    for step in range(1, sp):
        sends.append(remote(partial, parts.at[s], psend, precv, step - 1, "sp", lax.rem(s + step, sp)))
    for item in sends:
        item.start()
    for n in range(slots):
        row = q_gain[...] * scale if n < groups else k_gain[...]
        gains[n] = jnp.concatenate([row] * (width // head), axis=1) if width > head else row
    for step in range(1, sp):
        origin = lax.rem(s - step + sp, sp)
        remote(parts.at[origin], parts.at[origin], psend, precv, step - 1, "sp", origin).wait_recv()
    summed = parts[0]
    for n in range(1, sp):
        summed = summed + parts[n]
    total[...] = summed
    here = pl.ds(pl.multiple_of(f * mcols, mcols), mcols)
    mod[:, here] = summed
    outs = []
    for step in range(1, tp):
        outs.append(remote(total, mod.at[:, here], msend, mrecv, step - 1, "tp", lax.rem(f + step, tp)))
    for item in outs:
        item.start()
    gather.second()
    top[...] = jnp.full(top.shape, -1e30, F32)
    acc[...] = jnp.zeros(acc.shape, F32)
    for step in range(1, tp):
        origin = lax.rem(f - step + tp, tp)
        ref = mod.at[:, pl.ds(pl.multiple_of(origin * mcols, mcols), mcols)]
        remote(ref, ref, msend, mrecv, step - 1, "tp", origin).wait_recv()
    for r in range(2):
        gsc[r] = gain[...] * (1.0 + mod[r : r + 1, model : 2 * model])
        shf[r] = mod[r : r + 1, :model]
    gate[...] = mod[0:1, 2 * model :]
    gather.relay()
    for item in ctx_in + copies:
        item.wait()
    own.wait()

    ring = sp == 4
    right, left, far = (s + 1) % sp, (s + sp - 1) % sp, (s + 2) % sp

    def tile_first(number):
        if isinstance(number, int):
            return lat_rows if number == 0 else pl.multiple_of(gather.chip(number - 1) * tile, tile)
        chip = jnp.where(number == 0, tp // 2, gather.chip(jnp.maximum(number - 1, 0)))
        return pl.multiple_of(chip * tile, tile)

    def ring_copy(number, index):
        which, origin, peer = {
            0: (0, s, right), 1: (1, s, right), 2: (1, s, left), 3: (0, s, left), 4: (0, left, right), 5: (1, right, left),
        }[index]
        ref = kvs.at[origin, which, pl.ds(tile_first(number), tile)]
        return remote(ref, ref, zsend, zrecv, number * 6 + index, "sp", peer)

    def ring_wait(number, index):
        which, origin = {0: (0, left), 1: (1, left), 2: (1, right), 3: (0, right), 4: (0, far), 5: (1, far)}[index]
        ref = kvs.at[origin, which, pl.ds(tile_first(number), tile)]
        remote(ref, ref, zsend, zrecv, number * 6 + index, "sp", right).wait_recv()

    def forward(number):
        ring_wait(number, 0)
        ring_copy(number, 4).start()
        ring_wait(number, 2)
        ring_copy(number, 5).start()

    def direct(step):
        return remote(kvs.at[s], kvs.at[s], zsend, zrecv, step - 1, "sp", lax.rem(s + step, sp))

    even = lax.broadcasted_iota(jnp.int32, (tile, width), 1) % 2 == 0
    same = (
        lax.broadcasted_iota(jnp.int32, (width, width), 0) // head
        == lax.broadcasted_iota(jnp.int32, (width, width), 1) // head
    )
    ones = jnp.where(same, 1.0, 0.0).astype(BF16)
    by_row = (lax.broadcasted_iota(jnp.int32, (1, 2 * head), 1) % head) // 2 < head // 4
    grid_rows = cos.shape[0] - GRID_W
    part = min(tile, GRID_W)
    step_rows = 16

    def roll(v, by):
        if width % 128 == 0:
            return pltpu.roll(v, by % width, axis=1)
        return jnp.concatenate([v[:, width - by % width :], v[:, : width - by % width]], axis=1)

    def table(ref, first, is_ctx, fill):
        pieces = []
        for k in range(tile // part):
            at = jnp.where(is_ctx == 1, 0, first + k * part)
            row = ref[pl.ds(at // GRID_W, 1), :]
            col = ref[pl.ds(pl.multiple_of(grid_rows + at % GRID_W, 8), part), :]
            pieces.append(jnp.where(by_row, row, col))
        v = jnp.concatenate(pieces, axis=0) if len(pieces) > 1 else pieces[0]
        v = jnp.where(is_ctx == 1, fill, v)
        if width > v.shape[1]:
            return jnp.concatenate([v] * (width // v.shape[1]), axis=1)
        return v[:, :width]

    def one_tile(number, unused):
        @pl.when(number > 0)
        def _():
            gather.before(number - 1)

        is_ctx = jnp.where(number == 0, 1, 0)
        first = tile_first(number)
        base = first // rows

        def norm_rows(j, unused):
            slot = base + (j * step_rows) // rows
            row = pl.multiple_of((j * step_rows) % rows, step_rows)
            v = full[slot, pl.ds(row, step_rows), :].astype(F32)
            inv = lax.rsqrt(jnp.mean(v * v, axis=-1, keepdims=True) + EPS)
            out = v * inv * gsc[is_ctx] + shf[is_ctx]
            normed[pl.ds(pl.multiple_of(j * step_rows, step_rows), step_rows), :] = out.astype(BF16)
            return unused

        lax.fori_loop(0, tile // step_rows, norm_rows, 0)

        def turned(y, n):
            sq = y * y
            hi = sq.astype(BF16)
            lo = (sq - hi.astype(F32)).astype(BF16)
            mean = jnp.dot(hi, ones, preferred_element_type=F32) + jnp.dot(lo, ones, preferred_element_type=F32)
            u = y * lax.rsqrt(mean * (1.0 / head) + EPS) * gains[n]
            other = jnp.where(even, roll(u, -1), roll(u, 1))
            return (u * table(cos, first, is_ctx, 1.0) + other * table(sin, first, is_ctx, 0.0)).astype(BF16)

        def one_slot(m, unused):
            n = (m + groups) % slots
            y = jnp.dot(normed[...], wide[n], preferred_element_type=F32)

            @pl.when(m == 1)
            def _():
                kvs[s, 1, pl.ds(first, tile), :] = y.astype(BF16)
                if ring:
                    for index in (0, 2, 1, 3):
                        ring_copy(number, index).start()

            @pl.when(m == 0)
            def _():
                kvs[s, 0, pl.ds(first, tile), :] = turned(y, n)

            @pl.when(m > 1)
            def _():
                q_all[n, pl.ds(first, tile), :] = turned(y, n)

            return unused

        lax.fori_loop(0, jnp.where(number == 0, 2, slots), one_slot, 0)
        return unused

    lax.fori_loop(0, tiles, one_tile, 0)

    if not ring:
        for step in range(1, sp):
            direct(step).start()
    group = heads // kv_heads
    q_tile = min(256, lat_rows)
    q_tiles = lat_rows // q_tile

    def block(b, unused):
        if ring:
            @pl.when(b == 0)
            def _():
                for number in range(tiles - 2):
                    forward(number)

            @pl.when(b == 1)
            def _():
                forward(tiles - 1)
                for number in range(tiles):
                    ring_wait(number, 1)

            @pl.when(b == 2)
            def _():
                for number in range(tiles):
                    ring_wait(number, 3)

            @pl.when(b == 3)
            def _():
                for number in range(tiles):
                    ring_wait(number, 4)
                    ring_wait(number, 5)

            origin = (s + jnp.where(b == 1, sp - 1, jnp.where(b == 2, 1, jnp.where(b == 3, 2, 0)))) % sp
        else:
            @pl.when(b == 1)
            def _():
                for step in range(1, sp):
                    source = lax.rem(s - step + sp, sp)
                    remote(kvs.at[source], kvs.at[source], zsend, zrecv, step - 1, "sp", source).wait_recv()

            origin = (s + b) % sp

        def q_rows(t, unused):
            if ring:
                @pl.when((b == 0) & (t == q_tiles - 1))
                def _():
                    forward(tiles - 2)

            at = pl.ds(pl.multiple_of(t * q_tile, q_tile), q_tile)
            for h in range(kv_heads):
                k = kvs[origin, 0, :, h * head : (h + 1) * head]
                v = kvs[origin, 1, :, h * head : (h + 1) * head]
                v_wide = jnp.concatenate([v, jnp.ones((keys, head), BF16)], axis=1)
                for g in range(group):
                    n = h * group + g
                    slot, lane = (n * head) // width, (n * head) % width
                    q = q_all[slot, at, lane : lane + head]
                    scores = lax.dot_general(q, k, (((1,), (1,)), ((), ())), preferred_element_type=F32)
                    scores = jnp.concatenate([scores[:, :lat_rows], scores[:, lat_rows:] + lift[n]], axis=1)
                    before = top[n, at, :]
                    now = jnp.maximum(before, jnp.max(scores, axis=-1, keepdims=True))
                    expo = jnp.exp(scores - now)
                    keep = jnp.exp(before - now)
                    top[n, at, :] = now
                    acc[n, at, :] = acc[n, at, :] * keep + jnp.dot(expo.astype(BF16), v_wide, preferred_element_type=F32)
            return unused

        lax.fori_loop(0, q_tiles, q_rows, 0)
        return unused

    lax.fori_loop(0, sp, block, 0)

    def close(t, unused):
        at = pl.ds(pl.multiple_of(t * q_tile, q_tile), q_tile)
        for pair in range(heads // 2):
            two = [acc[2 * pair + n, at, :] for n in range(2)]
            two = [v[:, :head] / v[:, head:] for v in two]
            attended[at, pair * 2 * head : (pair + 1) * 2 * head] = jnp.concatenate(two, axis=1).astype(BF16)
        return unused

    lax.fori_loop(0, q_tiles, close, 0)
    if ring:
        for number in range(tiles):
            for index in range(6):
                ring_copy(number, index).wait_send()
    else:
        for step in range(1, sp):
            direct(step).wait_send()
    for item in sends + outs:
        item.wait_send()
    gather.finish()


def back_kernel(tp, att, weight, out, full, wide, total, mixed, landed, send, recv, asend, arecv, local):
    f = lax.axis_index("tp")
    rows, cols = att.shape
    own_rows = out.shape[0]
    out_cols = weight.shape[1]
    load = pltpu.make_async_copy(weight, wide, local.at[0])
    load.start()
    mine = pltpu.make_async_copy(att, full.at[f], local.at[1])
    mine.start()
    greet(others("tp", tp))
    gather = Gather(tp, att, full, send, recv)
    gather.start()
    gather.second()
    total[...] = jnp.zeros(total.shape, F32)
    gather.relay()
    mine.wait()
    load.wait()
    r_tile = min(256, rows)

    def chip_step(index, unused):
        gather.before(index)
        chip = gather.chip(index)

        def row_step(t, unused):
            at = pl.ds(pl.multiple_of(t * r_tile, r_tile), r_tile)
            value = total[at, :]
            for n in range(2):
                source = chip * 2 + n
                depth = pl.ds(pl.multiple_of(source * cols, cols), cols)
                value = value + jnp.dot(full[source, at, :], wide[depth, :], preferred_element_type=F32)
            total[at, :] = value
            return unused

        lax.fori_loop(0, rows // r_tile, row_step, 0)
        return unused

    lax.fori_loop(0, tp // 2, chip_step, 0)
    for peer in range(tp):
        mixed[peer] = total[peer * own_rows : (peer + 1) * own_rows, :].astype(BF16)
    sends = []
    for step in range(1, tp):
        peer = lax.rem(f + step, tp)
        sends.append(remote(mixed.at[peer], landed.at[f], asend, arecv, step - 1, "tp", peer))
    for item in sends:
        item.start()
    landed[f] = mixed[f]
    for step in range(1, tp):
        origin = lax.rem(f - step + tp, tp)
        remote(landed.at[origin], landed.at[origin], asend, arecv, step - 1, "tp", origin).wait_recv()
    for n in range(tp):
        out[:, n * out_cols : (n + 1) * out_cols] = landed[n]
    for item in sends:
        item.wait_send()
    gather.finish()


def tables(first, count, head):
    freqs = head // 4
    lane = jnp.arange(2 * head, dtype=jnp.int32) % head
    inverse = 10000.0 ** (-(lane // 2 % freqs).astype(F32) / freqs)
    sign = jnp.where(lane % 2 == 0, -1.0, 1.0)
    grid_rows = -(-(count // GRID_W) // 8) * 8
    index = jnp.arange(grid_rows + GRID_W, dtype=jnp.int32)
    spot = jnp.where(index < grid_rows, index + first // GRID_W, index - grid_rows)
    angles = spot.astype(F32)[:, None] * inverse
    return jnp.cos(angles), jnp.sin(angles) * sign


def local(sp, tp, latent, context, condition, context_cond, mod_weight, norm_gain, query_weight, key_weight,
          value_weight, out_weight, query_gain, key_gain, context_lift):
    rows, model = latent.shape
    ctx_rows = context.shape[0]
    head = query_gain.shape[0]
    heads = query_weight.shape[1] // head
    kv_heads = key_weight.shape[1] // head
    width = key_weight.shape[1]
    slots = query_weight.shape[1] // width + 2
    block = rows * tp
    keys = block + ctx_rows
    limit = 60 * 1024 * 1024
    cond_pair = jax.nn.silu(jnp.stack([condition, context_cond])).astype(BF16)
    mcols = mod_weight.shape[1]
    cos, sin = tables(lax.axis_index("sp") * block, block, head)
    stacked = width % 128 != 0
    weights = [query_weight, key_weight, value_weight]
    if stacked:
        weights = [jnp.stack([query_weight[:, n * width : (n + 1) * width] for n in range(slots - 2)] + weights[1:])]
    dma = pltpu.SemaphoreType.DMA
    count = gather_sems(tp)
    pieces = (tp // 2 + 1) * 6 if sp == 4 else sp - 1
    attended, gate = pl.pallas_call(
        functools.partial(front_kernel, sp, tp, heads, kv_heads, head, stacked),
        name="front",
        out_shape=(jax.ShapeDtypeStruct((block, heads * head), BF16), jax.ShapeDtypeStruct((1, model), F32)),
        in_specs=[ANY, ANY, VMEM, ANY, VMEM, VMEM, VMEM, VMEM, VMEM, SMEM] + [ANY] * len(weights),
        out_specs=(VMEM, VMEM),
        scratch_shapes=[
            pltpu.VMEM((tp + 2, rows, model), BF16),
            pltpu.VMEM((2 * rows, model), BF16),
            pltpu.VMEM((slots, model, width), BF16),
            pltpu.VMEM(mod_weight.shape, BF16),
            pltpu.VMEM((sp, 2, mcols), F32),
            pltpu.VMEM((2, mcols), F32),
            pltpu.VMEM((2, mcols), F32),
            pltpu.VMEM((2, mcols * tp), F32),
            pltpu.VMEM((2, 1, model), F32),
            pltpu.VMEM((2, 1, model), F32),
            pltpu.VMEM((slots, 1, width), F32),
            pltpu.VMEM((slots - 2, block, width), BF16),
            pltpu.VMEM((sp, 2, keys, width), BF16),
            pltpu.VMEM((heads, block, 1), F32),
            pltpu.VMEM((heads, block, 2 * head), F32),
            dma((count,)), dma((count,)), dma((sp - 1,)), dma((sp - 1,)), dma((tp - 1,)), dma((tp - 1,)),
            dma((pieces,)), dma((pieces,)),
            dma((slots + 4,)),
        ],
        compiler_params=pltpu.CompilerParams(collective_id=0, has_side_effects=True, vmem_limit_bytes=limit),
    )(latent, context, cond_pair, mod_weight, norm_gain.reshape(1, model), cos, sin, query_gain.reshape(1, head),
      key_gain.reshape(1, head), context_lift, *weights)
    mixed = pl.pallas_call(
        functools.partial(back_kernel, tp),
        name="back",
        out_shape=jax.ShapeDtypeStruct((rows, model), BF16),
        in_specs=[VMEM, ANY],
        out_specs=VMEM,
        scratch_shapes=[
            pltpu.VMEM((tp, block, heads * head), BF16),
            pltpu.VMEM(out_weight.shape, BF16),
            pltpu.VMEM((block, out_weight.shape[1]), F32),
            pltpu.VMEM((tp, rows, out_weight.shape[1]), BF16),
            pltpu.VMEM((tp, rows, out_weight.shape[1]), BF16),
            dma((count,)), dma((count,)), dma((tp - 1,)), dma((tp - 1,)), dma((2,)),
        ],
        compiler_params=pltpu.CompilerParams(collective_id=2, has_side_effects=True, vmem_limit_bytes=limit),
    )(attended, out_weight)
    return (latent.astype(F32) + gate * mixed.astype(F32)).astype(BF16)


def partner(s, order):
    return jnp.where(order == 0, s, jnp.where(order == 1, s + 1 - 2 * (s % 2), jnp.where(order == 2, 3 - s, (s + 2) % 4)))


class Square:
    def __init__(self, own, full, send, recv, base):
        self.own, self.full, self.send, self.recv, self.base = own, full, send, recv, base
        me = lax.axis_index("tp")
        self.me = me
        self.half = own.shape[0] // 2
        core, x, y = me % 2, (me // 2) % 2, me // 4
        self.sib = me + 1 - 2 * core
        self.step = 1 - 2 * core
        self.xn = me + 2 - 4 * x
        self.yn = me + 4 - 8 * y
        self.dn = self.xn + 4 - 8 * y

    def part(self, ref, which):
        return ref if which is None else ref.at[pl.ds(which * self.half, self.half)]

    def copy(self, index):
        me, xn, yn, dn, sib = self.me, self.xn, self.yn, self.dn, self.sib
        origin, half, peer = {
            0: (me, 0, xn), 1: (me, 1, xn), 2: (me, 0, yn), 3: (me, 1, yn), 4: (me, None, sib),
            5: (xn, 1, yn), 6: (yn, 0, xn),
            7: (xn, 0, sib), 8: (xn, 1, sib), 9: (yn, 0, sib), 10: (yn, 1, sib),
            11: (dn, 0, sib), 12: (dn, 1, sib),
        }[index]
        source = self.own if index < 5 else self.full.at[origin]
        return remote(self.part(source, half), self.part(self.full.at[origin], half), self.send, self.recv,
                      self.base + index, "tp", peer)

    def start(self, *indices):
        for index in indices:
            self.copy(index).start()

    def arrived(self, *indices):
        xn, yn, dn, sib, step = self.xn, self.yn, self.dn, self.sib, self.step
        for index in indices:
            origin, half = {
                0: (xn, 0), 1: (xn, 1), 2: (yn, 0), 3: (yn, 1), 4: (sib, None), 5: (dn, 1), 6: (dn, 0),
                7: (xn + step, 0), 8: (xn + step, 1), 9: (yn + step, 0), 10: (yn + step, 1),
                11: (dn + step, 0), 12: (dn + step, 1),
            }[index]
            ref = self.part(self.full.at[origin], half)
            remote(ref, ref, self.send, self.recv, self.base + index, "tp", sib).wait_recv()

    def finish(self):
        for index in range(13):
            self.copy(index).wait_send()


class Cross(Square):
    def copy(self, index):
        origin, peer = {
            0: (self.me, self.xn), 1: (self.me, self.yn), 2: (self.me, self.dn), 3: (self.me, self.sib),
            4: (self.xn, self.sib), 5: (self.yn, self.sib), 6: (self.dn, self.sib),
        }[index]
        ref = self.full.at[origin]
        return remote(ref, ref, self.send, self.recv, self.base + index, "tp", peer)

    def arrived(self, *indices):
        for index in indices:
            origin = {
                0: self.xn, 1: self.yn, 2: self.dn, 3: self.sib,
                4: self.xn + self.step, 5: self.yn + self.step, 6: self.dn + self.step,
            }[index]
            ref = self.full.at[origin]
            remote(ref, ref, self.send, self.recv, self.base + index, "tp", self.sib).wait_recv()

    def finish(self):
        for index in range(7):
            self.copy(index).wait_send()


def whole_kernel(head, lat, ctx, cond_in, ctx_cond_in, mod_weight, gain_in, cos_in, sin_in, q_gain_in, k_gain_in, lift_in, wq, wk, wv, wo_in, out,
                 full, normed, wide, mod_wide, wo, parts, partial, total_mod, mod, gsc, shf, gains, cos, sin,
                 kv_out, kv_in, v_rows, q_out, q_in, o_out, att, total, mixed, landed, result, sc_a, sc_b, max_a, max_b,
                 cond, ctx_cond, gain, q_gain, k_gain, lift,
                 send, recv, psend, precv, msend, mrecv, ksend, krecv, qsend, qrecv, osend, orecv, asend, arecv,
                 bsend, brecv, local):
    sp, tp = 4, 8
    s, f = lax.axis_index("sp"), lax.axis_index("tp")
    rows, model = lat.shape
    tile = 2 * rows
    block = rows * tp
    ctx_rows = ctx.shape[0]
    mcols = partial.shape[1]
    half_rows = rows // 2
    width = wk.shape[1]
    pack = 2 * head
    chunk = block // 2
    scale = head ** -0.5

    mod_in = pltpu.make_async_copy(mod_weight, mod_wide, local.at[0])
    mod_in.start()
    small = [
        pltpu.make_async_copy(src, dst, local.at[9 + 4 + 2 + n])
        for n, (src, dst) in enumerate((
            (cond_in, cond), (ctx_cond_in, ctx_cond), (gain_in, gain), (q_gain_in, q_gain), (k_gain_in, k_gain), (lift_in, lift),
        ))
    ]
    for item in small:
        item.start()
    barrier = pltpu.get_barrier_semaphore()
    peers = others("tp", tp) + others("sp", sp)
    for axis, peer in peers:
        pl.semaphore_signal(barrier, inc=1, device_id={axis: peer}, device_id_type=MESH)
    ctx_in = [pltpu.make_async_copy(ctx.at[pl.ds(n * rows, rows)], full.at[tp + n], local.at[1 + n]) for n in range(2)]
    own = pltpu.make_async_copy(lat, full.at[f], local.at[3])
    weights = [
        pltpu.make_async_copy(wk, wide.at[0, :, pl.ds(0, width)], local.at[4]),
        pltpu.make_async_copy(wv, wide.at[0, :, pl.ds(width, width)], local.at[5]),
        pltpu.make_async_copy(wq, wide.at[1], local.at[6]),
    ]
    tabs = [pltpu.make_async_copy(cos_in, cos, local.at[7]), pltpu.make_async_copy(sin_in, sin, local.at[8])]
    out_w = [pltpu.make_async_copy(wo_in.at[:, n], wo.at[n], local.at[9 + n]) for n in range(sp)]
    pl.semaphore_wait(barrier, len(peers))
    gather = Square(lat, full, send, recv, 0)
    gather.start(1, 2, 4)
    for item in small:
        item.wait()
    pair = jnp.concatenate([cond[...], ctx_cond[...]], axis=0)
    pair = (pair / (1.0 + jnp.exp(-pair))).astype(BF16)
    mod_in.wait()
    for item in ctx_in + [own] + weights + tabs + out_w:
        item.start()
    first_sum = jnp.dot(pair, mod_wide[...], preferred_element_type=F32)
    partial[...] = first_sum
    parts[s] = first_sum
    sends = [remote(partial, parts.at[s], psend, precv, n - 1, "sp", partner(s, n)) for n in range(1, sp)]
    for item in sends:
        item.start()
    gains[0] = jnp.concatenate([k_gain[...]] * (width // head), axis=1)
    gains[1] = jnp.concatenate([q_gain[...] * scale] * (width // head), axis=1)
    total[...] = jnp.zeros(total.shape, F32)
    for n in range(1, sp):
        origin = partner(s, n)
        remote(parts.at[origin], parts.at[origin], psend, precv, n - 1, "sp", origin).wait_recv()
    summed = parts[0] + parts[1] + parts[2] + parts[3]
    total_mod[...] = summed
    here = pl.ds(pl.multiple_of(f * mcols, mcols), mcols)
    mod[:, here] = summed
    outs = [remote(total_mod, mod.at[:, here], msend, mrecv, step - 1, "tp", lax.rem(f + step, tp)) for step in range(1, tp)]
    for item in outs:
        item.start()
    gather.start(0, 3)
    for step in range(1, tp):
        origin = lax.rem(f - step + tp, tp)
        ref = mod.at[:, pl.ds(pl.multiple_of(origin * mcols, mcols), mcols)]
        remote(ref, ref, msend, mrecv, step - 1, "tp", origin).wait_recv()
    for r in range(2):
        gsc[r] = gain[...] * (1.0 + mod[r : r + 1, model : 2 * model])
        shf[r] = mod[r : r + 1, :model]
    gather.arrived(1)
    gather.start(5, 8)
    gather.arrived(2)
    gather.start(6, 9)
    for item in ctx_in + [own] + weights + tabs:
        item.wait()

    even = lax.broadcasted_iota(jnp.int32, (tile, width), 1) % 2 == 0
    same = (
        lax.broadcasted_iota(jnp.int32, (width, width), 0) // head
        == lax.broadcasted_iota(jnp.int32, (width, width), 1) // head
    )
    ones = jnp.where(same, 1.0, 0.0).astype(BF16)
    by_row = (lax.broadcasted_iota(jnp.int32, (1, pack), 1) % head) // 2 < head // 4
    low = lax.broadcasted_iota(jnp.int32, (tile, pack), 1) < head
    grid_rows = cos.shape[0] - GRID_W
    step_rows, wide_step = 16, 512
    steps = half_rows // step_rows

    def chip_at(index):
        x, y = (f // 2) % 2, f // 4
        return ((y + index // 2) % 2) * 2 + (x + index) % 2

    odd = s % 2

    def rows_at(number, plane):
        chip = chip_at(jnp.maximum(number - 1, 0))
        at_out = jnp.where(number == 0, block, chip * tile)
        at_in = jnp.where(number == 0, sp * block + plane * ctx_rows, plane * block + chip * tile)
        return pl.ds(pl.multiple_of(at_out, tile), tile), pl.ds(pl.multiple_of(at_in, tile), tile)

    def kv_send(number, a, n):
        at_out, at_in = rows_at(number, s)
        head_pack = 2 * odd + a if n == 3 else 2 * (1 - odd) + a
        return remote(kv_out.at[head_pack, at_out], kv_in.at[a, at_in], ksend, krecv, number * 6 + a * 3 + n - 1, "sp",
                      partner(s, n))

    def kv_wait(number, a, n):
        ref = kv_in.at[a, rows_at(number, partner(s, n))[1]]
        remote(ref, ref, ksend, krecv, number * 6 + a * 3 + n - 1, "sp", partner(s, n)).wait_recv()

    def q_copy(number, a):
        there = pl.ds(pl.multiple_of(chip_at(number - 1) * rows, rows), rows)
        return remote(q_out.at[2 * (1 - odd) + a, :, there], q_in.at[a, 1, :, there], qsend, qrecv, (number - 1) * 2 + a, "sp",
                      partner(s, 1))

    def q_wait(number, a):
        ref = q_in.at[a, 1, :, pl.ds(pl.multiple_of(chip_at(number - 1) * rows, rows), rows)]
        remote(ref, ref, qsend, qrecv, (number - 1) * 2 + a, "sp", partner(s, 1)).wait_recv()

    def one_tile(number, unused):
        @pl.when(number == 1)
        def _():
            gather.arrived(4)

        @pl.when(number == 2)
        def _():
            gather.arrived(0)
            gather.start(7)
            gather.arrived(3)
            gather.start(10)
            gather.arrived(7, 8)

        @pl.when(number == 3)
        def _():
            gather.arrived(9, 10)

        @pl.when(number == 4)
        def _():
            gather.arrived(5)
            gather.start(12)
            gather.arrived(6)
            gather.start(11)
            gather.arrived(12, 11)

        is_ctx = jnp.where(number == 0, 1, 0)
        chip = chip_at(jnp.maximum(number - 1, 0))
        base = jnp.where(number == 0, tp, chip * 2)

        def norm_rows(j, unused):
            slot = base + (j // steps) % 2
            row = pl.multiple_of((j // (2 * steps)) * half_rows + (j % steps) * step_rows, step_rows)
            there = pl.ds(pl.multiple_of(j * step_rows, step_rows), step_rows)
            squares = jnp.zeros((step_rows, 128), F32)
            for n in range(model // wide_step):
                v = full[slot, pl.ds(row, step_rows), n * wide_step : (n + 1) * wide_step].astype(F32)
                v = v * v
                for m in range(wide_step // 128):
                    squares = squares + v[:, m * 128 : (m + 1) * 128]
            inv = lax.rsqrt(jnp.sum(squares, axis=-1, keepdims=True) * (1.0 / model) + EPS)
            for n in range(model // wide_step):
                cols = slice(n * wide_step, (n + 1) * wide_step)
                v = full[slot, pl.ds(row, step_rows), cols].astype(F32)
                normed[there, cols] = (v * inv * gsc[is_ctx, :, cols] + shf[is_ctx, :, cols]).astype(BF16)
            return unused

        lax.fori_loop(0, tile // step_rows, norm_rows, 0, unroll=4)

        def table(ref, fill):
            pieces = []
            for c in range(2):
                for owner in range(2):
                    row = ref[pl.ds(s * tp + chip * 2 + owner, 1), :]
                    col = ref[grid_rows + c * half_rows : grid_rows + (c + 1) * half_rows, :]
                    pieces.append(jnp.where(by_row, row, col))
            v = jnp.concatenate(pieces, axis=0)
            v = jnp.where(is_ctx == 1, fill, v)
            return jnp.concatenate([v] * (width // pack), axis=1)

        cos_t, sin_t = table(cos, 1.0), table(sin, 0.0)

        def turned(y, row):
            sq = y * y
            hi = sq.astype(BF16)
            lo = (sq - hi.astype(F32)).astype(BF16)
            mean = jnp.dot(hi, ones, preferred_element_type=F32) + jnp.dot(lo, ones, preferred_element_type=F32)
            u = y * lax.rsqrt(mean * (1.0 / head) + EPS) * row
            other = jnp.where(even, pltpu.roll(u, width - 1, axis=1), pltpu.roll(u, 1, axis=1))
            return u * cos_t + other * sin_t

        y = jnp.dot(normed[...], wide[0], preferred_element_type=F32)
        k, v = turned(y[:, :width], gains[0]), y[:, width:]
        at_out, at_in = rows_at(number, s)
        for n in range(width // pack):
            kc, vc = k[:, n * pack : (n + 1) * pack], v[:, n * pack : (n + 1) * pack]
            kv_out[2 * n, at_out, :] = jnp.where(low, kc, pltpu.roll(vc, head, axis=1)).astype(BF16)
            kv_out[2 * n + 1, at_out, :] = jnp.where(low, pltpu.roll(kc, head, axis=1), vc).astype(BF16)
        for n in (2, 3, 1):
            kv_send(number, 0, n).start()

        @pl.when(number == 1)
        def _():
            for n in (2, 3, 1):
                kv_send(number - 1, 1, n).start()

        for a in range(2):
            kv_in[a, at_in, :] = kv_out[2 * odd + a, at_out, :]

        @pl.when(number > 0)
        def _():
            y = jnp.dot(normed[...], wide[1], preferred_element_type=F32)
            for n in range(2):
                q = turned(y[:, n * width : (n + 1) * width], gains[1]).astype(BF16)
                for m in range(2):
                    for c in range(2):
                        q_out[2 * n + m, c, pl.ds(pl.multiple_of(chip * rows, rows), rows), :] = (
                            q[c * rows : (c + 1) * rows, m * pack : (m + 1) * pack])
            for a in range(2):
                q_copy(number, a).start()

        return unused

    lax.fori_loop(0, tp // 2 + 1, one_tile, 0)

    def late_kv(number, unused):
        for n in (2, 3, 1):
            kv_send(number, 1, n).start()
        return unused

    lax.fori_loop(1, tp // 2 + 1, late_kv, 0)
    for a in range(2):
        q_in[a, 0] = q_out[2 * odd + a]
    keys = kv_in.shape[1]
    for item in out_w:
        item.wait()
    pieces = 2 * sp

    def step_at(p):
        return p // 4, (p % 4) // 2, p % 2

    def o_send(a, c):
        return remote(o_out.at[a, c], att.at[a * 4 + 2 + c, f], osend, orecv, a * 2 + c, "sp", partner(s, 1))

    def piece_of(p):
        return Cross(att.at[p, f], att.at[p], asend, arecv, p * 7)

    def back_send(c, step):
        peer = lax.rem(f + step, tp)
        return remote(mixed.at[c, peer], landed.at[c, f], bsend, brecv, c * (tp - 1) + step - 1, "tp", peer)

    def stage_zero(p):
        a, other, c = step_at(p)
        if other:
            ref = att.at[p, f]
            remote(ref, ref, osend, orecv, a * 2 + c, "sp", partner(s, 1)).wait_recv()
        piece_of(p).start(2, 0, 1, 3)

    def stage_one(p):
        piece = piece_of(p)
        piece.arrived(0, 1, 2)
        piece.start(4, 5, 6)

    def stage_three(p):
        piece_of(p).arrived(3, 4, 5, 6)
        a, other, c = step_at(p)
        source = 2 * (1 - odd) + a if other else 2 * odd + a
        left = jnp.concatenate([att[p, n] for n in range(tp)], axis=1)
        total[c] += jnp.dot(left, wo[source].reshape(tp * pack, wo.shape[3]), preferred_element_type=F32)

    def back(c):
        for n in range(tp):
            mixed[c, n] = total[c, n * half_rows : (n + 1) * half_rows, :].astype(BF16)
        for step in range(1, tp):
            back_send(c, step).start()
        landed[c, f] = mixed[c, f]

    key_step = block
    first_head = lax.broadcasted_iota(jnp.int32, (1, 2 * chunk), 1) < chunk

    def advance(a, m, old, old_max, new, new_max):
        if new is not None:
            _, other, c = step_at(m + 1)
            if m + 1 == 2:
                for number in range(1, tp // 2 + 1):
                    q_wait(number, a)
            lifts = jnp.where(first_head, lift[4 * odd + 2 * a], lift[4 * odd + 2 * a + 1])
            q = q_in[a, other, c]
            both = jnp.concatenate([q[:, :head], q[:, head:]], axis=0)
            high = None
        if old is not None:
            peak = jnp.max(old_max[...], axis=0, keepdims=True)
            acc = None
        for n in range(keys // key_step):
            there = slice(n * key_step, (n + 1) * key_step)
            if new is not None:
                scores = lax.dot_general(kv_in[a, there, :head], both, (((1,), (1,)), ((), ())), preferred_element_type=F32)
                if n >= sp:
                    scores = scores + lifts
                new[there, :] = scores
                part = jnp.max(scores.reshape(key_step // 8, 8, 2 * chunk), axis=0)
                high = part if high is None else jnp.maximum(high, part)
            if old is not None:
                expo = jnp.exp(old[there, :] - peak).astype(BF16)
                part = jnp.dot(v_rows[:, there], expo, preferred_element_type=F32)
                acc = part if acc is None else acc + part
        if new is not None:
            new_max[...] = high
        if old is None:
            return
        value = acc[:head] / acc[head : head + 1]
        value = jnp.concatenate([value[:, :chunk], value[:, chunk:]], axis=0).T.astype(BF16)
        _, other, c = step_at(m)
        if other:
            o_out[a, c] = value
            o_send(a, c).start()
        else:
            att[a * 4 + m, f] = value

    def run(a, m, *stages):
        @pl.when(a == m // 4)
        def _():
            for stage, p in stages:
                stage(p)

    zero, one, three = stage_zero, stage_one, stage_three

    def one_head(a, unused):
        def wait_near(number, unused):
            kv_wait(number, a, 1)
            return unused

        def wait_kv(number, unused):
            for n in (2, 3):
                kv_wait(number, a, n)
            return unused

        def turn_values(there, count):
            values = kv_in[a, there, head:].astype(F32)
            v_rows[:, there] = jnp.concatenate([values, jnp.ones((count, head), F32)], axis=1).T.astype(BF16)

        def turn_block(plane):
            turn_values(pl.ds(pl.multiple_of(plane * block, block), block), block)

        run(a, 4, (one, 0), (zero, 2), (zero, 3), (one, 1))
        lax.fori_loop(0, tp // 2 + 1, wait_near, 0)
        turn_block(s)
        turn_block(partner(s, 1))
        lax.fori_loop(0, tp // 2 + 1, wait_kv, 0)
        turn_block(partner(s, 2))
        turn_block(partner(s, 3))
        turn_values(slice(sp * block, keys), keys - sp * block)
        advance(a, -1, None, None, sc_a, max_a)
        advance(a, 0, sc_a, max_a, sc_b, max_b)
        run(a, 0, (zero, 0))
        run(a, 4, (zero, 4), (three, 0), (three, 1))
        advance(a, 1, sc_b, max_b, sc_a, max_a)
        run(a, 1, (zero, 1))
        run(a, 5, (zero, 5), (one, 2))
        advance(a, 2, sc_a, max_a, sc_b, max_b)
        run(a, 6, (three, 2))
        advance(a, 3, sc_b, max_b, None, None)
        return unused

    lax.fori_loop(0, 2, one_head, 0)
    one(3)
    zero(6)
    zero(7)
    three(3)
    one(4)
    one(5)
    three(4)
    one(6)
    three(5)
    three(6)
    back(0)
    one(7)
    three(7)
    back(1)
    cols = wo.shape[3]
    writes = []
    for c in range(2):
        for step in range(1, tp):
            origin = lax.rem(f - step + tp, tp)
            ref = landed.at[c, origin]
            remote(ref, ref, bsend, brecv, c * (tp - 1) + step - 1, "tp", origin).wait_recv()
        at = slice(c * half_rows, (c + 1) * half_rows)
        for n in range(tp):
            there = slice(n * cols, (n + 1) * cols)
            gate = mod[0:1, 2 * model + n * cols : 2 * model + (n + 1) * cols]
            result[at, there] = (full[f, at, there].astype(F32) + gate * landed[c, n].astype(F32)).astype(BF16)
        writes.append(pltpu.make_async_copy(result.at[pl.ds(c * half_rows, half_rows)], out.at[pl.ds(c * half_rows, half_rows)],
                                            local.at[9 + sp + c]))
        writes[-1].start()
    for item in sends + outs:
        item.wait_send()
    gather.finish()

    def drain_kv(number, unused):
        for a in range(2):
            for n in range(1, sp):
                kv_send(number, a, n).wait_send()
        return unused

    lax.fori_loop(0, tp // 2 + 1, drain_kv, 0)
    for a in range(2):
        for c in range(2):
            o_send(a, c).wait_send()
        for number in range(1, tp // 2 + 1):
            q_copy(number, a).wait_send()

    def drain_pieces(p, unused):
        piece_of(p).finish()
        return unused

    lax.fori_loop(0, pieces, drain_pieces, 0)
    for c in range(2):
        for step in range(1, tp):
            back_send(c, step).wait_send()
    for item in writes:
        item.wait()


def all_tables(count, head):
    freqs = head // 4
    lane = np.arange(2 * head) % head
    inverse = (10000.0 ** (-(lane // 2 % freqs).astype(np.float32) / freqs)).astype(np.float32)
    sign = np.where(lane % 2 == 0, -1.0, 1.0).astype(np.float32)
    spot = np.concatenate([np.arange(count // GRID_W), np.arange(GRID_W)]).astype(np.float32)
    angles = (spot[:, None] * inverse).astype(np.float32)
    return np.cos(angles).astype(np.float32), (np.sin(angles) * sign).astype(np.float32)


def whole(sp, tp, latent, context, condition, context_cond, mod_weight, norm_gain, query_weight, key_weight,
          value_weight, out_weight, query_gain, key_gain, context_lift):
    rows, model = latent.shape
    head = query_gain.shape[0]
    block = rows * tp
    ctx_rows = context.shape[0]
    width = key_weight.shape[1]
    mcols = mod_weight.shape[1]
    out_cols = out_weight.shape[1]
    pack = 2 * head
    chunk = block // 2
    keys = sp * (block + ctx_rows)
    cos, sin = all_tables(sp * block, head)
    dma = lambda *shape: pltpu.SemaphoreType.DMA(shape)
    vm = pltpu.VMEM
    tiles = tp // 2 + 1
    return pl.pallas_call(
        functools.partial(whole_kernel, head),
        name="whole",
        out_shape=jax.ShapeDtypeStruct((rows, model), BF16),
        in_specs=[ANY] * 15,
        out_specs=ANY,
        scratch_shapes=[
            vm((tp + 2, rows, model), BF16),
            vm((2 * rows, model), BF16),
            vm((2, model, 2 * width), BF16),
            vm(mod_weight.shape, BF16),
            vm((sp, tp, pack, out_cols), BF16),
            vm((sp, 2, mcols), F32),
            vm((2, mcols), F32),
            vm((2, mcols), F32),
            vm((2, mcols * tp), F32),
            vm((2, 1, model), F32),
            vm((2, 1, model), F32),
            vm((2, 1, width), F32),
            vm(cos.shape, F32),
            vm(sin.shape, F32),
            vm((sp, block + ctx_rows, pack), BF16),
            vm((2, keys, pack), BF16),
            vm((pack, keys), BF16),
            vm((sp, 2, chunk, pack), BF16),
            vm((2, 2, 2, chunk, pack), BF16),
            vm((2, 2, chunk, pack), BF16),
            vm((2 * sp, tp, chunk, pack), BF16),
            vm((2, chunk, out_cols), F32),
            vm((2, tp, rows // 2, out_cols), BF16),
            vm((2, tp, rows // 2, out_cols), BF16),
            vm((rows, model), BF16),
            vm((keys, 2 * chunk), F32),
            vm((keys, 2 * chunk), F32),
            vm((8, 2 * chunk), F32),
            vm((8, 2 * chunk), F32),
            vm((1, condition.shape[0]), F32),
            vm((1, condition.shape[0]), F32),
            vm((1, model), F32),
            vm((1, head), F32),
            vm((1, head), F32),
            pltpu.SMEM(context_lift.shape, F32),
            dma(13), dma(13), dma(sp - 1), dma(sp - 1), dma(tp - 1), dma(tp - 1),
            dma(tiles * 6), dma(tiles * 6), dma(8), dma(8), dma(4), dma(4),
            dma(7 * 8), dma(7 * 8), dma(2 * (tp - 1)), dma(2 * (tp - 1)),
            dma(9 + sp + 8),
        ],
        compiler_params=pltpu.CompilerParams(collective_id=1, has_side_effects=True, vmem_limit_bytes=62 * 1024 * 1024),
    )(latent, context, condition.reshape(1, -1), context_cond.reshape(1, -1), mod_weight, norm_gain.reshape(1, model),
      cos, sin, query_gain.reshape(1, head), key_gain.reshape(1, head), context_lift, query_weight, key_weight,
      value_weight, out_weight.reshape(tp, sp, pack, out_cols))


def fits(sp, tp, latent, context, key_weight, query_weight, query_gain):
    head = query_gain.shape[0]
    return (
        sp == 4 and tp == 8 and latent.shape[0] == GRID_W and context.shape[0] == 2 * latent.shape[0]
        and 2 * head == 128 and key_weight.shape[1] == sp * head and query_weight.shape[1] == 2 * sp * head
    )


def chosen(sp, tp, *args):
    latent, context, query_weight, key_weight, query_gain = args[0], args[1], args[6], args[7], args[10]
    if fits(sp, tp, latent, context, key_weight, query_weight, query_gain):
        return whole(sp, tp, *args)
    return local(sp, tp, *args)


def solution(mesh):
    return jax.shard_map(
        functools.partial(chosen, mesh.shape["sp"], mesh.shape["tp"]),
        mesh=mesh,
        in_specs=(
            P(("sp", "tp"), None),
            P("sp", None),
            P("sp"),
            P("sp"),
            P("sp", "tp"),
            P(),
            P(None, "tp"),
            P(None, "tp"),
            P(None, "tp"),
            P(None, "tp"),
            P(),
            P(),
            P("tp"),
        ),
        out_specs=P(("sp", "tp"), None),
        check_vma=False,
    )
```
